128 devices in a mesh: sp: 16 (over z, y), dp: 8 (over x, core).
Axes of the slice: x: 4, y: 4, z: 4, core: 2. Of those that a mesh axis runs over, the one named last changes fastest.
Arguments:
- residual: bfloat16 [8, 2048, 2048], P('dp', 'sp'), may hold values from -6 to 6
- head_input: bfloat16 [8, 2048, 2048], P('dp', 'sp'), may hold values from -6 to 6
- gate_input: bfloat16 [8, 2048, 2048], P('dp', 'sp'), may hold values from -6 to 6
- b_input: bfloat16 [8, 2048, 1024], P('dp', 'sp'), may hold values from -6 to 6
- c_input: bfloat16 [8, 2048, 1024], P('dp', 'sp'), may hold values from -6 to 6
- step_input: bfloat16 [8, 2048, 32], P('dp', 'sp'), may hold values from -4.8 to 4.8
- conv_weight: bfloat16 [4, 2048], replicated, may hold values from -3 to 3
- conv_b_weight: bfloat16 [4, 1024], replicated, may hold values from -3 to 3
- conv_c_weight: bfloat16 [4, 1024], replicated, may hold values from -3 to 3
- step_bias: float32 [32], replicated, may hold values from -1 to 1
- decay_log: float32 [32], replicated, may hold values from -9.92 to -2.99
- skip: float32 [32], replicated, may hold values from 0.5 to 1.5
- norm_gain: float32 [2048], replicated, may hold values from 0.1 to 1.9
- out_weight: bfloat16 [2048, 2048], P('dp'), may hold values from -0.125 to 0.125
- ffn_gain: float32 [2048], replicated, may hold values from 0.1 to 1.9
- shared_gate: bfloat16 [2048, 512], replicated, may hold values from -0.125 to 0.125
- shared_up: bfloat16 [2048, 512], replicated, may hold values from -0.125 to 0.125
- shared_down: bfloat16 [512, 2048], replicated, may hold values from -0.25 to 0.25
- expert_gate: bfloat16 [128, 2048, 512], P(('sp', 'dp')), may hold values from -0.125 to 0.125
- expert_up: bfloat16 [128, 2048, 512], P(('sp', 'dp')), may hold values from -0.125 to 0.125
- expert_down: bfloat16 [128, 512, 2048], P(('sp', 'dp')), may hold values from -0.25 to 0.25
- routes: int32 [8, 2048, 2], P('dp', 'sp'), may hold values from 0 to 127, all different within a row; in each aligned block of 128 rows (0 to 127, 128 to 255, ..., all dimensions but the last counted through in order) at most 4 rows name the same one
- route_weights: float32 [8, 2048, 2], P('dp', 'sp'), may hold values from 0.25 to 1.25
Outputs:
- layer_out: bfloat16 [8, 2048, 2048], P('dp', 'sp')
The draws below stay inside these ranges and needn't reach their ends.
Inputs may be any that keep to these rules, and one draw needn't show every extreme that they name: `routes`: each token names 2 different experts; among the rows of one device no expert is named more than 4 times, a bound that some block reaches.
All inputs are finite; a program needn't handle non-finite values.
Results may differ from the reference program's by a relative error of at most 0.015.
Values may be sent and summed in bfloat16 or wider, within the bound.
No kernel may reach another device: no remote copies, remote signals or barrier semaphores. Data moves between devices by JAX's collectives and lax.ppermute only.
A program may use at most 128 MiB of HBM per device.

```python
import math
import jax
import jax.numpy as jnp
import numpy as np
from jax import lax

D = 2048
HEADS = 32
HEAD_DIM = 64
GROUPS = 8
STATE = 128
CONV_K = 4
BLOCK = 128
EXPERT_FF = 512
SHARED_FF = 512
TOP_K = 2
TOK_DEV = 128
INNER = 2048
SEQS = 8
LENGTH = 2048
EXPERTS = 128
CAP = 4
N_SP = 16
N_DP = 8


def draw_decay_log(key, part):
    first, second, third = jax.random.split(key, 3)
    share = 0.5
    quick = jax.random.uniform(first, (HEADS,), jnp.float32) < share
    slow = jax.random.uniform(second, (HEADS,), jnp.float32, math.log(5e-05), math.log(0.0002))
    fast = jax.random.uniform(third, (HEADS,), jnp.float32, math.log(0.015), math.log(0.05))
    return jnp.where(quick, fast, slow).astype(jnp.float32)


def draw_step_input(key, part):
    first, second = jax.random.split(key)
    count = LENGTH // TOK_DEV
    offset = jax.random.uniform(second, (SEQS, count, 1, HEADS), jnp.float32, -1.2, 1.2)
    noise = jnp.clip(jax.random.normal(first, (SEQS, count, TOK_DEV, HEADS), jnp.float32) * 0.6, -3.5, 3.5)
    return (offset + noise).reshape(SEQS, LENGTH, HEADS).astype(jnp.bfloat16)


def shard_levels(own_key, shape, pieces, least, largest):
    factor_of = 1.0
    for dim, blocks in pieces:
        steps = jax.random.uniform(jax.random.fold_in(jax.random.fold_in(own_key, 6), dim), (blocks,), jnp.float32, least / len(pieces), largest / len(pieces))
        factor_of = factor_of * jnp.repeat(jnp.exp(steps), shape[dim] // blocks).reshape((-1,) + (1,) * (len(shape) - 1 - dim))
    return factor_of


def routed_block(stream_key, own, number, rows, count, top, limit, slope):
    sequence = jax.random.permutation(stream_key, count)
    crowded, ordinary = load_shares(count, rows * top, limit, slope, True), load_shares(count, rows * top, limit, slope, False)
    places = jnp.arange(count)

    def named(lengths, rotation):
        used = int((lengths > 0).sum())
        fixed = max(1, used // 4)
        shifted = fixed + (places - fixed + rotation * (used - fixed)) % max(1, count - fixed)
        return jnp.zeros((count,), jnp.int32).at[sequence[jnp.where(places < fixed, places, shifted)]].set(jnp.asarray(lengths, jnp.int32))

    lengths = jnp.where(number % 4 == 0, named(crowded, number // 4), named(ordinary, number - number // 4 - 1))
    mixed = jax.random.permutation(jax.random.fold_in(own, 3), count)
    donor, receiver = mixed[0:count // 2 * 2:2], mixed[1:count // 2 * 2:2]
    room = jnp.minimum(lengths[donor] - 1, limit - lengths[receiver]) // 2
    room = jnp.where((donor == sequence[0]) | (receiver == sequence[0]) | (lengths[receiver] == 0), 0, jnp.maximum(room, 0))
    shifted = jax.random.randint(jax.random.fold_in(own, 4), (count // 2,), 0, 1 << 20) % (room + 1)
    lengths = lengths.at[donor].add(-shifted).at[receiver].add(shifted)
    labels = jnp.searchsorted(jnp.cumsum(lengths), jnp.arange(rows * top), side="right").astype(jnp.int32)
    listing = labels.reshape(top, rows).T
    listing = listing[jax.random.permutation(jax.random.fold_in(own, 1), rows)]
    rotation = jax.random.randint(jax.random.fold_in(own, 2), (rows, 1), 0, top)
    return jnp.take_along_axis(listing, (jnp.arange(top)[None, :] + rotation) % top, axis=1)


def load_shares(count, total, reach, slope, full):
    loads = [(1 << 20) // math.isqrt(rank ** slope) + 1 for rank in range(1, count + 1)]
    largest = reach if full else min(reach, max(-(-total // count), total * loads[0] // sum(loads)))
    least = 1 if total - largest >= count - 1 else 0
    given, rest = [largest] + [least] * (count - 1), total - largest - least * (count - 1)
    while rest > 0:
        movable = [i for i in range(1, count) if given[i] < largest] or [i for i in range(1, count) if given[i] < reach]
        pool, budget = sum([loads[i] for i in movable]), rest
        for i in movable:
            extra = min(reach - given[i], max(1, budget * loads[i] // pool), rest)
            given[i] = given[i] + extra
            rest = rest - extra
    return np.array(given)


def scatter_about(own_key, extent, scale, bound, pieces=(), kind=jnp.bfloat16):
    values = scale * jax.random.normal(own_key, extent, jnp.float32)
    if pieces:
        values = values * shard_levels(own_key, extent, pieces, -0.22, 0.18)
    return jnp.clip(values, -bound, bound).astype(kind)


def setup_inputs(seed: int = 0) -> dict:
    keys = jax.random.split(jax.random.key(seed), 24)
    residual = scatter_about(keys[0], (SEQS, LENGTH, D), 1.0, 6.0, ((0, 8), (1, 16)))
    head_input = scatter_about(keys[1], (SEQS, LENGTH, INNER), 1.0, 6.0, ((0, 8), (1, 16)))
    gate_input = scatter_about(keys[2], (SEQS, LENGTH, INNER), 1.0, 6.0, ((0, 8), (1, 16)))
    b_input = scatter_about(keys[3], (SEQS, LENGTH, GROUPS * STATE), 1.0, 6.0, ((0, 8), (1, 16)))
    c_input = scatter_about(keys[4], (SEQS, LENGTH, GROUPS * STATE), 1.0, 6.0, ((0, 8), (1, 16)))
    step_input = draw_step_input(jax.random.fold_in(keys[23], 71), 0)
    conv_weight = scatter_about(keys[6], (CONV_K, INNER), 0.5, 3.0)
    conv_b_weight = scatter_about(keys[7], (CONV_K, GROUPS * STATE), 0.5, 3.0)
    conv_c_weight = scatter_about(keys[8], (CONV_K, GROUPS * STATE), 0.5, 3.0)
    step_bias = jnp.clip(jax.random.uniform(keys[9], (HEADS,), jnp.float32, -1.0, 1.0), -1.0, 1.0)
    decay_log = draw_decay_log(jax.random.fold_in(keys[23], 71), 0)
    skip = jnp.clip(jax.random.uniform(keys[11], (HEADS,), jnp.float32, 0.5, 1.5), 0.5, 1.5)
    norm_gain = jnp.clip(1.0 + 0.18 * jax.random.normal(keys[12], (INNER,), jnp.float32), 0.1, 1.9)
    out_weight = scatter_about(keys[13], (INNER, D), INNER ** -0.5, 0.125, ((0, 8),))
    ffn_gain = jnp.clip(1.0 + 0.18 * jax.random.normal(keys[14], (D,), jnp.float32), 0.1, 1.9)
    shared_gate = scatter_about(keys[15], (D, SHARED_FF), D ** -0.5, 0.125)
    shared_up = scatter_about(keys[16], (D, SHARED_FF), D ** -0.5, 0.125)
    shared_down = scatter_about(keys[17], (SHARED_FF, D), SHARED_FF ** -0.5, 0.25)
    expert_gate = scatter_about(keys[18], (EXPERTS, D, EXPERT_FF), D ** -0.5, 0.125, ((0, 128),))
    expert_up = scatter_about(keys[19], (EXPERTS, D, EXPERT_FF), D ** -0.5, 0.125, ((0, 128),))
    expert_down = scatter_about(keys[20], (EXPERTS, EXPERT_FF, D), EXPERT_FF ** -0.5, 0.25, ((0, 128),))
    routes_keys = jax.random.split(jax.random.fold_in(keys[21], 1), SEQS * LENGTH // TOK_DEV)
    routes_turns = jax.random.permutation(jax.random.fold_in(keys[21], 3), SEQS * LENGTH // TOK_DEV)
    routes = jax.vmap(lambda own, number: routed_block(jax.random.fold_in(keys[21], 2), own, number, TOK_DEV, EXPERTS, TOP_K, CAP, 2))(routes_keys, routes_turns).reshape((SEQS, LENGTH, TOP_K))
    route_weights = jnp.clip(0.25 + 1.0 * jax.random.uniform(keys[22], (SEQS, LENGTH, TOP_K), jnp.float32) ** shard_levels(keys[22], (SEQS, LENGTH, TOP_K), ((0, 8), (1, 16)), -0.2, 0.2), 0.25, 1.25)
    return {"residual": residual, "head_input": head_input, "gate_input": gate_input, "b_input": b_input, "c_input": c_input, "step_input": step_input, "conv_weight": conv_weight, "conv_b_weight": conv_b_weight, "conv_c_weight": conv_c_weight, "step_bias": step_bias, "decay_log": decay_log, "skip": skip, "norm_gain": norm_gain, "out_weight": out_weight, "ffn_gain": ffn_gain, "shared_gate": shared_gate, "shared_up": shared_up, "shared_down": shared_down, "expert_gate": expert_gate, "expert_up": expert_up, "expert_down": expert_down, "routes": routes, "route_weights": route_weights}


EPS = 1e-06
HIGH = lax.Precision.HIGHEST

def conv_silu(padded, weight, length):
    total = jnp.zeros((length, padded.shape[1]), jnp.float32)
    for tap in range(weight.shape[0]):
        total = total + padded[tap:tap + length].astype(jnp.float32) * weight[tap].astype(jnp.float32)
    return jax.nn.silu(total)

def block_scan(xs, step, rate, bmat, cmat, block, init):
    length, heads, width = xs.shape
    count = length // block
    logs = (step * rate[None, :]).reshape(count, block, heads)
    weighted = (xs * step[:, :, None]).reshape(count, block, heads, width)
    bb = bmat.reshape(count, block, heads, -1)
    cc = cmat.reshape(count, block, heads, -1)
    cum = jnp.cumsum(logs, axis=1)
    lower = jnp.tril(jnp.ones((block, block), dtype=bool))[None, :, :, None]
    diff = cum[:, :, None, :] - cum[:, None, :, :]
    decay = jnp.where(lower, jnp.exp(jnp.where(lower, diff, 0.0)), 0.0)
    scores = jnp.einsum('clhn,cshn->clsh', cc, bb, precision=HIGH) * decay
    inner = jnp.einsum('clsh,cshp->clhp', scores, weighted, precision=HIGH)
    to_end = jnp.exp(cum[:, -1:, :] - cum)
    states = jnp.einsum('cshn,cshp->chpn', bb * to_end[..., None], weighted, precision=HIGH)
    totals = jnp.exp(cum[:, -1, :])

    def advance(carry, item):
        fresh, factor = item
        return (carry * factor[:, None, None] + fresh, carry)
    last, before = lax.scan(advance, init, (states, totals))
    outer = jnp.einsum('clhn,chpn->clhp', cc * jnp.exp(cum)[..., None], before, precision=HIGH)
    return ((inner + outer).reshape(length, heads, width), last)

def reference(residual, head_input, gate_input, b_input, c_input, step_input, conv_weight, conv_b_weight, conv_c_weight, step_bias, decay_log, skip, norm_gain, out_weight, ffn_gain, shared_gate, shared_up, shared_down, expert_gate, expert_up, expert_down, routes, route_weights):
    taps = jnp.concatenate([conv_weight, conv_b_weight, conv_c_weight], axis=1)
    rate = -jnp.exp(decay_log)
    per_group = HEADS // GROUPS
    span = GROUPS * STATE

    def one_sequence(items):
        x_seq, b_seq, c_seq, s_seq, g_seq, r_seq = items
        rows = jnp.concatenate([x_seq, b_seq, c_seq], axis=1)
        act = conv_silu(jnp.pad(rows, ((CONV_K - 1, 0), (0, 0))), taps, LENGTH)
        xs = act[:, :INNER].reshape(LENGTH, HEADS, HEAD_DIM)
        bm = jnp.repeat(act[:, INNER:INNER + span].reshape(LENGTH, GROUPS, STATE), per_group, axis=1)
        cm = jnp.repeat(act[:, INNER + span:].reshape(LENGTH, GROUPS, STATE), per_group, axis=1)
        step = jax.nn.softplus(s_seq.astype(jnp.float32) + step_bias[None, :])
        y, _ = block_scan(xs, step, rate, bm, cm, BLOCK, jnp.zeros((HEADS, HEAD_DIM, STATE), jnp.float32))
        scanned = (y + skip[None, :, None] * xs).reshape(LENGTH, INNER).astype(jnp.bfloat16)
        gated = (scanned.astype(jnp.float32) * jax.nn.silu(g_seq.astype(jnp.float32))).reshape(LENGTH, GROUPS, INNER // GROUPS)
        gated = gated * lax.rsqrt(lax.optimization_barrier(jnp.mean(gated * gated, axis=2, keepdims=True)) + EPS)
        normed = (gated.reshape(LENGTH, INNER) * norm_gain[None, :]).astype(jnp.bfloat16)
        mixed = (r_seq.astype(jnp.float32) + jnp.dot(normed, out_weight, preferred_element_type=jnp.float32)).astype(jnp.bfloat16)
        mixed_f = mixed.astype(jnp.float32)
        expert_in = (mixed_f * lax.rsqrt(lax.optimization_barrier(jnp.mean(mixed_f * mixed_f, axis=1, keepdims=True)) + EPS) * ffn_gain[None, :]).astype(jnp.bfloat16)
        shared_hidden = (jax.nn.silu(jnp.dot(expert_in, shared_gate, preferred_element_type=jnp.float32)) * jnp.dot(expert_in, shared_up, preferred_element_type=jnp.float32)).astype(jnp.bfloat16)
        base = mixed_f + jnp.dot(shared_hidden, shared_down, preferred_element_type=jnp.float32)
        return (base, expert_in)
    base, expert_in = lax.map(one_sequence, (head_input, b_input, c_input, step_input, gate_input, residual))
    rows_all = SEQS * LENGTH
    flat_in = expert_in.reshape(rows_all, D)
    chosen = routes.reshape(-1).astype(jnp.int32)
    pairs = chosen.shape[0]
    onehot = (chosen[:, None] == jnp.arange(EXPERTS, dtype=jnp.int32)[None, :]).astype(jnp.int32)
    rank = lax.optimization_barrier(jnp.sum((jnp.cumsum(onehot, axis=0) - onehot) * onehot, axis=1)).astype(jnp.int32)
    room = N_SP * N_DP * CAP
    table = jnp.full((EXPERTS, room), pairs, jnp.int32).at[chosen, rank].set(jnp.arange(pairs, dtype=jnp.int32))

    def serve(carry, item):
        index, gate_w, up_w, down_w = item
        rows = jnp.take(flat_in, jnp.minimum(index, pairs - 1) // TOP_K, axis=0)
        hidden = (jax.nn.silu(jnp.dot(rows, gate_w, preferred_element_type=jnp.float32)) * jnp.dot(rows, up_w, preferred_element_type=jnp.float32)).astype(jnp.bfloat16)
        done = jnp.dot(hidden, down_w, preferred_element_type=jnp.float32).astype(jnp.bfloat16)
        return (carry.at[index].set(done, mode='drop'), None)
    pair_out, _ = lax.scan(serve, jnp.zeros((pairs, D), jnp.bfloat16), (table, expert_gate, expert_up, expert_down))
    routed = lax.optimization_barrier(jnp.sum(pair_out.reshape(rows_all, TOP_K, D).astype(jnp.float32) * route_weights.reshape(rows_all, TOP_K, 1), axis=1))
    return (base.reshape(rows_all, D) + routed).astype(jnp.bfloat16).reshape(SEQS, LENGTH, D)
```

```python
import jax
import jax.numpy as jnp
from jax import lax
from jax.experimental import pallas as pl
from jax.experimental.pallas import tpu as pltpu
from jax.sharding import PartitionSpec as P

D = 2048
HEADS = 32
HEAD_DIM = 64
GROUPS = 8
STATE = 128
TOK = 128
EPS = 1e-06
BF = jnp.bfloat16
F32 = jnp.float32
PER = HEADS // GROUPS
GW = PER * HEAD_DIM
HALF = D // 2
ROWS = 1024
ST_ROWS = 144


def full():
    return pl.BlockSpec(memory_space=pltpu.VMEM)


def smem():
    return pl.BlockSpec(memory_space=pltpu.SMEM)


def call(kernel, outs, n_in, name, scratch=(), smem_in=(), flops=10**6, nbytes=10**6):
    return pl.pallas_call(
        kernel,
        out_shape=tuple(jax.ShapeDtypeStruct(s, d) for s, d in outs),
        in_specs=[smem() if i in smem_in else full() for i in range(n_in)],
        out_specs=tuple(full() for _ in outs),
        scratch_shapes=list(scratch),
        name=name,
        cost_estimate=pl.CostEstimate(flops=flops, bytes_accessed=nbytes, transcendentals=0),
    )


def silu(v):
    return v / (1.0 + jnp.exp(-v))


def tap(pad, halo, rows, weight):
    pad[0:8, :] = halo.astype(F32)
    pad[8 : 8 + TOK, :] = rows.astype(F32)
    w = weight.astype(F32)
    total = pad[5 : 5 + TOK, :] * w[0:1, :]
    for k in range(1, 4):
        total = total + pad[5 + k : 5 + k + TOK, :] * w[k : k + 1, :]
    return silu(total)


def spread(cols, g):
    lane = lax.broadcasted_iota(jnp.int32, (TOK, 128), 1)
    out = []
    for i in range(0, PER, 2):
        h = g * PER + i
        out.append(jnp.where(lane < HEAD_DIM, cols[:, h : h + 1], cols[:, h + 1 : h + 2]))
    return jnp.concatenate(out, axis=1)


def states_kernel(
    x, b, hx, hb, step_in, cw, cbw, bias, dlog, st, v_out, xs_out, b_out, ec_out, padx, padb
):
    s = step_in[...].astype(F32) + bias[...]
    step = jnp.maximum(s, 0.0) + jnp.log(1.0 + jnp.exp(-jnp.abs(s)))
    logs = step * (-jnp.exp(dlog[...]))
    r = lax.broadcasted_iota(jnp.int32, (TOK, TOK), 0)
    c = lax.broadcasted_iota(jnp.int32, (TOK, TOK), 1)
    tri = (c <= r).astype(F32)
    cum = jnp.dot(tri, logs, precision=lax.Precision.HIGHEST, preferred_element_type=F32)
    ec_out[...] = jnp.exp(cum)
    grow = step * jnp.exp(-cum)
    tot = cum[TOK - 1 : TOK, :]
    etot = jnp.exp(tot)
    sub = lax.broadcasted_iota(jnp.int32, (16, 128), 0)
    for g in range(GROUPS):
        xc = slice(g * GW, (g + 1) * GW)
        bc = slice(g * STATE, (g + 1) * STATE)
        xs = tap(padx.at[g % 2], hx[:, xc], x[:, xc], cw[:, xc])
        bm = tap(padb.at[g % 2], hb[:, bc], b[:, bc], cbw[:, bc]).astype(BF)
        v = (xs * spread(grow, g)).astype(BF)
        xs_out[:, xc] = xs
        v_out[:, xc] = v
        b_out[:, bc] = bm
        fresh = lax.dot_general(v, bm, (((0,), (0,)), ((), ())), preferred_element_type=F32)
        for i in range(2):
            h = g * PER + 2 * i
            o = g * 2 + i
            for j in range(2):
                k = (2 * i + j) * HEAD_DIM
                st[o, j * HEAD_DIM : (j + 1) * HEAD_DIM, :] = (
                    fresh[k : k + HEAD_DIM, :] * etot[0:1, h + j : h + j + 1]
                ).astype(BF)
            tail = jnp.zeros((16, 128), F32)
            for j in range(2):
                rest = jnp.broadcast_to(tot[0:1, h + j : h + j + 1], (16, 128))
                for q in range(3):
                    part = rest.astype(BF).astype(F32)
                    tail = jnp.where(sub == 3 * j + q, part, tail)
                    rest = rest - part
            st[o, 2 * HEAD_DIM : ST_ROWS, :] = tail.astype(BF)


def inner_kernel(c, hc, ccw, v, bm, xs, ec, skip, a_out, c_out, padc):
    r = lax.broadcasted_iota(jnp.int32, (TOK, TOK), 0)
    s = lax.broadcasted_iota(jnp.int32, (TOK, TOK), 1)
    lower = s <= r
    cols = ec[...]
    sk = jnp.broadcast_to(skip[...], (TOK, HEADS))
    for g in range(GROUPS):
        xc = slice(g * GW, (g + 1) * GW)
        bc = slice(g * STATE, (g + 1) * STATE)
        cm = tap(padc.at[g % 2], hc[:, bc], c[:, bc], ccw[:, bc]).astype(BF)
        c_out[:, bc] = cm
        cb = lax.dot_general(cm, bm[:, bc], (((1,), (1,)), ((), ())), preferred_element_type=F32)
        cb = jnp.where(lower, cb, 0.0).astype(BF)
        u = jnp.dot(cb, v[:, xc], preferred_element_type=F32)
        a_out[:, xc] = u * spread(cols, g) + xs[:, xc] * spread(sk, g)


def carry_kernel(got, out):
    row = lax.broadcasted_iota(jnp.int32, (2 * HEAD_DIM, 128), 0)
    carry = jnp.zeros((2 * HEAD_DIM, 128), F32)
    count = got.shape[0]
    for i in range(count):
        out[i] = carry.astype(BF)
        if i + 1 < count:
            tail = got[i, 2 * HEAD_DIM : ST_ROWS, :].astype(F32)
            fa = jnp.exp(tail[0:1] + tail[1:2] + tail[2:3])
            fb = jnp.exp(tail[3:4] + tail[4:5] + tail[5:6])
            factor = jnp.where(row < HEAD_DIM, fa, fb)
            carry = carry * factor + got[i, 0 : 2 * HEAD_DIM, :].astype(F32)


def routes_kernel(routes, rw, d_out, hi_out, lo_out):
    e = lax.broadcasted_iota(jnp.int32, (TOK, 128), 1)
    r = lax.broadcasted_iota(jnp.int32, (TOK, TOK), 0)
    s = lax.broadcasted_iota(jnp.int32, (TOK, TOK), 1)
    tri = (s < r).astype(BF)
    ids = routes[...]
    hot = [(ids[:, k : k + 1] == e).astype(F32) for k in range(2)]
    before0 = jnp.dot(tri, hot[0].astype(BF), preferred_element_type=F32)
    before1 = jnp.dot(tri, hot[1].astype(BF), preferred_element_type=F32)
    before1 = before1 + jnp.sum(hot[0], axis=0, keepdims=True)
    pos = [
        jnp.sum(before0 * hot[0], axis=1, keepdims=True).astype(jnp.int32),
        jnp.sum(before1 * hot[1], axis=1, keepdims=True).astype(jnp.int32),
    ]
    lane = lax.broadcasted_iota(jnp.int32, (TOK, ROWS), 1)
    w = rw[...]
    for h in range(2):
        mask = [lane == ids[:, k : k + 1] * 8 + pos[k] + 4 * h for k in range(2)]
        disp = jnp.where(mask[0] | mask[1], 1.0, 0.0)
        d_out[:, h * TOK : (h + 1) * TOK] = disp.T.astype(BF)
        comb = jnp.where(mask[0], w[:, 0:1], 0.0) + jnp.where(mask[1], w[:, 1:2], 0.0)
        hi = comb.astype(BF)
        hi_out[h * TOK : (h + 1) * TOK, :] = hi
        lo_out[h * TOK : (h + 1) * TOK, :] = (comb - hi.astype(F32)).astype(BF)


def mix_kernel(
    place, a, cm, ec, pref, gate, gain, resid, fgain, disp,
    w0, w1, w2, w3, w4, w5, w6, w7, mixed_out, ein_out, send, norm
):
    cols = ec[...]
    for g in range(GROUPS):
        xc = slice(g * GW, (g + 1) * GW)
        bc = slice(g * STATE, (g + 1) * STATE)
        outer = lax.dot_general(
            cm[:, bc], pref[g], (((1,), (1,)), ((), ())), preferred_element_type=F32
        )
        y = (a[:, xc] + outer * spread(cols, g)).astype(BF).astype(F32)
        y = y * silu(gate[:, xc].astype(F32))
        y = y * lax.rsqrt(jnp.mean(y * y, axis=1, keepdims=True) + EPS)
        norm[g] = (y * gain[:, xc]).astype(BF)
    proj = resid[...].astype(F32)
    for k, w in enumerate((w0, w1, w2, w3, w4, w5, w6, w7)):
        proj = proj + jnp.dot(norm[place[k]], w[...], preferred_element_type=F32)
    mixed = proj.astype(BF)
    mixed_out[...] = mixed
    m = mixed.astype(F32)
    ein = (m * lax.rsqrt(jnp.mean(m * m, axis=1, keepdims=True) + EPS) * fgain[...]).astype(BF)
    ein_out[...] = ein
    stack = jnp.concatenate([ein[:, :HALF], ein[:, HALF:]], axis=0)
    send[...] = jnp.dot(disp[...], stack, preferred_element_type=F32).astype(BF)


def shared_kernel(ein, mixed, sg, su, sd, out):
    x = ein[...]
    gate = jnp.dot(x, sg[...], preferred_element_type=F32)
    up = jnp.dot(x, su[...], preferred_element_type=F32)
    hidden = (silu(gate) * up).astype(BF)
    out[...] = mixed[...].astype(F32) + jnp.dot(hidden, sd[...], preferred_element_type=F32)


def expert_kernel(got, wg, wu, wd, out, xbuf):
    n = 256
    sub = lax.broadcasted_iota(jnp.int32, (ROWS // 16, 8, n), 1)
    for q in range(HALF // n):
        t = got[:, q * n : (q + 1) * n].astype(F32).reshape(ROWS // 16, 2, 8, n)
        r0, r1 = t[:, 0], t[:, 1]
        x0 = jnp.where(sub < 4, r0, pltpu.roll(r1, 4, 1))
        x1 = jnp.where(sub < 4, pltpu.roll(r0, 4, 1), r1)
        xbuf[:, q * n : (q + 1) * n] = x0.reshape(ROWS // 2, n).astype(BF)
        xbuf[:, HALF + q * n : HALF + (q + 1) * n] = x1.reshape(ROWS // 2, n).astype(BF)
    x = xbuf[...]
    gate = jnp.dot(x, wg[...], preferred_element_type=F32)
    up = jnp.dot(x, wu[...], preferred_element_type=F32)
    hidden = (silu(gate) * up).astype(BF)
    for q in range(HALF // n):
        y0 = jnp.dot(hidden, wd[:, q * n : (q + 1) * n], preferred_element_type=F32)
        y1 = jnp.dot(hidden, wd[:, HALF + q * n : HALF + (q + 1) * n], preferred_element_type=F32)
        y0 = y0.reshape(ROWS // 16, 8, n)
        y1 = y1.reshape(ROWS // 16, 8, n)
        o0 = jnp.where(sub < 4, y0, pltpu.roll(y1, 4, 1))
        o1 = jnp.where(sub < 4, pltpu.roll(y0, 4, 1), y1)
        out[:, q * n : (q + 1) * n] = jnp.stack([o0, o1], axis=1).reshape(ROWS, n).astype(BF)


def combine_kernel(got, hi, lo, base, out):
    g = got[...]
    y = jnp.dot(hi[...], g, preferred_element_type=F32) + jnp.dot(
        lo[...], g, preferred_element_type=F32
    )
    out[:, :HALF] = (base[:, :HALF] + y[:TOK]).astype(BF)
    out[:, HALF:] = (base[:, HALF:] + y[TOK:]).astype(BF)


def body(
    residual,
    head_input,
    gate_input,
    b_input,
    c_input,
    step_input,
    conv_weight,
    conv_b_weight,
    conv_c_weight,
    step_bias,
    decay_log,
    skip,
    norm_gain,
    out_weight,
    ffn_gain,
    shared_gate,
    shared_up,
    shared_down,
    expert_gate,
    expert_up,
    expert_down,
    routes,
    route_weights,
):
    ways = lax.axis_size("sp")
    dps = lax.axis_size("dp")
    x, b, c = head_input[0], b_input[0], c_input[0]
    ends = jnp.concatenate([x[TOK - 8 :], b[TOK - 8 :], c[TOK - 8 :]], axis=1)
    halo = lax.ppermute(ends, "sp", [(i, i + 1) for i in range(ways - 1)])

    def along(v, k):
        return lax.ppermute(v, "dp", [(i, (i + k) % dps) for i in range(dps)])

    def swap(v):
        return lax.ppermute(v, "dp", [(i, i ^ 1) for i in range(dps)])

    own = [out_weight, along(out_weight, 2), along(out_weight, -2), along(out_weight, 4)]
    pieces = own + [swap(v) for v in own]
    me = lax.axis_index("dp")
    mine = [me, (me + dps - 2) % dps, (me + 2) % dps, (me + 4) % dps]
    place = jnp.stack(mine + [v ^ 1 for v in mine]).astype(jnp.int32)

    st, v, xs, bm, ec = call(
        states_kernel,
        [((ways, ST_ROWS, 128), BF), ((TOK, D), BF), ((TOK, D), F32), ((TOK, 1024), BF), ((TOK, HEADS), F32)],
        9,
        "states",
        scratch=[pltpu.VMEM((2, TOK + 8, GW), F32), pltpu.VMEM((2, TOK + 8, STATE), F32)],
    )(
        x, b, halo[:, :D], halo[:, D : D + 1024], step_input[0], conv_weight, conv_b_weight,
        step_bias[None], decay_log[None],
    )
    got = lax.all_to_all(st, "sp", split_axis=0, concat_axis=0, tiled=True)
    a, cm = call(
        inner_kernel,
        [((TOK, D), F32), ((TOK, 1024), BF)],
        8,
        "inner",
        scratch=[pltpu.VMEM((2, TOK + 8, STATE), F32)],
        flops=4 * 10**9,
    )(c, halo[:, D + 1024 :], conv_c_weight, v, bm, xs, ec, skip[None])
    disp, hi, lo = call(
        routes_kernel,
        [((ROWS, 2 * TOK), BF), ((2 * TOK, ROWS), BF), ((2 * TOK, ROWS), BF)],
        2,
        "routing",
        flops=2 * 10**9,
    )(routes[0], route_weights[0])
    (carried,) = call(carry_kernel, [((ways, 128, 128), BF)], 1, "carry")(got)
    pref = lax.all_to_all(carried, "sp", split_axis=0, concat_axis=0, tiled=True)
    mixed, ein, send = call(
        mix_kernel,
        [((TOK, D), BF), ((TOK, D), BF), ((ROWS, HALF), BF)],
        18,
        "mix",
        scratch=[pltpu.VMEM((GROUPS, TOK, GW), BF)],
        smem_in=(0,),
        flops=2 * 10**9,
    )(
        place, a, cm, ec, pref.reshape(GROUPS, GW, STATE), gate_input[0], norm_gain[None],
        residual[0], ffn_gain[None], disp, *pieces,
    )
    experts = ways * dps
    arrived = lax.all_to_all(
        send.reshape(experts, 8, HALF), ("sp", "dp"), split_axis=0, concat_axis=0, tiled=True
    )
    (base,) = call(shared_kernel, [((TOK, D), F32)], 5, "shared", flops=4 * 10**9)(
        ein, mixed, shared_gate, shared_up, shared_down
    )
    (done,) = call(
        expert_kernel,
        [((ROWS, HALF), BF)],
        4,
        "expert",
        scratch=[pltpu.VMEM((ROWS // 2, D), BF)],
        flops=3 * 10**9,
    )(arrived.reshape(ROWS, HALF), expert_gate[0], expert_up[0], expert_down[0])
    back = lax.all_to_all(
        done.reshape(experts, 8, HALF), ("sp", "dp"), split_axis=0, concat_axis=0, tiled=True
    )
    (out,) = call(combine_kernel, [((TOK, D), BF)], 4, "combine")(
        back.reshape(ROWS, HALF), hi, lo, base
    )
    return out[None]


def solution(mesh):
    rows = P("dp", "sp", None)
    one = P(("sp", "dp"), None, None)
    return jax.shard_map(
        body,
        mesh=mesh,
        in_specs=(
            (rows,) * 6 + (P(),) * 7 + (P("dp", None),) + (P(),) * 4 + (one,) * 3 + (rows, rows)
        ),
        out_specs=rows,
        check_vma=False,
    )
```

```python
import jax
import jax.numpy as jnp
from jax import lax
from jax._src.core import MemorySpace
from jax._src.state.primitives import with_memory_space_constraint
from jax.experimental import pallas as pl
from jax.experimental.pallas import tpu as pltpu
from jax.sharding import PartitionSpec as P


D = 2048
HEADS = 32
HEAD_DIM = 64
GROUPS = 8
STATE = 128
TOK = 128
EPS = 1e-06
BF = jnp.bfloat16
F32 = jnp.float32
PER = HEADS // GROUPS
GW = PER * HEAD_DIM
HALF = D // 2
ROWS = 1024
ST_ROWS = 144


def full():
    return pl.BlockSpec(memory_space=pltpu.VMEM)


def smem():
    return pl.BlockSpec(memory_space=pltpu.SMEM)


def anywhere():
    return pl.BlockSpec(memory_space=pl.ANY)


def call(
    kernel, outs, args, scratch=(), vmem=(), smem_in=(), raw=(), out_vmem=(), limit=12, flops=10**6
):
    placed = [
        v
        if i in smem_in
        else pltpu.with_memory_space_constraint(v, pltpu.VMEM if i in vmem else pltpu.HBM)
        for i, v in enumerate(args)
    ]
    return pl.pallas_call(
        kernel,
        out_shape=tuple(
            pltpu.VMEM(s, d) if i in out_vmem else pltpu.HBM(s, d)
            for i, (s, d) in enumerate(outs)
        ),
        in_specs=[
            smem() if i in smem_in else anywhere() if i in raw else full() for i in range(len(args))
        ],
        out_specs=tuple(full() for _ in outs),
        scratch_shapes=list(scratch),
        compiler_params=pltpu.CompilerParams(vmem_limit_bytes=limit << 20),
        cost_estimate=pl.CostEstimate(flops=flops, bytes_accessed=10**6, transcendentals=0),
    )(*placed)


def silu(v):
    return v / (1.0 + jnp.exp(-v))


def tap(pad, halo, rows, weight):
    pad[0:8, :] = halo.astype(F32)
    pad[8 : 8 + TOK, :] = rows.astype(F32)
    w = weight.astype(F32)
    total = pad[5 : 5 + TOK, :] * w[0:1, :]
    for k in range(1, 4):
        total = total + pad[5 + k : 5 + k + TOK, :] * w[k : k + 1, :]
    return silu(total)


def spread(cols, g):
    lane = lax.broadcasted_iota(jnp.int32, (TOK, 128), 1)
    out = []
    for i in range(0, PER, 2):
        h = g * PER + i
        out.append(jnp.where(lane < HEAD_DIM, cols[:, h : h + 1], cols[:, h + 1 : h + 2]))
    return jnp.concatenate(out, axis=1)


def states_kernel(
    x, b, halo, step_in, cw, cbw, bias, dlog, st, v_out, xs_out, b_out, ec_out, padx, padb
):
    s = step_in[...].astype(F32).T + bias[...]
    step = jnp.maximum(s, 0.0) + jnp.log(1.0 + jnp.exp(-jnp.abs(s)))
    logs = step * (-jnp.exp(dlog[...]))
    r = lax.broadcasted_iota(jnp.int32, (TOK, TOK), 0)
    c = lax.broadcasted_iota(jnp.int32, (TOK, TOK), 1)
    tri = (c <= r).astype(F32)
    cum = jnp.dot(tri, logs, precision=lax.Precision.HIGHEST, preferred_element_type=F32)
    ec_out[...] = jnp.exp(cum)
    grow = step * jnp.exp(-cum)
    tot = cum[TOK - 1 : TOK, :]
    etot = jnp.exp(tot)
    sub = lax.broadcasted_iota(jnp.int32, (16, 128), 0)
    for g in range(GROUPS):
        xc = slice(g * GW, (g + 1) * GW)
        bc = slice(g * STATE, (g + 1) * STATE)
        xs = tap(padx.at[g % 2], halo[:, xc], x[:, xc], cw[:, xc])
        bm = tap(padb.at[g % 2], halo[:, D + g * STATE : D + (g + 1) * STATE], b[:, bc], cbw[:, bc]).astype(BF)
        v = (xs * spread(grow, g)).astype(BF)
        xs_out[:, xc] = xs
        v_out[:, xc] = v
        b_out[:, bc] = bm
        fresh = lax.dot_general(v, bm, (((0,), (0,)), ((), ())), preferred_element_type=F32)
        for i in range(2):
            h = g * PER + 2 * i
            o = g * 2 + i
            for j in range(2):
                k = (2 * i + j) * HEAD_DIM
                st[o, j * HEAD_DIM : (j + 1) * HEAD_DIM, :] = (
                    fresh[k : k + HEAD_DIM, :] * etot[0:1, h + j : h + j + 1]
                ).astype(BF)
            tail = jnp.zeros((16, 128), F32)
            for j in range(2):
                rest = jnp.broadcast_to(tot[0:1, h + j : h + j + 1], (16, 128))
                for q in range(3):
                    part = rest.astype(BF).astype(F32)
                    tail = jnp.where(sub == 3 * j + q, part, tail)
                    rest = rest - part
            st[o, 2 * HEAD_DIM : ST_ROWS, :] = tail.astype(BF)


def inner_kernel(c, halo, ccw, v, bm, xs, ec, skip, a_out, c_out, padc):
    r = lax.broadcasted_iota(jnp.int32, (TOK, TOK), 0)
    s = lax.broadcasted_iota(jnp.int32, (TOK, TOK), 1)
    lower = s <= r
    cols = ec[...]
    sk = jnp.broadcast_to(skip[...], (TOK, HEADS))
    for g in range(GROUPS):
        xc = slice(g * GW, (g + 1) * GW)
        bc = slice(g * STATE, (g + 1) * STATE)
        cm = tap(padc.at[g % 2], halo[:, D + 1024 + g * STATE : D + 1024 + (g + 1) * STATE], c[:, bc], ccw[:, bc]).astype(BF)
        c_out[:, bc] = cm
        cb = lax.dot_general(cm, bm[:, bc], (((1,), (1,)), ((), ())), preferred_element_type=F32)
        cb = jnp.where(lower, cb, 0.0).astype(BF)
        u = jnp.dot(cb, v[:, xc], preferred_element_type=F32)
        a_out[:, xc] = u * spread(cols, g) + xs[:, xc] * spread(sk, g)


def carry_kernel(got, out):
    row = lax.broadcasted_iota(jnp.int32, (2 * HEAD_DIM, 128), 0)
    carry = jnp.zeros((2 * HEAD_DIM, 128), F32)
    count = got.shape[0]
    for i in range(count):
        out[i] = carry.astype(BF)
        if i + 1 < count:
            tail = got[i, 2 * HEAD_DIM : ST_ROWS, :].astype(F32)
            fa = jnp.exp(tail[0:1] + tail[1:2] + tail[2:3])
            fb = jnp.exp(tail[3:4] + tail[4:5] + tail[5:6])
            factor = jnp.where(row < HEAD_DIM, fa, fb)
            carry = carry * factor + got[i, 0 : 2 * HEAD_DIM, :].astype(F32)


def routes_kernel(routes, rw, d_out, hi_out, lo_out):
    e = lax.broadcasted_iota(jnp.int32, (TOK, 128), 1)
    r = lax.broadcasted_iota(jnp.int32, (TOK, TOK), 0)
    s = lax.broadcasted_iota(jnp.int32, (TOK, TOK), 1)
    tri = (s < r).astype(BF)
    both = jnp.concatenate([routes[...].astype(F32), rw[...], jnp.zeros((4, TOK), F32)], axis=0).T
    ids = both[:, 0:2].astype(jnp.int32)
    w = both[:, 2:4]
    hot = [(ids[:, k : k + 1] == e).astype(F32) for k in range(2)]
    before0 = jnp.dot(tri, hot[0].astype(BF), preferred_element_type=F32)
    before1 = jnp.dot(tri, hot[1].astype(BF), preferred_element_type=F32)
    before1 = before1 + jnp.sum(hot[0], axis=0, keepdims=True)
    pos = [
        jnp.sum(before0 * hot[0], axis=1, keepdims=True).astype(jnp.int32),
        jnp.sum(before1 * hot[1], axis=1, keepdims=True).astype(jnp.int32),
    ]
    lane = lax.broadcasted_iota(jnp.int32, (TOK, ROWS), 1)
    for h in range(2):
        mask = [lane == ids[:, k : k + 1] * 8 + pos[k] + 4 * h for k in range(2)]
        disp = jnp.where(mask[0] | mask[1], 1.0, 0.0)
        d_out[:, h * TOK : (h + 1) * TOK] = disp.T.astype(BF)
        comb = jnp.where(mask[0], w[:, 0:1], 0.0) + jnp.where(mask[1], w[:, 1:2], 0.0)
        hi = comb.astype(BF)
        hi_out[h * TOK : (h + 1) * TOK, :] = hi
        lo_out[h * TOK : (h + 1) * TOK, :] = (comb - hi.astype(F32)).astype(BF)


def mix_kernel(
    place, a, cm, ec, pref, gate, gain, resid, fgain, disp,
    w0, w1, w2, w3, w4, w5, w6, w7, w8, w9, mixed_out, ein_out, send, norm,
    wide, half, sems
):
    loads = []
    for k, w in enumerate((w0, w1, w2, w5, w6, w7)):
        loads.append(pltpu.make_async_copy(w, wide.at[k], sems.at[k]))
    for k, w in enumerate((w3, w4, w8, w9)):
        loads.append(pltpu.make_async_copy(w, half.at[k], sems.at[6 + k]))
    for load in loads:
        load.start()
    cols = ec[...]
    for g in range(GROUPS):
        xc = slice(g * GW, (g + 1) * GW)
        bc = slice(g * STATE, (g + 1) * STATE)
        outer = lax.dot_general(
            cm[:, bc], pref[g], (((1,), (1,)), ((), ())), preferred_element_type=F32
        )
        y = (a[:, xc] + outer * spread(cols, g)).astype(BF).astype(F32)
        y = y * silu(gate[:, xc].astype(F32))
        y = y * lax.rsqrt(jnp.mean(y * y, axis=1, keepdims=True) + EPS)
        norm[g] = (y * gain[:, xc]).astype(BF)
    proj = resid[...].astype(F32)
    for k in range(6):
        loads[k].wait()
        proj = proj + jnp.dot(norm[place[k]], wide[k], preferred_element_type=F32)
    for k in range(4):
        loads[6 + k].wait()
        row = norm[place[6 + k // 2]][:, (k % 2) * 128 : (k % 2) * 128 + 128]
        proj = proj + jnp.dot(row, half[k], preferred_element_type=F32)
    mixed = proj.astype(BF)
    mixed_out[...] = mixed
    m = mixed.astype(F32)
    ein = (m * lax.rsqrt(jnp.mean(m * m, axis=1, keepdims=True) + EPS) * fgain[...]).astype(BF)
    ein_out[...] = ein
    stack = jnp.concatenate([ein[:, :HALF], ein[:, HALF:]], axis=0)
    send[...] = jnp.dot(disp[...], stack, preferred_element_type=F32).astype(BF)


def shared_kernel(ein, mixed, sg, su, sd, out):
    x = ein[...]
    gate = jnp.dot(x, sg[...], preferred_element_type=F32)
    up = jnp.dot(x, su[...], preferred_element_type=F32)
    hidden = (silu(gate) * up).astype(BF)
    out[...] = mixed[...].astype(F32) + jnp.dot(hidden, sd[...], preferred_element_type=F32)


def expert_kernel(got, wg_in, wu_in, wd_in, out, xbuf, wg, wu, wd, sems):
    pairs = ((wg_in, wg), (wu_in, wu), (wd_in, wd))
    loads = [pltpu.make_async_copy(v, w, sems.at[k]) for k, (v, w) in enumerate(pairs)]
    for load in loads:
        load.start()
    n = 256
    sub = lax.broadcasted_iota(jnp.int32, (ROWS // 16, 8, n), 1)
    for q in range(HALF // n):
        t = got[:, q * n : (q + 1) * n].astype(F32).reshape(ROWS // 16, 2, 8, n)
        r0, r1 = t[:, 0], t[:, 1]
        x0 = jnp.where(sub < 4, r0, pltpu.roll(r1, 4, 1))
        x1 = jnp.where(sub < 4, pltpu.roll(r0, 4, 1), r1)
        xbuf[:, q * n : (q + 1) * n] = x0.reshape(ROWS // 2, n).astype(BF)
        xbuf[:, HALF + q * n : HALF + (q + 1) * n] = x1.reshape(ROWS // 2, n).astype(BF)
    x = xbuf[...]
    loads[0].wait()
    gate = jnp.dot(x, wg[...], preferred_element_type=F32)
    loads[1].wait()
    up = jnp.dot(x, wu[...], preferred_element_type=F32)
    hidden = (silu(gate) * up).astype(BF)
    loads[2].wait()
    for q in range(HALF // n):
        y0 = jnp.dot(hidden, wd[:, q * n : (q + 1) * n], preferred_element_type=F32)
        y1 = jnp.dot(hidden, wd[:, HALF + q * n : HALF + (q + 1) * n], preferred_element_type=F32)
        y0 = y0.reshape(ROWS // 16, 8, n)
        y1 = y1.reshape(ROWS // 16, 8, n)
        o0 = jnp.where(sub < 4, y0, pltpu.roll(y1, 4, 1))
        o1 = jnp.where(sub < 4, pltpu.roll(y0, 4, 1), y1)
        out[:, q * n : (q + 1) * n] = jnp.stack([o0, o1], axis=1).reshape(ROWS, n).astype(BF)


def combine_kernel(got, hi, lo, base, out):
    g = got[...]
    y = jnp.dot(hi[...], g, preferred_element_type=F32) + jnp.dot(
        lo[...], g, preferred_element_type=F32
    )
    out[:, :HALF] = (base[:, :HALF] + y[:TOK]).astype(BF)
    out[:, HALF:] = (base[:, HALF:] + y[TOK:]).astype(BF)


def plain(v):
    return with_memory_space_constraint(v, MemorySpace.Device)


def exchange(v, axis):
    return lax.all_to_all(plain(v), axis, split_axis=0, concat_axis=0, tiled=True)


def layer(
    residual, head_input, gate_input, b_input, c_input, step_input, conv_weight,
    conv_b_weight, conv_c_weight, step_bias, decay_log, skip, norm_gain, out_weight,
    ffn_gain, shared_gate, shared_up, shared_down, expert_gate, expert_up, expert_down,
    routes, route_weights,
):
    ways = lax.axis_size("sp")
    dps = lax.axis_size("dp")
    experts = ways * dps
    x, b, c = head_input[0], b_input[0], c_input[0]
    ends = jnp.concatenate([x[TOK - 8 :], b[TOK - 8 :], c[TOK - 8 :]], axis=1)
    halo = lax.ppermute(ends, "sp", [(i, i + 1) for i in range(ways - 1)])

    def along(v, k):
        return lax.ppermute(v, "dp", [(i, (i + k) % dps) for i in range(dps)])

    def swap(v):
        return lax.ppermute(v, "dp", [(i, i ^ 1) for i in range(dps)])

    left = along(out_weight, 2)
    right = along(out_weight, -2)
    far = [along(left[:128], 2), along(right[128:], -2)]
    pieces = [out_weight, left, right, *far, swap(out_weight), swap(left)]
    pieces += [swap(right), swap(far[0]), swap(far[1])]
    me = lax.axis_index("dp")
    near = [me, (me + dps - 2) % dps, (me + 2) % dps]
    far_at = (me + 4) % dps
    place = jnp.stack(near + [v ^ 1 for v in near] + [far_at, far_at ^ 1]).astype(jnp.int32)

    st, v, xs, bm, ec = call(
        states_kernel,
        [((ways, ST_ROWS, 128), BF), ((TOK, D), BF), ((TOK, D), F32), ((TOK, 1024), BF), ((TOK, HEADS), F32)],
        (x, b, halo, step_input[0].T, conv_weight, conv_b_weight, step_bias[None], decay_log[None]),
        vmem=(2,),
        scratch=[pltpu.VMEM((2, TOK + 8, GW), F32), pltpu.VMEM((2, TOK + 8, STATE), F32)],
    )
    got = exchange(st, "sp")
    a, cm = call(
        inner_kernel,
        [((TOK, D), F32), ((TOK, 1024), BF)],
        (c, halo, conv_c_weight, v, bm, xs, ec, skip[None]),
        scratch=[pltpu.VMEM((2, TOK + 8, STATE), F32)],
        flops=4 * 10**9,
    )
    disp, hi, lo = call(
        routes_kernel,
        [((ROWS, 2 * TOK), BF), ((2 * TOK, ROWS), BF), ((2 * TOK, ROWS), BF)],
        (routes[0].T, route_weights[0].T),
        flops=2 * 10**9,
    )
    (carried,) = call(carry_kernel, [((ways, 128, 128), BF)], (got,), vmem=(0,))
    pref = exchange(carried, "sp")
    mixed, ein, send = call(
        mix_kernel,
        [((TOK, D), BF), ((TOK, D), BF), ((ROWS, HALF), BF)],
        (
            place, a, cm, ec, pref.reshape(GROUPS, GW, STATE), gate_input[0], norm_gain[None],
            residual[0], ffn_gain[None], disp, *pieces,
        ),
        scratch=[
            pltpu.VMEM((GROUPS, TOK, GW), BF),
            pltpu.VMEM((6, 256, D), BF),
            pltpu.VMEM((4, 128, D), BF),
            pltpu.SemaphoreType.DMA((10,)),
        ],
        smem_in=(0,),
        vmem=(4,),
        raw=range(10, 20),
        limit=32,
        flops=2 * 10**9,
    )
    arrived = exchange(plain(send).reshape(experts, 8, HALF), ("sp", "dp"))
    (base,) = call(
        shared_kernel,
        [((TOK, D), F32)],
        (ein, mixed, shared_gate, shared_up, shared_down),
        limit=20,
        flops=4 * 10**9,
    )
    (done,) = call(
        expert_kernel,
        [((ROWS, HALF), BF)],
        (arrived.reshape(ROWS, HALF), expert_gate[0], expert_up[0], expert_down[0]),
        scratch=[
            pltpu.VMEM((ROWS // 2, D), BF),
            pltpu.VMEM((D, 512), BF),
            pltpu.VMEM((D, 512), BF),
            pltpu.VMEM((512, D), BF),
            pltpu.SemaphoreType.DMA((3,)),
        ],
        vmem=(0,),
        raw=(1, 2, 3),
        out_vmem=(0,),
        limit=32,
        flops=3 * 10**9,
    )
    back = exchange(plain(done).reshape(experts, 8, HALF), ("sp", "dp"))
    (out,) = call(
        combine_kernel, [((TOK, D), BF)], (back.reshape(ROWS, HALF), hi, lo, base), vmem=(0,)
    )
    return plain(out)[None]


def solution(mesh):
    rows = P("dp", "sp", None)
    one = P(("sp", "dp"), None, None)
    return jax.shard_map(
        layer,
        mesh=mesh,
        in_specs=(
            (rows,) * 6 + (P(),) * 7 + (P("dp", None),) + (P(),) * 4 + (one,) * 3 + (rows, rows)
        ),
        out_specs=rows,
        check_vma=False,
    )
```

```python
import jax
import jax.numpy as jnp
from jax import lax
from jax._src.core import MemorySpace
from jax._src.state.primitives import with_memory_space_constraint
from jax.experimental import pallas as pl
from jax.experimental.pallas import tpu as pltpu
from jax.sharding import PartitionSpec as P


D = 2048
HEADS = 32
HEAD_DIM = 64
GROUPS = 8
STATE = 128
TOK = 128
EPS = 1e-06
BF = jnp.bfloat16
F32 = jnp.float32
PER = HEADS // GROUPS
GW = PER * HEAD_DIM
HALF = D // 2
ROWS = 1024
ST_ROWS = 160
TOP = 16


def full():
    return pl.BlockSpec(memory_space=pltpu.VMEM)


def smem():
    return pl.BlockSpec(memory_space=pltpu.SMEM)


def anywhere():
    return pl.BlockSpec(memory_space=pl.ANY)


def call(
    kernel, outs, args, scratch=(), vmem=(), smem_in=(), raw=(), free=(), out_vmem=(), limit=12,
    flops=10**6,
):
    placed = [
        v
        if i in smem_in or i in free
        else pltpu.with_memory_space_constraint(v, pltpu.VMEM if i in vmem else pltpu.HBM)
        for i, v in enumerate(args)
    ]
    return pl.pallas_call(
        kernel,
        out_shape=tuple(
            pltpu.VMEM(s, d) if i in out_vmem else pltpu.HBM(s, d)
            for i, (s, d) in enumerate(outs)
        ),
        in_specs=[
            smem() if i in smem_in else anywhere() if i in raw else full() for i in range(len(args))
        ],
        out_specs=tuple(full() for _ in outs),
        scratch_shapes=list(scratch),
        compiler_params=pltpu.CompilerParams(vmem_limit_bytes=limit << 20),
        cost_estimate=pl.CostEstimate(flops=flops, bytes_accessed=10**6, transcendentals=0),
    )(*placed)


def silu(v):
    return v / (1.0 + jnp.exp(-v))


def tap(pad, rows, weight):
    pad[0:8, :] = jnp.zeros((8, pad.shape[1]), F32)
    pad[8 : 8 + TOK, :] = rows.astype(F32)
    w = weight.astype(F32)
    total = pad[5 : 5 + TOK, :] * w[0:1, :]
    for k in range(1, 4):
        total = total + pad[5 + k : 5 + k + TOK, :] * w[k : k + 1, :]
    return silu(total)


def tap_top(pad, halo, rows, weight):
    pad[0:8, :] = halo.astype(F32)
    pad[8 : 8 + TOP, :] = rows.astype(F32)
    w = weight.astype(F32)
    total = pad[5 : 5 + TOP, :] * w[0:1, :]
    for k in range(1, 4):
        total = total + pad[5 + k : 5 + k + TOP, :] * w[k : k + 1, :]
    return silu(total)


def spread(cols, g):
    lane = lax.broadcasted_iota(jnp.int32, (cols.shape[0], 128), 1)
    out = []
    for i in range(0, PER, 2):
        h = g * PER + i
        out.append(jnp.where(lane < HEAD_DIM, cols[:, h : h + 1], cols[:, h + 1 : h + 2]))
    return jnp.concatenate(out, axis=1)


def states_kernel(
    x, b, step_in, cw, cbw, bias, dlog, st, v_out, xs_out, b_out, ec_out, grow_out, padx, padb
):
    s = step_in[...].astype(F32).T + bias[...]
    step = jnp.maximum(s, 0.0) + jnp.log(1.0 + jnp.exp(-jnp.abs(s)))
    logs = step * (-jnp.exp(dlog[...]))
    r = lax.broadcasted_iota(jnp.int32, (TOK, TOK), 0)
    c = lax.broadcasted_iota(jnp.int32, (TOK, TOK), 1)
    tri = (c <= r).astype(F32)
    cum = jnp.dot(tri, logs, precision=lax.Precision.HIGHEST, preferred_element_type=F32)
    ec_out[...] = jnp.exp(cum)
    grow = step * jnp.exp(-cum)
    grow_out[...] = grow
    later = jnp.where(lax.broadcasted_iota(jnp.int32, (TOK, HEADS), 0) < 3, 0.0, grow)
    tot = cum[TOK - 1 : TOK, :]
    etot = jnp.exp(tot)
    first = grow[0:8, :] * etot
    sub = lax.broadcasted_iota(jnp.int32, (8, 128), 0)
    low = lax.broadcasted_iota(jnp.int32, (8, 128), 1) < HEAD_DIM
    for g in range(GROUPS):
        xc = slice(g * GW, (g + 1) * GW)
        bc = slice(g * STATE, (g + 1) * STATE)
        xs = tap(padx.at[g % 2], x[:, xc], cw[:, xc])
        bm = tap(padb.at[g % 2], b[:, bc], cbw[:, bc]).astype(BF)
        v = (xs * spread(later, g)).astype(BF)
        xs_out[:, xc] = xs
        v_out[:, xc] = v
        b_out[:, bc] = bm
        fresh = lax.dot_general(v, bm, (((0,), (0,)), ((), ())), preferred_element_type=F32)

        def ends(rows):
            return jnp.where(sub < 3, pltpu.roll(rows[TOK - 8 :], 3, 0), pltpu.roll(rows[:8], 3, 0))

        b_ends = ends(b[:, bc].astype(F32))
        for i in range(2):
            h = g * PER + 2 * i
            o = g * 2 + i
            for j in range(2):
                k = (2 * i + j) * HEAD_DIM
                st[o, j * HEAD_DIM : (j + 1) * HEAD_DIM, :] = (
                    fresh[k : k + HEAD_DIM, :] * etot[0:1, h + j : h + j + 1]
                ).astype(BF)
            tail = jnp.zeros((8, 128), F32)
            for j in range(2):
                rest = jnp.broadcast_to(tot[0:1, h + j : h + j + 1], (8, 128))
                for q in range(3):
                    part = rest.astype(BF).astype(F32)
                    tail = jnp.where(sub == 3 * j + q, part, tail)
                    rest = rest - part
            w = jnp.where(low, first[:, h : h + 1], first[:, h + 1 : h + 2])
            w_hi = w.astype(BF).astype(F32)
            w_both = jnp.where(sub < 3, w_hi, pltpu.roll(w - w_hi, 3, 0))
            x_ends = ends(x[:, o * 128 : (o + 1) * 128].astype(F32))
            st[o, 128:144, :] = jnp.concatenate([tail, w_both], axis=0).astype(BF)
            st[o, 144:160, :] = jnp.concatenate([x_ends, b_ends], axis=0).astype(BF)


def inner_kernel(
    x, b, c, halo, cw, cbw, ccw, v_in, b_in, xs_in, ec, grow, skip, a_out, c_out, padx, padb, padc
):
    r = lax.broadcasted_iota(jnp.int32, (TOK, TOK), 0)
    s = lax.broadcasted_iota(jnp.int32, (TOK, TOK), 1)
    lower = s <= r
    cols = ec[...]
    top = grow[0:TOP, :]
    sk = jnp.broadcast_to(skip[...], (TOK, HEADS))
    for g in range(GROUPS):
        xc = slice(g * GW, (g + 1) * GW)
        bc = slice(g * STATE, (g + 1) * STATE)
        bh = slice(D + g * STATE, D + (g + 1) * STATE)
        ch = slice(D + 1024 + g * STATE, D + 1024 + (g + 1) * STATE)
        xt = tap_top(padx.at[g % 2], halo[:, xc], x[0:TOP, xc], cw[:, xc])
        bt = tap_top(padb.at[g % 2, 0], halo[:, bh], b[0:TOP, bc], cbw[:, bc]).astype(BF)
        ct = tap_top(padb.at[g % 2, 1], halo[:, ch], c[0:TOP, bc], ccw[:, bc])
        vt = (xt * spread(top, g)).astype(BF)
        cm = tap(padc.at[g % 2], c[:, bc], ccw[:, bc])
        cm = jnp.concatenate([ct, cm[TOP:]], axis=0).astype(BF)
        c_out[:, bc] = cm
        bm = jnp.concatenate([bt, b_in[TOP:, bc]], axis=0)
        v = jnp.concatenate([vt, v_in[TOP:, xc]], axis=0)
        xs = jnp.concatenate([xt, xs_in[TOP:, xc]], axis=0)
        cb = lax.dot_general(cm, bm, (((1,), (1,)), ((), ())), preferred_element_type=F32)
        cb = jnp.where(lower, cb, 0.0).astype(BF)
        u = jnp.dot(cb, v, preferred_element_type=F32)
        a_out[:, xc] = u * spread(cols, g) + xs * spread(sk, g)


def carry_kernel(place, cw, cbw, got, out):
    count = got.shape[0]
    o = place[8]
    sub = lax.broadcasted_iota(jnp.int32, (count, 8, 128), 1)

    def starts(rows, weight):
        rows = rows.astype(F32)
        before = jnp.concatenate([jnp.zeros((1, 8, 128), F32), rows[:-1]], axis=0)
        seq = jnp.where(sub < 3, before, rows)
        w = weight.astype(F32)
        total = seq * w[0:1, :][None]
        for k in range(1, 4):
            total = total + pltpu.roll(seq, 8 - k, 1) * w[k : k + 1, :][None]
        return jnp.where(sub < 3, silu(total), 0.0)

    tails = got[:, 128:144, :].astype(F32)
    ends = got[:, 144:160, :].astype(F32)
    w = tails[:, 8:16]
    w = w + pltpu.roll(w, 5, 1)
    xs = starts(ends[:, 0:8], cw[:, pl.ds(pl.multiple_of(o * 128, 128), 128)])
    bm = starts(ends[:, 8:16], cbw[:, pl.ds(pl.multiple_of((o // 2) * 128, 128), 128)])
    vt = jnp.where(sub < 3, xs * w, 0.0).reshape(count * 8, 128).T
    bm = bm.reshape(count * 8, 128).astype(BF)
    lane = lax.broadcasted_iota(jnp.int32, (128, 128), 1)
    row = lax.broadcasted_iota(jnp.int32, (2 * HEAD_DIM, 128), 0)
    carry = jnp.zeros((2 * HEAD_DIM, 128), F32)
    for i in range(count):
        out[i] = carry.astype(BF)
        if i + 1 < count:
            mine = jnp.where(lane // 8 == i, vt, 0.0).astype(BF)
            extra = jnp.dot(mine, bm, preferred_element_type=F32)
            tail = tails[i, 0:8]
            fa = jnp.exp(tail[0:1] + tail[1:2] + tail[2:3])
            fb = jnp.exp(tail[3:4] + tail[4:5] + tail[5:6])
            factor = jnp.where(row < HEAD_DIM, fa, fb)
            carry = carry * factor + (got[i, 0 : 2 * HEAD_DIM, :].astype(F32) + extra)


def routes_kernel(routes, rw, d_out, hi_out, lo_out):
    e = lax.broadcasted_iota(jnp.int32, (TOK, 128), 1)
    r = lax.broadcasted_iota(jnp.int32, (TOK, TOK), 0)
    s = lax.broadcasted_iota(jnp.int32, (TOK, TOK), 1)
    tri = (s < r).astype(BF)
    both = jnp.concatenate([routes[...].astype(F32), rw[...], jnp.zeros((4, TOK), F32)], axis=0).T
    ids = both[:, 0:2].astype(jnp.int32)
    w = both[:, 2:4]
    hot = [(ids[:, k : k + 1] == e).astype(F32) for k in range(2)]
    before0 = jnp.dot(tri, hot[0].astype(BF), preferred_element_type=F32)
    before1 = jnp.dot(tri, hot[1].astype(BF), preferred_element_type=F32)
    before1 = before1 + jnp.sum(hot[0], axis=0, keepdims=True)
    pos = [
        jnp.sum(before0 * hot[0], axis=1, keepdims=True).astype(jnp.int32),
        jnp.sum(before1 * hot[1], axis=1, keepdims=True).astype(jnp.int32),
    ]
    lane = lax.broadcasted_iota(jnp.int32, (TOK, ROWS), 1)
    for h in range(2):
        mask = [lane == ids[:, k : k + 1] * 8 + pos[k] + 4 * h for k in range(2)]
        disp = jnp.where(mask[0] | mask[1], 1.0, 0.0)
        d_out[:, h * TOK : (h + 1) * TOK] = disp.T.astype(BF)
        comb = jnp.where(mask[0], w[:, 0:1], 0.0) + jnp.where(mask[1], w[:, 1:2], 0.0)
        hi = comb.astype(BF)
        hi_out[h * TOK : (h + 1) * TOK, :] = hi
        lo_out[h * TOK : (h + 1) * TOK, :] = (comb - hi.astype(F32)).astype(BF)


def norm_kernel(a, cm, ec, pref, gate, gain, norm):
    cols = ec[...]
    for g in range(GROUPS):
        xc = slice(g * GW, (g + 1) * GW)
        bc = slice(g * STATE, (g + 1) * STATE)
        outer = lax.dot_general(
            cm[:, bc], pref[g], (((1,), (1,)), ((), ())), preferred_element_type=F32
        )
        y = (a[:, xc] + outer * spread(cols, g)).astype(BF).astype(F32)
        y = y * silu(gate[:, xc].astype(F32))
        y = y * lax.rsqrt(jnp.mean(y * y, axis=1, keepdims=True) + EPS)
        norm[g] = (y * gain[:, xc]).astype(BF)


def mix_kernel(
    place, norm, resid, fgain, disp, w0, w1, w2, w3, w4, w5, w6, w7,
    mixed_out, ein_out, send, wide, sems
):
    loads = [
        pltpu.make_async_copy(w, wide.at[k], sems.at[k])
        for k, w in enumerate((w0, w1, w2, w3, w4, w5, w6, w7))
    ]
    for load in loads:
        load.start()
    proj = resid[...].astype(F32)
    for k, load in enumerate(loads):
        load.wait()
        proj = proj + jnp.dot(norm[place[k]], wide[k], preferred_element_type=F32)
    mixed = proj.astype(BF)
    mixed_out[...] = mixed
    m = mixed.astype(F32)
    ein = (m * lax.rsqrt(jnp.mean(m * m, axis=1, keepdims=True) + EPS) * fgain[...]).astype(BF)
    ein_out[...] = ein
    stack = jnp.concatenate([ein[:, :HALF], ein[:, HALF:]], axis=0)
    send[...] = jnp.dot(disp[...], stack, preferred_element_type=F32).astype(BF)


def shared_kernel(ein, mixed, sg, su, sd, out):
    x = ein[...]
    gate = jnp.dot(x, sg[...], preferred_element_type=F32)
    up = jnp.dot(x, su[...], preferred_element_type=F32)
    hidden = (silu(gate) * up).astype(BF)
    out[...] = mixed[...].astype(F32) + jnp.dot(hidden, sd[...], preferred_element_type=F32)


def expert_kernel(got, wg_in, wu_in, wd_in, out, xbuf, wg, wu, wd, sems):
    pairs = ((wg_in, wg), (wu_in, wu), (wd_in, wd))
    loads = [pltpu.make_async_copy(v, w, sems.at[k]) for k, (v, w) in enumerate(pairs)]
    for load in loads:
        load.start()
    n = 256
    sub = lax.broadcasted_iota(jnp.int32, (ROWS // 16, 8, n), 1)
    for q in range(HALF // n):
        t = got[:, q * n : (q + 1) * n].astype(F32).reshape(ROWS // 16, 2, 8, n)
        r0, r1 = t[:, 0], t[:, 1]
        x0 = jnp.where(sub < 4, r0, pltpu.roll(r1, 4, 1))
        x1 = jnp.where(sub < 4, pltpu.roll(r0, 4, 1), r1)
        xbuf[:, q * n : (q + 1) * n] = x0.reshape(ROWS // 2, n).astype(BF)
        xbuf[:, HALF + q * n : HALF + (q + 1) * n] = x1.reshape(ROWS // 2, n).astype(BF)
    x = xbuf[...]
    loads[0].wait()
    gate = jnp.dot(x, wg[...], preferred_element_type=F32)
    loads[1].wait()
    up = jnp.dot(x, wu[...], preferred_element_type=F32)
    hidden = (silu(gate) * up).astype(BF)
    loads[2].wait()
    for q in range(HALF // n):
        y0 = jnp.dot(hidden, wd[:, q * n : (q + 1) * n], preferred_element_type=F32)
        y1 = jnp.dot(hidden, wd[:, HALF + q * n : HALF + (q + 1) * n], preferred_element_type=F32)
        y0 = y0.reshape(ROWS // 16, 8, n)
        y1 = y1.reshape(ROWS // 16, 8, n)
        o0 = jnp.where(sub < 4, y0, pltpu.roll(y1, 4, 1))
        o1 = jnp.where(sub < 4, pltpu.roll(y0, 4, 1), y1)
        out[:, q * n : (q + 1) * n] = jnp.stack([o0, o1], axis=1).reshape(ROWS, n).astype(BF)


def combine_kernel(got, hi, lo, base, out):
    g = got[...]
    y = jnp.dot(hi[...], g, preferred_element_type=F32) + jnp.dot(
        lo[...], g, preferred_element_type=F32
    )
    out[:, :HALF] = (base[:, :HALF] + y[:TOK]).astype(BF)
    out[:, HALF:] = (base[:, HALF:] + y[TOK:]).astype(BF)


def plain(v):
    return with_memory_space_constraint(v, MemorySpace.Device)


def exchange(v, axis):
    return lax.all_to_all(plain(v), axis, split_axis=0, concat_axis=0, tiled=True)


def layer(
    residual, head_input, gate_input, b_input, c_input, step_input, conv_weight,
    conv_b_weight, conv_c_weight, step_bias, decay_log, skip, norm_gain, out_weight,
    ffn_gain, shared_gate, shared_up, shared_down, expert_gate, expert_up, expert_down,
    routes, route_weights,
):
    ways = lax.axis_size("sp")
    dps = lax.axis_size("dp")
    experts = ways * dps
    x, b, c = head_input[0], b_input[0], c_input[0]
    ends = jnp.concatenate([x[TOK - 8 :], b[TOK - 8 :], c[TOK - 8 :]], axis=1)
    halo = lax.ppermute(ends, "sp", [(i, i + 1) for i in range(ways - 1)])

    def ring(v):
        return lax.ppermute(v, "dp", [(i, (i + (-2 if i % 2 else 2)) % dps) for i in range(dps)])

    def swap(v):
        return lax.ppermute(v, "dp", [(i, i ^ 1) for i in range(dps)])

    partner = swap(out_weight)
    near = ring(out_weight)
    near2 = ring(partner)
    far = ring(near)
    pieces = [out_weight, partner, near, near2, swap(near), swap(near2)]
    pieces += [far, swap(far)]
    me = lax.axis_index("dp")
    odd = me & 1
    at = (me + dps - 2 + 4 * odd) % dps
    other = ((me ^ 1) + 2 + (dps - 4) * odd) % dps
    place = jnp.stack(
        [me, me ^ 1, at, at ^ 1, other, other ^ 1, me ^ 4, me ^ 5, lax.axis_index("sp")]
    ).astype(jnp.int32)

    st, v, xs, bm, ec, grow = call(
        states_kernel,
        [
            ((ways, ST_ROWS, 128), BF), ((TOK, D), BF), ((TOK, D), F32), ((TOK, 1024), BF),
            ((TOK, HEADS), F32), ((TOK, HEADS), F32),
        ],
        (x, b, step_input[0].T, conv_weight, conv_b_weight, step_bias[None], decay_log[None]),
        scratch=[pltpu.VMEM((2, TOK + 8, GW), F32), pltpu.VMEM((2, TOK + 8, STATE), F32)],
    )
    got = exchange(st, "sp")
    a, cm = call(
        inner_kernel,
        [((TOK, D), F32), ((TOK, 1024), BF)],
        (
            x, b, c, halo, conv_weight, conv_b_weight, conv_c_weight, v, bm, xs, ec, grow,
            skip[None],
        ),
        scratch=[
            pltpu.VMEM((2, TOP + 8, GW), F32),
            pltpu.VMEM((2, 2, TOP + 8, STATE), F32),
            pltpu.VMEM((2, TOK + 8, STATE), F32),
        ],
        flops=4 * 10**9,
    )
    disp, hi, lo = call(
        routes_kernel,
        [((ROWS, 2 * TOK), BF), ((2 * TOK, ROWS), BF), ((2 * TOK, ROWS), BF)],
        (routes[0].T, route_weights[0].T),
        flops=2 * 10**9,
    )
    (carried,) = call(
        carry_kernel,
        [((ways, 128, 128), BF)],
        (place, conv_weight, conv_b_weight, got),
        smem_in=(0,),
        vmem=(3,),
    )
    pref = exchange(carried, "sp")
    (norm,) = call(
        norm_kernel,
        [((GROUPS, TOK, GW), BF)],
        (a, cm, ec, pref.reshape(GROUPS, GW, STATE), gate_input[0], norm_gain[None]),
        vmem=(3,),
        out_vmem=(0,),
        flops=10**9,
    )
    mixed, ein, send = call(
        mix_kernel,
        [((TOK, D), BF), ((TOK, D), BF), ((ROWS, HALF), BF)],
        (place, norm, residual[0], ffn_gain[None], disp, *pieces),
        scratch=[pltpu.VMEM((8, 256, D), BF), pltpu.SemaphoreType.DMA((8,))],
        smem_in=(0,),
        vmem=(1,),
        raw=range(5, 13),
        free=range(6, 13),
        limit=32,
        flops=2 * 10**9,
    )
    arrived = exchange(plain(send).reshape(experts, 8, HALF), ("sp", "dp"))
    (base,) = call(
        shared_kernel,
        [((TOK, D), F32)],
        (ein, mixed, shared_gate, shared_up, shared_down),
        limit=20,
        flops=4 * 10**9,
    )
    (done,) = call(
        expert_kernel,
        [((ROWS, HALF), BF)],
        (arrived.reshape(ROWS, HALF), expert_gate[0], expert_up[0], expert_down[0]),
        scratch=[
            pltpu.VMEM((ROWS // 2, D), BF),
            pltpu.VMEM((D, 512), BF),
            pltpu.VMEM((D, 512), BF),
            pltpu.VMEM((512, D), BF),
            pltpu.SemaphoreType.DMA((3,)),
        ],
        vmem=(0,),
        raw=(1, 2, 3),
        out_vmem=(0,),
        limit=32,
        flops=3 * 10**9,
    )
    back = exchange(plain(done).reshape(experts, 8, HALF), ("sp", "dp"))
    (out,) = call(
        combine_kernel, [((TOK, D), BF)], (back.reshape(ROWS, HALF), hi, lo, base), vmem=(0,)
    )
    return plain(out)[None]


def solution(mesh):
    rows = P("dp", "sp", None)
    one = P(("sp", "dp"), None, None)
    return jax.shard_map(
        layer,
        mesh=mesh,
        in_specs=(
            (rows,) * 6 + (P(),) * 7 + (P("dp", None),) + (P(),) * 4 + (one,) * 3 + (rows, rows)
        ),
        out_specs=rows,
        check_vma=False,
    )
```

```python
import jax
import jax.numpy as jnp
from jax import lax
from jax._src.core import MemorySpace
from jax._src.state.primitives import with_memory_space_constraint
from jax.experimental import pallas as pl
from jax.experimental.pallas import tpu as pltpu
from jax.sharding import PartitionSpec as P


D = 2048
HEADS = 32
HEAD_DIM = 64
GROUPS = 8
STATE = 128
TOK = 128
EPS = 1e-06
BF = jnp.bfloat16
F32 = jnp.float32
PER = HEADS // GROUPS
GW = PER * HEAD_DIM
HALF = D // 2
ROWS = 1024
ST_ROWS = 160


def full():
    return pl.BlockSpec(memory_space=pltpu.VMEM)


def smem():
    return pl.BlockSpec(memory_space=pltpu.SMEM)


def anywhere():
    return pl.BlockSpec(memory_space=pl.ANY)


def call(
    kernel, outs, args, scratch=(), vmem=(), smem_in=(), raw=(), free=(), out_vmem=(), raw_out=(), limit=12,
    flops=10**6,
):
    placed = [
        v
        if i in smem_in or i in free
        else pltpu.with_memory_space_constraint(v, pltpu.VMEM if i in vmem else pltpu.HBM)
        for i, v in enumerate(args)
    ]
    return pl.pallas_call(
        kernel,
        out_shape=tuple(
            pltpu.VMEM(s, d) if i in out_vmem else pltpu.HBM(s, d)
            for i, (s, d) in enumerate(outs)
        ),
        in_specs=[
            smem() if i in smem_in else anywhere() if i in raw else full() for i in range(len(args))
        ],
        out_specs=tuple(anywhere() if i in raw_out else full() for i in range(len(outs))),
        scratch_shapes=list(scratch),
        compiler_params=pltpu.CompilerParams(vmem_limit_bytes=limit << 20),
        cost_estimate=pl.CostEstimate(flops=flops, bytes_accessed=10**6, transcendentals=0),
    )(*placed)


def silu(v):
    return v / (1.0 + jnp.exp(-v))


def tap(pad, halo, rows, weight):
    pad[0:8, :] = jnp.zeros((8, pad.shape[1]), F32) if halo is None else halo.astype(F32)
    pad[8 : 8 + TOK, :] = rows.astype(F32)
    w = weight.astype(F32)
    total = pad[5 : 5 + TOK, :] * w[0:1, :]
    for k in range(1, 4):
        total = total + pad[5 + k : 5 + k + TOK, :] * w[k : k + 1, :]
    return silu(total)


def spread(cols, g):
    lane = lax.broadcasted_iota(jnp.int32, (cols.shape[0], 128), 1)
    out = []
    for i in range(0, PER, 2):
        h = g * PER + i
        out.append(jnp.where(lane < HEAD_DIM, cols[:, h : h + 1], cols[:, h + 1 : h + 2]))
    return jnp.concatenate(out, axis=1)


def states_kernel(
    x, b, c, step_in, cw, cbw, bias, dlog, st, ec_out, grow_out, ends_out, padx, padb, last, sem
):
    load = pltpu.make_async_copy(c.at[pl.ds(TOK - 8, 8), :], last, sem)
    load.start()
    s = step_in[...].astype(F32).T + bias[...]
    step = jnp.maximum(s, 0.0) + jnp.log(1.0 + jnp.exp(-jnp.abs(s)))
    logs = step * (-jnp.exp(dlog[...]))
    r = lax.broadcasted_iota(jnp.int32, (TOK, TOK), 0)
    c = lax.broadcasted_iota(jnp.int32, (TOK, TOK), 1)
    tri = (c <= r).astype(F32)
    cum = jnp.dot(tri, logs, precision=lax.Precision.HIGHEST, preferred_element_type=F32)
    ec_out[...] = jnp.exp(cum)
    grow = step * jnp.exp(-cum)
    grow_out[...] = grow
    later = jnp.where(lax.broadcasted_iota(jnp.int32, (TOK, HEADS), 0) < 3, 0.0, grow)
    tot = cum[TOK - 1 : TOK, :]
    etot = jnp.exp(tot)
    first = grow[0:8, :] * etot
    sub = lax.broadcasted_iota(jnp.int32, (8, 128), 0)
    low = lax.broadcasted_iota(jnp.int32, (8, 128), 1) < HEAD_DIM
    for g in range(GROUPS):
        xc = slice(g * GW, (g + 1) * GW)
        bc = slice(g * STATE, (g + 1) * STATE)
        xs = tap(padx.at[g % 2], None, x[:, xc], cw[:, xc])
        bm = tap(padb.at[g % 2], None, b[:, bc], cbw[:, bc]).astype(BF)
        v = (xs * spread(later, g)).astype(BF)
        fresh = lax.dot_general(v, bm, (((0,), (0,)), ((), ())), preferred_element_type=F32)

        def ends(rows):
            return jnp.where(sub < 3, pltpu.roll(rows[TOK - 8 :], 3, 0), pltpu.roll(rows[:8], 3, 0))

        b_ends = ends(b[:, bc].astype(F32))
        for i in range(2):
            h = g * PER + 2 * i
            o = g * 2 + i
            for j in range(2):
                k = (2 * i + j) * HEAD_DIM
                st[o, j * HEAD_DIM : (j + 1) * HEAD_DIM, :] = (
                    fresh[k : k + HEAD_DIM, :] * etot[0:1, h + j : h + j + 1]
                ).astype(BF)
            tail = jnp.zeros((8, 128), F32)
            for j in range(2):
                rest = jnp.broadcast_to(tot[0:1, h + j : h + j + 1], (8, 128))
                for q in range(3):
                    part = rest.astype(BF).astype(F32)
                    tail = jnp.where(sub == 3 * j + q, part, tail)
                    rest = rest - part
            w = jnp.where(low, first[:, h : h + 1], first[:, h + 1 : h + 2])
            w_hi = w.astype(BF).astype(F32)
            w_both = jnp.where(sub < 3, w_hi, pltpu.roll(w - w_hi, 3, 0))
            x_ends = ends(x[:, o * 128 : (o + 1) * 128].astype(F32))
            st[o, 128:144, :] = jnp.concatenate([tail, w_both], axis=0).astype(BF)
            st[o, 144:160, :] = jnp.concatenate([x_ends, b_ends], axis=0).astype(BF)
    ends_out[:, 0:D] = x[TOK - 8 :, :]
    ends_out[:, D : D + 1024] = b[TOK - 8 :, :]
    load.wait()
    ends_out[:, D + 1024 :] = last[...]


def inner_kernel(x, b, c, halo, cw, cbw, ccw, ec, grow, skip, a_out, c_out, padx, padb):
    r = lax.broadcasted_iota(jnp.int32, (TOK, TOK), 0)
    s = lax.broadcasted_iota(jnp.int32, (TOK, TOK), 1)
    lower = s <= r
    cols = ec[...]
    rows = grow[...]
    sk = jnp.broadcast_to(skip[...], (TOK, HEADS))
    for g in range(GROUPS):
        xc = slice(g * GW, (g + 1) * GW)
        bc = slice(g * STATE, (g + 1) * STATE)
        bh = slice(D + g * STATE, D + (g + 1) * STATE)
        ch = slice(D + 1024 + g * STATE, D + 1024 + (g + 1) * STATE)
        xs = tap(padx.at[g % 2], halo[:, xc], x[:, xc], cw[:, xc])
        bm = tap(padb.at[g % 2, 0], halo[:, bh], b[:, bc], cbw[:, bc]).astype(BF)
        cm = tap(padb.at[g % 2, 1], halo[:, ch], c[:, bc], ccw[:, bc]).astype(BF)
        c_out[:, bc] = cm
        v = (xs * spread(rows, g)).astype(BF)
        cb = lax.dot_general(cm, bm, (((1,), (1,)), ((), ())), preferred_element_type=F32)
        cb = jnp.where(lower, cb, 0.0).astype(BF)
        u = jnp.dot(cb, v, preferred_element_type=F32)
        a_out[:, xc] = u * spread(cols, g) + xs * spread(sk, g)


def carry_kernel(place, cw, cbw, got, out):
    count = got.shape[0]
    o = place[8]
    sub = lax.broadcasted_iota(jnp.int32, (count, 8, 128), 1)

    def starts(rows, weight):
        rows = rows.astype(F32)
        before = jnp.concatenate([jnp.zeros((1, 8, 128), F32), rows[:-1]], axis=0)
        seq = jnp.where(sub < 3, before, rows)
        w = weight.astype(F32)
        total = seq * w[0:1, :][None]
        for k in range(1, 4):
            total = total + pltpu.roll(seq, 8 - k, 1) * w[k : k + 1, :][None]
        return jnp.where(sub < 3, silu(total), 0.0)

    tails = got[:, 128:144, :].astype(F32)
    ends = got[:, 144:160, :].astype(F32)
    w = tails[:, 8:16]
    w = w + pltpu.roll(w, 5, 1)
    xs = starts(ends[:, 0:8], cw[:, pl.ds(pl.multiple_of(o * 128, 128), 128)])
    bm = starts(ends[:, 8:16], cbw[:, pl.ds(pl.multiple_of((o // 2) * 128, 128), 128)])
    vt = jnp.where(sub < 3, xs * w, 0.0).reshape(count * 8, 128).T
    bm = bm.reshape(count * 8, 128).astype(BF)
    lane = lax.broadcasted_iota(jnp.int32, (128, 128), 1)
    row = lax.broadcasted_iota(jnp.int32, (2 * HEAD_DIM, 128), 0)
    carry = jnp.zeros((2 * HEAD_DIM, 128), F32)
    for i in range(count):
        out[i] = carry.astype(BF)
        if i + 1 < count:
            mine = jnp.where(lane // 8 == i, vt, 0.0).astype(BF)
            extra = jnp.dot(mine, bm, preferred_element_type=F32)
            tail = tails[i, 0:8]
            fa = jnp.exp(tail[0:1] + tail[1:2] + tail[2:3])
            fb = jnp.exp(tail[3:4] + tail[4:5] + tail[5:6])
            factor = jnp.where(row < HEAD_DIM, fa, fb)
            carry = carry * factor + (got[i, 0 : 2 * HEAD_DIM, :].astype(F32) + extra)


def slots(routes, rw):
    both = jnp.concatenate([routes[...].astype(F32), rw[...], jnp.zeros((4, TOK), F32)], axis=0).T
    ids = both[:, 0:2].astype(jnp.int32)
    e = lax.broadcasted_iota(jnp.int32, (TOK, 128), 1)
    r = lax.broadcasted_iota(jnp.int32, (TOK, TOK), 0)
    s = lax.broadcasted_iota(jnp.int32, (TOK, TOK), 1)
    tri = (s < r).astype(BF)
    hot = [(ids[:, k : k + 1] == e).astype(F32) for k in range(2)]
    before0 = jnp.dot(tri, hot[0].astype(BF), preferred_element_type=F32)
    before1 = jnp.dot(tri, hot[1].astype(BF), preferred_element_type=F32)
    before1 = before1 + jnp.sum(hot[0], axis=0, keepdims=True)
    pos = [
        jnp.sum(before0 * hot[0], axis=1, keepdims=True).astype(jnp.int32),
        jnp.sum(before1 * hot[1], axis=1, keepdims=True).astype(jnp.int32),
    ]
    return [ids[:, k : k + 1] * 8 + pos[k] for k in range(2)], both[:, 2:4]


def routes_kernel(routes, rw, d_out):
    at, _ = slots(routes, rw)
    lane = lax.broadcasted_iota(jnp.int32, (TOK, ROWS), 1)
    for h in range(2):
        hit = (lane == at[0] + 4 * h) | (lane == at[1] + 4 * h)
        d_out[:, h * TOK : (h + 1) * TOK] = jnp.where(hit, 1.0, 0.0).T.astype(BF)


def weights_kernel(routes, rw, w_out):
    at, w = slots(routes, rw)
    lane = lax.broadcasted_iota(jnp.int32, (TOK, ROWS), 1)
    for h in range(2):
        comb = jnp.where(lane == at[0] + 4 * h, w[:, 0:1], 0.0)
        comb = comb + jnp.where(lane == at[1] + 4 * h, w[:, 1:2], 0.0)
        w_out[h * TOK : (h + 1) * TOK, :] = comb.astype(BF)


def mix_kernel(
    place, a, cm, ec, pref, gate, gain, fgain, resid_in, disp_in,
    w0, w1, w2, w3, w4, w5, w6, w7, mixed_out, ein_out, send_out,
    norm, wide, resid, disp, mixed_buf, ein_buf, send, sems, out_sems
):
    loads = [
        pltpu.make_async_copy(w, wide.at[k], sems.at[k])
        for k, w in enumerate((w0, w1, w2, w3, w4, w5, w6, w7))
    ]
    loads.append(pltpu.make_async_copy(resid_in, resid, sems.at[8]))
    loads.append(pltpu.make_async_copy(disp_in, disp, sems.at[9]))
    for load in loads:
        load.start()
    cols = ec[...]
    for g in range(GROUPS):
        xc = slice(g * GW, (g + 1) * GW)
        bc = slice(g * STATE, (g + 1) * STATE)
        outer = lax.dot_general(
            cm[:, bc], pref[g], (((1,), (1,)), ((), ())), preferred_element_type=F32
        )
        y = (a[:, xc] + outer * spread(cols, g)).astype(BF).astype(F32)
        y = y * silu(gate[:, xc].astype(F32))
        y = y * lax.rsqrt(jnp.mean(y * y, axis=1, keepdims=True) + EPS)
        norm[g] = (y * gain[:, xc]).astype(BF)
    for load in loads:
        load.wait()
    proj = resid[...].astype(F32)
    for k in range(8):
        proj = proj + jnp.dot(norm[place[k]], wide[k], preferred_element_type=F32)
    mixed = proj.astype(BF)
    mixed_buf[...] = mixed
    stores = [pltpu.make_async_copy(mixed_buf, mixed_out, out_sems.at[0])]
    stores[0].start()
    m = mixed.astype(F32)
    ein = (m * lax.rsqrt(jnp.mean(m * m, axis=1, keepdims=True) + EPS) * fgain[...]).astype(BF)
    ein_buf[...] = ein
    stores.append(pltpu.make_async_copy(ein_buf, ein_out, out_sems.at[1]))
    stores[1].start()
    stack = jnp.concatenate([ein[:, :HALF], ein[:, HALF:]], axis=0)
    for q in range(4):
        part = pl.ds(q * 256, 256)
        send[part, :] = jnp.dot(disp[part, :], stack, preferred_element_type=F32).astype(BF)
        store = pltpu.make_async_copy(send.at[part, :], send_out.at[part, :], out_sems.at[2 + q])
        store.start()
        stores.append(store)
    for store in stores:
        store.wait()


def shared_kernel(ein, mixed, sg, su, sd, out):
    x = ein[...]
    gate = jnp.dot(x, sg[...], preferred_element_type=F32)
    up = jnp.dot(x, su[...], preferred_element_type=F32)
    hidden = (silu(gate) * up).astype(BF)
    out[...] = mixed[...].astype(F32) + jnp.dot(hidden, sd[...], preferred_element_type=F32)


def expert_kernel(got, wg_in, wu_in, wd_in, out, xbuf, wg, wu, wd, sems):
    pairs = ((wg_in, wg), (wu_in, wu), (wd_in, wd))
    loads = [pltpu.make_async_copy(v, w, sems.at[k]) for k, (v, w) in enumerate(pairs)]
    for load in loads:
        load.start()
    n = 256
    sub = lax.broadcasted_iota(jnp.int32, (ROWS // 16, 8, n), 1)
    for q in range(HALF // n):
        t = got[:, q * n : (q + 1) * n].astype(F32).reshape(ROWS // 16, 2, 8, n)
        r0, r1 = t[:, 0], t[:, 1]
        x0 = jnp.where(sub < 4, r0, pltpu.roll(r1, 4, 1))
        x1 = jnp.where(sub < 4, pltpu.roll(r0, 4, 1), r1)
        xbuf[:, q * n : (q + 1) * n] = x0.reshape(ROWS // 2, n).astype(BF)
        xbuf[:, HALF + q * n : HALF + (q + 1) * n] = x1.reshape(ROWS // 2, n).astype(BF)
    x = xbuf[...]
    loads[0].wait()
    gate = jnp.dot(x, wg[...], preferred_element_type=F32)
    loads[1].wait()
    up = jnp.dot(x, wu[...], preferred_element_type=F32)
    hidden = (silu(gate) * up).astype(BF)
    loads[2].wait()
    for q in range(HALF // n):
        y0 = jnp.dot(hidden, wd[:, q * n : (q + 1) * n], preferred_element_type=F32)
        y1 = jnp.dot(hidden, wd[:, HALF + q * n : HALF + (q + 1) * n], preferred_element_type=F32)
        y0 = y0.reshape(ROWS // 16, 8, n)
        y1 = y1.reshape(ROWS // 16, 8, n)
        o0 = jnp.where(sub < 4, y0, pltpu.roll(y1, 4, 1))
        o1 = jnp.where(sub < 4, pltpu.roll(y0, 4, 1), y1)
        out[:, q * n : (q + 1) * n] = jnp.stack([o0, o1], axis=1).reshape(ROWS, n).astype(BF)


def combine_kernel(got, w, base, out):
    y = jnp.dot(w[...], got[...], preferred_element_type=F32)
    out[:, :HALF] = (base[:, :HALF] + y[:TOK]).astype(BF)
    out[:, HALF:] = (base[:, HALF:] + y[TOK:]).astype(BF)


def plain(v):
    return with_memory_space_constraint(v, MemorySpace.Device)


def exchange(v, axis):
    return lax.all_to_all(plain(v), axis, split_axis=0, concat_axis=0, tiled=True)


def layer(
    residual, head_input, gate_input, b_input, c_input, step_input, conv_weight,
    conv_b_weight, conv_c_weight, step_bias, decay_log, skip, norm_gain, out_weight,
    ffn_gain, shared_gate, shared_up, shared_down, expert_gate, expert_up, expert_down,
    routes, route_weights,
):
    ways = lax.axis_size("sp")
    dps = lax.axis_size("dp")
    experts = ways * dps
    x, b, c = head_input[0], b_input[0], c_input[0]

    def ring(v):
        return lax.ppermute(v, "dp", [(i, (i + (-2 if i % 2 else 2)) % dps) for i in range(dps)])

    def swap(v):
        return lax.ppermute(v, "dp", [(i, i ^ 1) for i in range(dps)])

    partner = swap(out_weight)
    near = ring(out_weight)
    near2 = ring(partner)
    far = ring(near)
    pieces = [out_weight, partner, near, near2, swap(near), swap(near2)]
    pieces += [far, swap(far)]
    me = lax.axis_index("dp")
    odd = me & 1
    at = (me + dps - 2 + 4 * odd) % dps
    other = ((me ^ 1) + 2 + (dps - 4) * odd) % dps
    place = jnp.stack(
        [me, me ^ 1, at, at ^ 1, other, other ^ 1, me ^ 4, me ^ 5, lax.axis_index("sp")]
    ).astype(jnp.int32)

    st, ec, grow, ends = call(
        states_kernel,
        [((ways, ST_ROWS, 128), BF), ((TOK, HEADS), F32), ((TOK, HEADS), F32), ((8, 4096), BF)],
        (x, b, c, step_input[0].T, conv_weight, conv_b_weight, step_bias[None], decay_log[None]),
        raw=(2,),
        scratch=[
            pltpu.VMEM((2, TOK + 8, GW), F32),
            pltpu.VMEM((2, TOK + 8, STATE), F32),
            pltpu.VMEM((8, 1024), BF),
            pltpu.SemaphoreType.DMA,
        ],
    )
    got = exchange(st, "sp")
    halo = lax.ppermute(plain(ends), "sp", [(i, i + 1) for i in range(ways - 1)])
    a, cm = call(
        inner_kernel,
        [((TOK, D), F32), ((TOK, 1024), BF)],
        (x, b, c, halo, conv_weight, conv_b_weight, conv_c_weight, ec, grow, skip[None]),
        free=(3,),
        scratch=[pltpu.VMEM((2, TOK + 8, GW), F32), pltpu.VMEM((2, 2, TOK + 8, STATE), F32)],
        flops=4 * 10**9,
    )
    ways_in = (routes[0].T, route_weights[0].T)
    (disp,) = call(routes_kernel, [((ROWS, 2 * TOK), BF)], ways_in, flops=2 * 10**9)
    (comb,) = call(weights_kernel, [((2 * TOK, ROWS), BF)], ways_in, flops=2 * 10**9)
    (carried,) = call(
        carry_kernel,
        [((ways, 128, 128), BF)],
        (place, conv_weight, conv_b_weight, got),
        smem_in=(0,),
        vmem=(3,),
    )
    pref = exchange(carried, "sp")
    mixed, ein, send = call(
        mix_kernel,
        [((TOK, D), BF), ((TOK, D), BF), ((ROWS, HALF), BF)],
        (
            place, a, cm, ec, pref.reshape(GROUPS, GW, STATE), gate_input[0], norm_gain[None],
            ffn_gain[None], residual[0], disp, *pieces,
        ),
        scratch=[
            pltpu.VMEM((GROUPS, TOK, GW), BF),
            pltpu.VMEM((8, 256, D), BF),
            pltpu.VMEM((TOK, D), BF),
            pltpu.VMEM((ROWS, 2 * TOK), BF),
            pltpu.VMEM((TOK, D), BF),
            pltpu.VMEM((TOK, D), BF),
            pltpu.VMEM((ROWS, HALF), BF),
            pltpu.SemaphoreType.DMA((10,)),
            pltpu.SemaphoreType.DMA((6,)),
        ],
        smem_in=(0,),
        vmem=(4,),
        raw=range(8, 18),
        free=range(11, 18),
        raw_out=(0, 1, 2),
        limit=36,
        flops=2 * 10**9,
    )
    arrived = exchange(plain(send).reshape(experts, 8, HALF), ("sp", "dp"))
    (base,) = call(
        shared_kernel,
        [((TOK, D), F32)],
        (ein, mixed, shared_gate, shared_up, shared_down),
        limit=20,
        flops=4 * 10**9,
    )
    (done,) = call(
        expert_kernel,
        [((ROWS, HALF), BF)],
        (arrived.reshape(ROWS, HALF), expert_gate[0], expert_up[0], expert_down[0]),
        scratch=[
            pltpu.VMEM((ROWS // 2, D), BF),
            pltpu.VMEM((D, 512), BF),
            pltpu.VMEM((D, 512), BF),
            pltpu.VMEM((512, D), BF),
            pltpu.SemaphoreType.DMA((3,)),
        ],
        vmem=(0,),
        raw=(1, 2, 3),
        out_vmem=(0,),
        limit=32,
        flops=3 * 10**9,
    )
    back = exchange(plain(done).reshape(experts, 8, HALF), ("sp", "dp"))
    (out,) = call(
        combine_kernel, [((TOK, D), BF)], (back.reshape(ROWS, HALF), comb, base), vmem=(0,)
    )
    return plain(out)[None]


def solution(mesh):
    rows = P("dp", "sp", None)
    one = P(("sp", "dp"), None, None)
    return jax.shard_map(
        layer,
        mesh=mesh,
        in_specs=(
            (rows,) * 6 + (P(),) * 7 + (P("dp", None),) + (P(),) * 4 + (one,) * 3 + (rows, rows)
        ),
        out_specs=rows,
        check_vma=False,
    )
```

```python
import jax
import jax.numpy as jnp
from jax import lax
from jax._src.core import MemorySpace
from jax._src.state.primitives import with_memory_space_constraint
from jax.experimental import pallas as pl
from jax.experimental.pallas import tpu as pltpu
from jax.sharding import PartitionSpec as P


D = 2048
HEADS = 32
HEAD_DIM = 64
GROUPS = 8
STATE = 128
TOK = 128
EPS = 1e-06
BF = jnp.bfloat16
F32 = jnp.float32
PER = HEADS // GROUPS
GW = PER * HEAD_DIM
HALF = D // 2
ROWS = 1024
ST_ROWS = 160


def full():
    return pl.BlockSpec(memory_space=pltpu.VMEM)


def smem():
    return pl.BlockSpec(memory_space=pltpu.SMEM)


def anywhere():
    return pl.BlockSpec(memory_space=pl.ANY)


def call(
    kernel, outs, args, scratch=(), vmem=(), smem_in=(), raw=(), free=(), out_vmem=(), raw_out=(), limit=12,
    flops=10**6,
):
    placed = [
        v
        if i in smem_in or i in free
        else pltpu.with_memory_space_constraint(v, pltpu.VMEM if i in vmem else pltpu.HBM)
        for i, v in enumerate(args)
    ]
    return pl.pallas_call(
        kernel,
        out_shape=tuple(
            pltpu.VMEM(s, d) if i in out_vmem else pltpu.HBM(s, d)
            for i, (s, d) in enumerate(outs)
        ),
        in_specs=[
            smem() if i in smem_in else anywhere() if i in raw else full() for i in range(len(args))
        ],
        out_specs=tuple(anywhere() if i in raw_out else full() for i in range(len(outs))),
        scratch_shapes=list(scratch),
        compiler_params=pltpu.CompilerParams(vmem_limit_bytes=limit << 20),
        cost_estimate=pl.CostEstimate(flops=flops, bytes_accessed=10**6, transcendentals=0),
    )(*placed)


def silu(v):
    return v / (1.0 + jnp.exp(-v))


def tap(pad, halo, rows, weight):
    out = []
    for i in range(rows.shape[1] // 128):
        cols = slice(i * 128, (i + 1) * 128)
        pad[i, 0:8, :] = jnp.zeros((8, 128), F32) if halo is None else halo[:, cols].astype(F32)
        pad[i, 8 : 8 + TOK, :] = rows[:, cols].astype(F32)
        w = weight[:, cols].astype(F32)
        total = pad[i, 5 : 5 + TOK, :] * w[0:1, :]
        for k in range(1, 4):
            total = total + pad[i, 5 + k : 5 + k + TOK, :] * w[k : k + 1, :]
        out.append(silu(total))
    return jnp.concatenate(out, axis=1) if len(out) > 1 else out[0]


def spread(cols, g):
    lane = lax.broadcasted_iota(jnp.int32, (cols.shape[0], 128), 1)
    out = []
    for i in range(0, PER, 2):
        h = g * PER + i
        out.append(jnp.where(lane < HEAD_DIM, cols[:, h : h + 1], cols[:, h + 1 : h + 2]))
    return jnp.concatenate(out, axis=1)


def states_kernel(
    x, b, c, step_in, cw, cbw, bias, dlog, st, ec_out, grow_out, ends_out, padx, padb, last, sem
):
    load = pltpu.make_async_copy(c.at[pl.ds(TOK - 8, 8), :], last, sem)
    load.start()
    s = step_in[...].astype(F32).T + bias[...]
    step = jnp.maximum(s, 0.0) + jnp.log(1.0 + jnp.exp(-jnp.abs(s)))
    logs = step * (-jnp.exp(dlog[...]))
    r = lax.broadcasted_iota(jnp.int32, (TOK, TOK), 0)
    c = lax.broadcasted_iota(jnp.int32, (TOK, TOK), 1)
    tri = (c <= r).astype(F32)
    cum = jnp.dot(tri, logs, precision=lax.Precision.HIGHEST, preferred_element_type=F32)
    ec_out[...] = jnp.exp(cum)
    grow = step * jnp.exp(-cum)
    grow_out[...] = grow
    later = jnp.where(lax.broadcasted_iota(jnp.int32, (TOK, HEADS), 0) < 3, 0.0, grow)
    tot = cum[TOK - 1 : TOK, :]
    etot = jnp.exp(tot)
    first = grow[0:8, :] * etot
    sub = lax.broadcasted_iota(jnp.int32, (8, 128), 0)
    low = lax.broadcasted_iota(jnp.int32, (8, 128), 1) < HEAD_DIM
    for g in range(GROUPS):
        xc = slice(g * GW, (g + 1) * GW)
        bc = slice(g * STATE, (g + 1) * STATE)
        xs = tap(padx.at[g], None, x[:, xc], cw[:, xc])
        bm = tap(padb.at[g], None, b[:, bc], cbw[:, bc]).astype(BF)
        v = (xs * spread(later, g)).astype(BF)
        fresh = lax.dot_general(v, bm, (((0,), (0,)), ((), ())), preferred_element_type=F32)

        def ends(rows):
            return jnp.where(sub < 3, pltpu.roll(rows[TOK - 8 :], 3, 0), pltpu.roll(rows[:8], 3, 0))

        b_ends = ends(b[:, bc].astype(F32))
        for i in range(2):
            h = g * PER + 2 * i
            o = g * 2 + i
            for j in range(2):
                k = (2 * i + j) * HEAD_DIM
                st[o, j * HEAD_DIM : (j + 1) * HEAD_DIM, :] = (
                    fresh[k : k + HEAD_DIM, :] * etot[0:1, h + j : h + j + 1]
                ).astype(BF)
            tail = jnp.zeros((8, 128), F32)
            for j in range(2):
                rest = jnp.broadcast_to(tot[0:1, h + j : h + j + 1], (8, 128))
                for q in range(3):
                    part = rest.astype(BF).astype(F32)
                    tail = jnp.where(sub == 3 * j + q, part, tail)
                    rest = rest - part
            w = jnp.where(low, first[:, h : h + 1], first[:, h + 1 : h + 2])
            w_hi = w.astype(BF).astype(F32)
            w_both = jnp.where(sub < 3, w_hi, pltpu.roll(w - w_hi, 3, 0))
            x_ends = ends(x[:, o * 128 : (o + 1) * 128].astype(F32))
            st[o, 128:144, :] = jnp.concatenate([tail, w_both], axis=0).astype(BF)
            st[o, 144:160, :] = jnp.concatenate([x_ends, b_ends], axis=0).astype(BF)
    ends_out[:, 0:D] = x[TOK - 8 :, :]
    ends_out[:, D : D + 1024] = b[TOK - 8 :, :]
    load.wait()
    ends_out[:, D + 1024 :] = last[...]


def inner_kernel(x, b, c, halo, cw, cbw, ccw, ec, grow, skip, a_out, c_out, padx, padb, padc):
    r = lax.broadcasted_iota(jnp.int32, (TOK, TOK), 0)
    s = lax.broadcasted_iota(jnp.int32, (TOK, TOK), 1)
    lower = s <= r
    cols = ec[...]
    rows = grow[...]
    sk = jnp.broadcast_to(skip[...], (TOK, HEADS))
    for g in range(GROUPS):
        xc = slice(g * GW, (g + 1) * GW)
        bc = slice(g * STATE, (g + 1) * STATE)
        bh = slice(D + g * STATE, D + (g + 1) * STATE)
        ch = slice(D + 1024 + g * STATE, D + 1024 + (g + 1) * STATE)
        xs = tap(padx.at[g], halo[:, xc], x[:, xc], cw[:, xc])
        bm = tap(padb.at[g], halo[:, bh], b[:, bc], cbw[:, bc]).astype(BF)
        cm = tap(padc.at[g], halo[:, ch], c[:, bc], ccw[:, bc]).astype(BF)
        c_out[:, bc] = cm
        v = (xs * spread(rows, g)).astype(BF)
        cb = lax.dot_general(cm, bm, (((1,), (1,)), ((), ())), preferred_element_type=F32)
        cb = jnp.where(lower, cb, 0.0).astype(BF)
        u = jnp.dot(cb, v, preferred_element_type=F32)
        a_out[:, xc] = u * spread(cols, g) + xs * spread(sk, g)


def carry_kernel(place, cw, cbw, got, out):
    count = got.shape[0]
    o = place[8]
    sub = lax.broadcasted_iota(jnp.int32, (count, 8, 128), 1)

    def starts(rows, weight):
        rows = rows.astype(F32)
        before = jnp.concatenate([jnp.zeros((1, 8, 128), F32), rows[:-1]], axis=0)
        seq = jnp.where(sub < 3, before, rows)
        w = weight.astype(F32)
        total = seq * w[0:1, :][None]
        for k in range(1, 4):
            total = total + pltpu.roll(seq, 8 - k, 1) * w[k : k + 1, :][None]
        return jnp.where(sub < 3, silu(total), 0.0)

    tails = got[:, 128:144, :].astype(F32)
    ends = got[:, 144:160, :].astype(F32)
    w = tails[:, 8:16]
    w = w + pltpu.roll(w, 5, 1)
    xs = starts(ends[:, 0:8], cw[:, pl.ds(pl.multiple_of(o * 128, 128), 128)])
    bm = starts(ends[:, 8:16], cbw[:, pl.ds(pl.multiple_of((o // 2) * 128, 128), 128)])
    vt = jnp.where(sub < 3, xs * w, 0.0).reshape(count * 8, 128).T
    bm = bm.reshape(count * 8, 128).astype(BF)
    lane = lax.broadcasted_iota(jnp.int32, (128, 128), 1)
    row = lax.broadcasted_iota(jnp.int32, (2 * HEAD_DIM, 128), 0)
    carry = jnp.zeros((2 * HEAD_DIM, 128), F32)
    for i in range(count):
        out[i] = carry.astype(BF)
        if i + 1 < count:
            mine = jnp.where(lane // 8 == i, vt, 0.0).astype(BF)
            extra = jnp.dot(mine, bm, preferred_element_type=F32)
            tail = tails[i, 0:8]
            fa = jnp.exp(tail[0:1] + tail[1:2] + tail[2:3])
            fb = jnp.exp(tail[3:4] + tail[4:5] + tail[5:6])
            factor = jnp.where(row < HEAD_DIM, fa, fb)
            carry = carry * factor + (got[i, 0 : 2 * HEAD_DIM, :].astype(F32) + extra)


def slots(routes, rw):
    both = jnp.concatenate([routes[...].astype(F32), rw[...], jnp.zeros((4, TOK), F32)], axis=0).T
    ids = both[:, 0:2].astype(jnp.int32)
    e = lax.broadcasted_iota(jnp.int32, (TOK, 128), 1)
    r = lax.broadcasted_iota(jnp.int32, (TOK, TOK), 0)
    s = lax.broadcasted_iota(jnp.int32, (TOK, TOK), 1)
    tri = (s < r).astype(BF)
    hot = [(ids[:, k : k + 1] == e).astype(F32) for k in range(2)]
    before0 = jnp.dot(tri, hot[0].astype(BF), preferred_element_type=F32)
    before1 = jnp.dot(tri, hot[1].astype(BF), preferred_element_type=F32)
    before1 = before1 + jnp.sum(hot[0], axis=0, keepdims=True)
    pos = [
        jnp.sum(before0 * hot[0], axis=1, keepdims=True).astype(jnp.int32),
        jnp.sum(before1 * hot[1], axis=1, keepdims=True).astype(jnp.int32),
    ]
    return [ids[:, k : k + 1] * 8 + pos[k] for k in range(2)], both[:, 2:4]


def routes_kernel(routes, rw, d_out):
    at, _ = slots(routes, rw)
    lane = lax.broadcasted_iota(jnp.int32, (TOK, ROWS), 1)
    for h in range(2):
        hit = (lane == at[0] + 4 * h) | (lane == at[1] + 4 * h)
        d_out[:, h * TOK : (h + 1) * TOK] = jnp.where(hit, 1.0, 0.0).T.astype(BF)


def weights_kernel(routes, rw, w_out):
    at, w = slots(routes, rw)
    lane = lax.broadcasted_iota(jnp.int32, (TOK, ROWS), 1)
    for h in range(2):
        comb = jnp.where(lane == at[0] + 4 * h, w[:, 0:1], 0.0)
        comb = comb + jnp.where(lane == at[1] + 4 * h, w[:, 1:2], 0.0)
        w_out[h * TOK : (h + 1) * TOK, :] = comb.astype(BF)


def norm_kernel(
    place, a, cm, ec, pref, gate, gain, resid_in, w0, w1, w2, w3, w4, w5, proj, rest,
    norm, wide, picked, resid, sems
):
    loads = [
        pltpu.make_async_copy(w, wide.at[pl.ds(k * GW, GW), :], sems.at[k])
        for k, w in enumerate((w0, w1, w2, w3, w4, w5))
    ]
    loads.append(pltpu.make_async_copy(resid_in, resid, sems.at[6]))
    for load in loads:
        load.start()
    cols = ec[...]
    for g in range(GROUPS):
        xc = slice(g * GW, (g + 1) * GW)
        bc = slice(g * STATE, (g + 1) * STATE)
        outer = lax.dot_general(
            cm[:, bc], pref[g], (((1,), (1,)), ((), ())), preferred_element_type=F32
        )
        y = (a[:, xc] + outer * spread(cols, g)).astype(BF).astype(F32)
        y = y * silu(gate[:, xc].astype(F32))
        y = y * lax.rsqrt(jnp.mean(y * y, axis=1, keepdims=True) + EPS)
        norm[g] = (y * gain[:, xc]).astype(BF)
    for k in range(6):
        picked[:, k * GW : (k + 1) * GW] = norm[place[k]]
    for k in range(2):
        rest[:, k * GW : (k + 1) * GW] = norm[place[6 + k]]
    for load in loads:
        load.wait()
    proj[...] = resid[...].astype(F32) + jnp.dot(
        picked[...], wide[...], preferred_element_type=F32
    )


def mix_kernel(
    proj_in, rest, fgain, disp_in, w6, w7, mixed_out, ein_out, send_out,
    wide, disp, mixed_buf, ein_buf, send, sems, out_sems
):
    loads = [
        pltpu.make_async_copy(w, wide.at[pl.ds(k * GW, GW), :], sems.at[k])
        for k, w in enumerate((w6, w7))
    ]
    loads.append(pltpu.make_async_copy(disp_in, disp, sems.at[2]))
    for load in loads:
        load.start()
    for load in loads[:2]:
        load.wait()
    proj = proj_in[...] + jnp.dot(rest[...], wide[...], preferred_element_type=F32)
    mixed = proj.astype(BF)
    mixed_buf[...] = mixed
    stores = [pltpu.make_async_copy(mixed_buf, mixed_out, out_sems.at[0])]
    stores[0].start()
    m = mixed.astype(F32)
    ein = (m * lax.rsqrt(jnp.mean(m * m, axis=1, keepdims=True) + EPS) * fgain[...]).astype(BF)
    ein_buf[...] = ein
    stores.append(pltpu.make_async_copy(ein_buf, ein_out, out_sems.at[1]))
    stores[1].start()
    stack = jnp.concatenate([ein[:, :HALF], ein[:, HALF:]], axis=0)
    loads[2].wait()
    for q in range(4):
        part = pl.ds(q * 256, 256)
        send[part, :] = jnp.dot(disp[part, :], stack, preferred_element_type=F32).astype(BF)
        store = pltpu.make_async_copy(send.at[part, :], send_out.at[part, :], out_sems.at[2 + q])
        store.start()
        stores.append(store)
    for store in stores:
        store.wait()


def shared_kernel(ein, mixed, sg, su, sd, out):
    x = ein[...]
    gate = jnp.dot(x, sg[...], preferred_element_type=F32)
    up = jnp.dot(x, su[...], preferred_element_type=F32)
    hidden = (silu(gate) * up).astype(BF)
    out[...] = mixed[...].astype(F32) + jnp.dot(hidden, sd[...], preferred_element_type=F32)


def expert_kernel(got, wg_in, wu_in, wd_in, out, xbuf, wg, wu, wd, sems):
    pairs = ((wg_in, wg), (wu_in, wu), (wd_in, wd))
    loads = [pltpu.make_async_copy(v, w, sems.at[k]) for k, (v, w) in enumerate(pairs)]
    for load in loads:
        load.start()
    n = 256
    sub = lax.broadcasted_iota(jnp.int32, (ROWS // 16, 8, n), 1)
    for q in range(HALF // n):
        t = got[:, q * n : (q + 1) * n].astype(F32).reshape(ROWS // 16, 2, 8, n)
        r0, r1 = t[:, 0], t[:, 1]
        x0 = jnp.where(sub < 4, r0, pltpu.roll(r1, 4, 1))
        x1 = jnp.where(sub < 4, pltpu.roll(r0, 4, 1), r1)
        xbuf[:, q * n : (q + 1) * n] = x0.reshape(ROWS // 2, n).astype(BF)
        xbuf[:, HALF + q * n : HALF + (q + 1) * n] = x1.reshape(ROWS // 2, n).astype(BF)
    x = xbuf[...]
    loads[0].wait()
    gate = jnp.dot(x, wg[...], preferred_element_type=F32)
    loads[1].wait()
    up = jnp.dot(x, wu[...], preferred_element_type=F32)
    hidden = (silu(gate) * up).astype(BF)
    loads[2].wait()
    for q in range(HALF // n):
        y0 = jnp.dot(hidden, wd[:, q * n : (q + 1) * n], preferred_element_type=F32)
        y1 = jnp.dot(hidden, wd[:, HALF + q * n : HALF + (q + 1) * n], preferred_element_type=F32)
        y0 = y0.reshape(ROWS // 16, 8, n)
        y1 = y1.reshape(ROWS // 16, 8, n)
        o0 = jnp.where(sub < 4, y0, pltpu.roll(y1, 4, 1))
        o1 = jnp.where(sub < 4, pltpu.roll(y0, 4, 1), y1)
        out[:, q * n : (q + 1) * n] = jnp.stack([o0, o1], axis=1).reshape(ROWS, n).astype(BF)


def combine_kernel(got, w, base, out):
    y = jnp.dot(w[...], got[...], preferred_element_type=F32)
    out[:, :HALF] = (base[:, :HALF] + y[:TOK]).astype(BF)
    out[:, HALF:] = (base[:, HALF:] + y[TOK:]).astype(BF)


def plain(v):
    return with_memory_space_constraint(v, MemorySpace.Device)


def exchange(v, axis):
    return lax.all_to_all(plain(v), axis, split_axis=0, concat_axis=0, tiled=True)


def layer(
    residual, head_input, gate_input, b_input, c_input, step_input, conv_weight,
    conv_b_weight, conv_c_weight, step_bias, decay_log, skip, norm_gain, out_weight,
    ffn_gain, shared_gate, shared_up, shared_down, expert_gate, expert_up, expert_down,
    routes, route_weights,
):
    ways = lax.axis_size("sp")
    dps = lax.axis_size("dp")
    experts = ways * dps
    x, b, c = head_input[0], b_input[0], c_input[0]

    def ring(v):
        return lax.ppermute(v, "dp", [(i, (i + (-2 if i % 2 else 2)) % dps) for i in range(dps)])

    def swap(v):
        return lax.ppermute(v, "dp", [(i, i ^ 1) for i in range(dps)])

    partner = swap(out_weight)
    near = ring(out_weight)
    near2 = ring(partner)
    far = ring(near)
    pieces = [out_weight, partner, near, near2, swap(near), swap(near2)]
    pieces += [far, swap(far)]
    me = lax.axis_index("dp")
    odd = me & 1
    at = (me + dps - 2 + 4 * odd) % dps
    other = ((me ^ 1) + 2 + (dps - 4) * odd) % dps
    place = jnp.stack(
        [me, me ^ 1, at, at ^ 1, other, other ^ 1, me ^ 4, me ^ 5, lax.axis_index("sp")]
    ).astype(jnp.int32)

    st, ec, grow, ends = call(
        states_kernel,
        [((ways, ST_ROWS, 128), BF), ((TOK, HEADS), F32), ((TOK, HEADS), F32), ((8, 4096), BF)],
        (x, b, c, step_input[0].T, conv_weight, conv_b_weight, step_bias[None], decay_log[None]),
        raw=(2,),
        scratch=[
            pltpu.VMEM((GROUPS, 2, TOK + 8, 128), F32),
            pltpu.VMEM((GROUPS, 1, TOK + 8, 128), F32),
            pltpu.VMEM((8, 1024), BF),
            pltpu.SemaphoreType.DMA,
        ],
    )
    got = exchange(st, "sp")
    halo = lax.ppermute(plain(ends), "sp", [(i, i + 1) for i in range(ways - 1)])
    a, cm = call(
        inner_kernel,
        [((TOK, D), F32), ((TOK, 1024), BF)],
        (x, b, c, halo, conv_weight, conv_b_weight, conv_c_weight, ec, grow, skip[None]),
        free=(3,),
        scratch=[
            pltpu.VMEM((GROUPS, 2, TOK + 8, 128), F32),
            pltpu.VMEM((GROUPS, 1, TOK + 8, 128), F32),
            pltpu.VMEM((GROUPS, 1, TOK + 8, 128), F32),
        ],
        flops=4 * 10**9,
    )
    ways_in = (routes[0].T, route_weights[0].T)
    (disp,) = call(routes_kernel, [((ROWS, 2 * TOK), BF)], ways_in, flops=2 * 10**9)
    (comb,) = call(weights_kernel, [((2 * TOK, ROWS), BF)], ways_in, flops=2 * 10**9)
    (carried,) = call(
        carry_kernel,
        [((ways, 128, 128), BF)],
        (place, conv_weight, conv_b_weight, got),
        smem_in=(0,),
        vmem=(3,),
    )
    pref = exchange(carried, "sp")
    proj, rest = call(
        norm_kernel,
        [((TOK, D), F32), ((TOK, 2 * GW), BF)],
        (
            place, a, cm, ec, pref.reshape(GROUPS, GW, STATE), gate_input[0], norm_gain[None],
            residual[0], *pieces[:6],
        ),
        scratch=[
            pltpu.VMEM((GROUPS, TOK, GW), BF),
            pltpu.VMEM((6 * GW, D), BF),
            pltpu.VMEM((TOK, 6 * GW), BF),
            pltpu.VMEM((TOK, D), BF),
            pltpu.SemaphoreType.DMA((7,)),
        ],
        smem_in=(0,),
        vmem=(4,),
        raw=range(7, 14),
        free=range(9, 14),
        out_vmem=(0, 1),
        limit=32,
        flops=2 * 10**9,
    )
    mixed, ein, send = call(
        mix_kernel,
        [((TOK, D), BF), ((TOK, D), BF), ((ROWS, HALF), BF)],
        (proj, rest, ffn_gain[None], disp, *pieces[6:]),
        scratch=[
            pltpu.VMEM((2 * GW, D), BF),
            pltpu.VMEM((ROWS, 2 * TOK), BF),
            pltpu.VMEM((TOK, D), BF),
            pltpu.VMEM((TOK, D), BF),
            pltpu.VMEM((ROWS, HALF), BF),
            pltpu.SemaphoreType.DMA((3,)),
            pltpu.SemaphoreType.DMA((6,)),
        ],
        vmem=(0, 1),
        raw=range(3, 6),
        free=range(4, 6),
        raw_out=(0, 1, 2),
        limit=28,
        flops=2 * 10**9,
    )
    arrived = exchange(plain(send).reshape(experts, 8, HALF), ("sp", "dp"))
    (base,) = call(
        shared_kernel,
        [((TOK, D), F32)],
        (ein, mixed, shared_gate, shared_up, shared_down),
        limit=20,
        flops=4 * 10**9,
    )
    (done,) = call(
        expert_kernel,
        [((ROWS, HALF), BF)],
        (arrived.reshape(ROWS, HALF), expert_gate[0], expert_up[0], expert_down[0]),
        scratch=[
            pltpu.VMEM((ROWS // 2, D), BF),
            pltpu.VMEM((D, 512), BF),
            pltpu.VMEM((D, 512), BF),
            pltpu.VMEM((512, D), BF),
            pltpu.SemaphoreType.DMA((3,)),
        ],
        vmem=(0,),
        raw=(1, 2, 3),
        out_vmem=(0,),
        limit=32,
        flops=3 * 10**9,
    )
    back = exchange(plain(done).reshape(experts, 8, HALF), ("sp", "dp"))
    (out,) = call(
        combine_kernel, [((TOK, D), BF)], (back.reshape(ROWS, HALF), comb, base), vmem=(0,)
    )
    return plain(out)[None]


def solution(mesh):
    rows = P("dp", "sp", None)
    one = P(("sp", "dp"), None, None)
    return jax.shard_map(
        layer,
        mesh=mesh,
        in_specs=(
            (rows,) * 6 + (P(),) * 7 + (P("dp", None),) + (P(),) * 4 + (one,) * 3 + (rows, rows)
        ),
        out_specs=rows,
        check_vma=False,
    )
```

```python
import jax
import jax.numpy as jnp
from jax import lax
from jax._src.core import MemorySpace
from jax._src.state.primitives import with_memory_space_constraint
from jax.experimental import pallas as pl
from jax.experimental.pallas import tpu as pltpu
from jax.sharding import PartitionSpec as P


D = 2048
HEADS = 32
HEAD_DIM = 64
GROUPS = 8
STATE = 128
TOK = 128
EPS = 1e-06
BF = jnp.bfloat16
F32 = jnp.float32
PER = HEADS // GROUPS
GW = PER * HEAD_DIM
HALF = D // 2
ROWS = 1024
ST_ROWS = 160


def full():
    return pl.BlockSpec(memory_space=pltpu.VMEM)


def smem():
    return pl.BlockSpec(memory_space=pltpu.SMEM)


def anywhere():
    return pl.BlockSpec(memory_space=pl.ANY)


def call(
    kernel, outs, args, scratch=(), vmem=(), smem_in=(), raw=(), free=(), out_vmem=(), raw_out=(), limit=12,
    flops=10**6,
):
    placed = [
        v
        if i in smem_in or i in free
        else pltpu.with_memory_space_constraint(v, pltpu.VMEM if i in vmem else pltpu.HBM)
        for i, v in enumerate(args)
    ]
    return pl.pallas_call(
        kernel,
        out_shape=tuple(
            pltpu.VMEM(s, d) if i in out_vmem else pltpu.HBM(s, d)
            for i, (s, d) in enumerate(outs)
        ),
        in_specs=[
            smem() if i in smem_in else anywhere() if i in raw else full() for i in range(len(args))
        ],
        out_specs=tuple(anywhere() if i in raw_out else full() for i in range(len(outs))),
        scratch_shapes=list(scratch),
        compiler_params=pltpu.CompilerParams(vmem_limit_bytes=limit << 20),
        cost_estimate=pl.CostEstimate(flops=flops, bytes_accessed=10**6, transcendentals=0),
    )(*placed)


def silu(v):
    return v / (1.0 + jnp.exp(-v))


def tap(pad, halo, rows, weight):
    out = []
    for i in range(rows.shape[1] // 128):
        cols = slice(i * 128, (i + 1) * 128)
        pad[i, 0:8, :] = jnp.zeros((8, 128), F32) if halo is None else halo[:, cols].astype(F32)
        pad[i, 8 : 8 + TOK, :] = rows[:, cols].astype(F32)
        w = weight[:, cols].astype(F32)
        total = pad[i, 5 : 5 + TOK, :] * w[0:1, :]
        for k in range(1, 4):
            total = total + pad[i, 5 + k : 5 + k + TOK, :] * w[k : k + 1, :]
        out.append(silu(total))
    return jnp.concatenate(out, axis=1) if len(out) > 1 else out[0]


def spread(cols, g):
    lane = lax.broadcasted_iota(jnp.int32, (cols.shape[0], 128), 1)
    out = []
    for i in range(0, PER, 2):
        h = g * PER + i
        out.append(jnp.where(lane < HEAD_DIM, cols[:, h : h + 1], cols[:, h + 1 : h + 2]))
    return jnp.concatenate(out, axis=1)


def begin(pairs, sems):
    copies = [pltpu.make_async_copy(v, w, sems.at[k]) for k, (v, w) in enumerate(pairs)]
    for copy in copies:
        copy.start()
    return copies


def group(g):
    return slice(g * GW, (g + 1) * GW), slice(g * STATE, (g + 1) * STATE)


def part(g, width):
    return pl.ds(g * width, width)


def states_kernel(
    step_in, cw, cbw, bias, dlog, x_in, b_in, c_in, st_out, ec_out, grow_out, ends_out,
    padx, padb, x, b, st, ec, grow_buf, ends_buf, sems, out_sems
):
    pairs = []
    for g in range(GROUPS):
        pairs.append((x_in.at[:, part(g, GW)], x.at[:, part(g, GW)]))
        pairs.append((b_in.at[:, part(g, STATE)], b.at[:, part(g, STATE)]))
    pairs.append((c_in.at[pl.ds(TOK - 8, 8), :], ends_buf.at[:, pl.ds(D + 1024, 1024)]))
    loads = begin(pairs, sems)
    stores = []

    def store(v, w):
        stores.append(pltpu.make_async_copy(v, w, out_sems.at[len(stores)]))
        stores[-1].start()

    s = step_in[...].astype(F32).T + bias[...]
    step = jnp.maximum(s, 0.0) + jnp.log(1.0 + jnp.exp(-jnp.abs(s)))
    logs = step * (-jnp.exp(dlog[...]))
    r = lax.broadcasted_iota(jnp.int32, (TOK, TOK), 0)
    c = lax.broadcasted_iota(jnp.int32, (TOK, TOK), 1)
    tri = (c <= r).astype(F32)
    cum = jnp.dot(tri, logs, precision=lax.Precision.HIGHEST, preferred_element_type=F32)
    ec[...] = jnp.exp(cum)
    store(ec, ec_out)
    grow = step * jnp.exp(-cum)
    grow_buf[...] = grow
    store(grow_buf, grow_out)
    later = jnp.where(lax.broadcasted_iota(jnp.int32, (TOK, HEADS), 0) < 3, 0.0, grow)
    tot = cum[TOK - 1 : TOK, :]
    etot = jnp.exp(tot)
    first = grow[0:8, :] * etot
    sub = lax.broadcasted_iota(jnp.int32, (8, 128), 0)
    low = lax.broadcasted_iota(jnp.int32, (8, 128), 1) < HEAD_DIM
    for g in range(GROUPS):
        xc, bc = group(g)
        loads[2 * g].wait()
        loads[2 * g + 1].wait()
        xs = tap(padx.at[g], None, x[:, xc], cw[:, xc])
        bm = tap(padb.at[g], None, b[:, bc], cbw[:, bc]).astype(BF)
        v = (xs * spread(later, g)).astype(BF)
        fresh = lax.dot_general(v, bm, (((0,), (0,)), ((), ())), preferred_element_type=F32)

        def ends(rows, taps):
            out = jnp.where(sub < 3, pltpu.roll(rows[TOK - 8 :], 3, 0), pltpu.roll(rows[:8], 3, 0))
            return with_taps(out, taps)

        def with_taps(rows, taps):
            taps = taps.astype(F32)
            return jnp.where(sub == 6, taps[0:1], jnp.where(sub == 7, taps[1:2], rows))

        b_taps = cbw[:, bc]
        for i in range(2):
            h = g * PER + 2 * i
            o = g * 2 + i
            for j in range(2):
                k = (2 * i + j) * HEAD_DIM
                st[o, j * HEAD_DIM : (j + 1) * HEAD_DIM, :] = (
                    fresh[k : k + HEAD_DIM, :] * etot[0:1, h + j : h + j + 1]
                ).astype(BF)
            tail = jnp.zeros((8, 128), F32)
            for j in range(2):
                rest = jnp.broadcast_to(tot[0:1, h + j : h + j + 1], (8, 128))
                for q in range(3):
                    piece = rest.astype(BF).astype(F32)
                    tail = jnp.where(sub == 3 * j + q, piece, tail)
                    rest = rest - piece
            w = jnp.where(low, first[:, h : h + 1], first[:, h + 1 : h + 2])
            w_hi = w.astype(BF).astype(F32)
            w_both = jnp.where(sub < 3, w_hi, pltpu.roll(w - w_hi, 3, 0))
            oc = slice(o * 128, (o + 1) * 128)
            tail = with_taps(tail, cw[0:2, oc])
            w_both = with_taps(w_both, cw[2:4, oc])
            x_ends = ends(x[:, oc].astype(F32), b_taps[0:2])
            b_ends = ends(b[:, bc].astype(F32), b_taps[2:4])
            st[o, 128:144, :] = jnp.concatenate([tail, w_both], axis=0).astype(BF)
            st[o, 144:160, :] = jnp.concatenate([x_ends, b_ends], axis=0).astype(BF)
        store(st.at[part(g, 2)], st_out.at[part(g, 2)])
    ends_buf[:, 0:D] = x[TOK - 8 :, :]
    ends_buf[:, D : D + 1024] = b[TOK - 8 :, :]
    loads[-1].wait()
    store(ends_buf, ends_out)
    for copy in stores:
        copy.wait()


def inner_kernel(
    halo, cw, cbw, ccw, ec, grow, skip, routes, rw, x_in, b_in, c_in, a_out, c_out, d_out,
    padx, padb, padc, x, b, c, a_buf, cm_buf, disp, sems, out_sems
):
    pairs = []
    for g in range(GROUPS):
        pairs.append((x_in.at[:, part(g, GW)], x.at[:, part(g, GW)]))
        pairs.append((b_in.at[:, part(g, STATE)], b.at[:, part(g, STATE)]))
        pairs.append((c_in.at[:, part(g, STATE)], c.at[:, part(g, STATE)]))
    loads = begin(pairs, sems)
    at, _ = slots(routes, rw)
    lane = lax.broadcasted_iota(jnp.int32, (TOK, ROWS), 1)
    for h in range(2):
        hit = (lane == at[0] + 4 * h) | (lane == at[1] + 4 * h)
        disp[:, h * TOK : (h + 1) * TOK] = jnp.where(hit, 1.0, 0.0).T.astype(BF)
    stores = [pltpu.make_async_copy(disp, d_out, out_sems.at[0])]
    stores[0].start()
    r = lax.broadcasted_iota(jnp.int32, (TOK, TOK), 0)
    s = lax.broadcasted_iota(jnp.int32, (TOK, TOK), 1)
    lower = s <= r
    cols = ec[...]
    rows = grow[...]
    sk = jnp.broadcast_to(skip[...], (TOK, HEADS))
    for g in range(GROUPS):
        xc, bc = group(g)
        bh = slice(D + g * STATE, D + (g + 1) * STATE)
        ch = slice(D + 1024 + g * STATE, D + 1024 + (g + 1) * STATE)
        for k in range(3):
            loads[3 * g + k].wait()
        xs = tap(padx.at[g], halo[:, xc], x[:, xc], cw[:, xc])
        bm = tap(padb.at[g], halo[:, bh], b[:, bc], cbw[:, bc]).astype(BF)
        cm = tap(padc.at[g], halo[:, ch], c[:, bc], ccw[:, bc]).astype(BF)
        cm_buf[:, bc] = cm
        v = (xs * spread(rows, g)).astype(BF)
        cb = lax.dot_general(cm, bm, (((1,), (1,)), ((), ())), preferred_element_type=F32)
        cb = jnp.where(lower, cb, 0.0).astype(BF)
        u = jnp.dot(cb, v, preferred_element_type=F32)
        a_buf[:, xc] = u * spread(cols, g) + xs * spread(sk, g)
        stores.append(
            pltpu.make_async_copy(
                a_buf.at[:, part(g, GW)], a_out.at[:, part(g, GW)], out_sems.at[1 + g]
            )
        )
        stores[-1].start()
    stores.append(pltpu.make_async_copy(cm_buf, c_out, out_sems.at[1 + GROUPS]))
    stores[-1].start()
    for copy in stores:
        copy.wait()


def carry_kernel(got, out, buf, sems):
    count = got.shape[0]
    sub = lax.broadcasted_iota(jnp.int32, (count, 8, 128), 1)

    def starts(rows, w):
        before = jnp.concatenate([jnp.zeros((1, 8, 128), F32), rows[:-1]], axis=0)
        seq = jnp.where(sub < 3, before, rows)
        total = seq * w[0]
        for k in range(1, 4):
            total = total + pltpu.roll(seq, 8 - k, 1) * w[k]
        return jnp.where(sub < 3, silu(total), 0.0)

    tails = got[:, 128:144, :].astype(F32)
    ends = got[:, 144:160, :].astype(F32)
    w = tails[:, 8:16]
    w = w + pltpu.roll(w, 5, 1)
    x_taps = [tails[0:1, k : k + 1] for k in (6, 7, 14, 15)]
    b_taps = [ends[0:1, k : k + 1] for k in (6, 7, 14, 15)]
    xs = starts(ends[:, 0:8], x_taps)
    bm = starts(ends[:, 8:16], b_taps)
    vt = jnp.where(sub < 3, xs * w, 0.0).reshape(count * 8, 128).T
    bm = bm.reshape(count * 8, 128).astype(BF)
    lane = lax.broadcasted_iota(jnp.int32, (128, 128), 1)
    row = lax.broadcasted_iota(jnp.int32, (2 * HEAD_DIM, 128), 0)
    carry = jnp.zeros((2 * HEAD_DIM, 128), F32)
    stores = []
    for i in range(count):
        buf[i] = carry.astype(BF)
        if i % 4 == 3:
            rows = pl.ds(i - 3, 4)
            stores.append(pltpu.make_async_copy(buf.at[rows], out.at[rows], sems.at[i // 4]))
            stores[-1].start()
        if i + 1 < count:
            mine = jnp.where(lane // 8 == i, vt, 0.0).astype(BF)
            extra = jnp.dot(mine, bm, preferred_element_type=F32)
            tail = tails[i, 0:8]
            fa = jnp.exp(tail[0:1] + tail[1:2] + tail[2:3])
            fb = jnp.exp(tail[3:4] + tail[4:5] + tail[5:6])
            factor = jnp.where(row < HEAD_DIM, fa, fb)
            carry = carry * factor + (got[i, 0 : 2 * HEAD_DIM, :].astype(F32) + extra)
    for copy in stores:
        copy.wait()


def slots(routes, rw):
    both = jnp.concatenate([routes[...].astype(F32), rw[...], jnp.zeros((4, TOK), F32)], axis=0).T
    ids = both[:, 0:2].astype(jnp.int32)
    e = lax.broadcasted_iota(jnp.int32, (TOK, 128), 1)
    r = lax.broadcasted_iota(jnp.int32, (TOK, TOK), 0)
    s = lax.broadcasted_iota(jnp.int32, (TOK, TOK), 1)
    tri = (s < r).astype(BF)
    hot = [(ids[:, k : k + 1] == e).astype(F32) for k in range(2)]
    before0 = jnp.dot(tri, hot[0].astype(BF), preferred_element_type=F32)
    before1 = jnp.dot(tri, hot[1].astype(BF), preferred_element_type=F32)
    before1 = before1 + jnp.sum(hot[0], axis=0, keepdims=True)
    pos = [
        jnp.sum(before0 * hot[0], axis=1, keepdims=True).astype(jnp.int32),
        jnp.sum(before1 * hot[1], axis=1, keepdims=True).astype(jnp.int32),
    ]
    return [ids[:, k : k + 1] * 8 + pos[k] for k in range(2)], both[:, 2:4]


def weights_kernel(routes, rw, w_out):
    at, w = slots(routes, rw)
    lane = lax.broadcasted_iota(jnp.int32, (TOK, ROWS), 1)
    for h in range(2):
        comb = jnp.where(lane == at[0] + 4 * h, w[:, 0:1], 0.0)
        comb = comb + jnp.where(lane == at[1] + 4 * h, w[:, 1:2], 0.0)
        w_out[h * TOK : (h + 1) * TOK, :] = comb.astype(BF)


def norm_kernel(
    place, pref, ec_in, a_in, cm_in, gate_in, gain_in, resid_in, w0, w1, w2, w3, w4, w5, proj, rest,
    norm, wide, picked, ec, a, cm, gate, gain, resid, sems
):
    pairs = [(ec_in, ec), (cm_in, cm), (gain_in, gain)]
    for q in range(4):
        pairs.append((a_in.at[:, part(q, 512)], a.at[:, part(q, 512)]))
        pairs.append((gate_in.at[:, part(q, 512)], gate.at[:, part(q, 512)]))
    for k, w in enumerate((w0, w1, w2, w3, w4, w5)):
        pairs.append((w, wide.at[part(k, GW), :]))
    pairs.append((resid_in, resid))
    loads = begin(pairs, sems)
    for load in loads[:3]:
        load.wait()
    cols = ec[...]
    for g in range(GROUPS):
        xc, bc = group(g)
        if g % 2 == 0:
            loads[3 + g].wait()
            loads[4 + g].wait()
        outer = lax.dot_general(
            cm[:, bc], pref[g], (((1,), (1,)), ((), ())), preferred_element_type=F32
        )
        y = (a[:, xc] + outer * spread(cols, g)).astype(BF).astype(F32)
        y = y * silu(gate[:, xc].astype(F32))
        y = y * lax.rsqrt(jnp.mean(y * y, axis=1, keepdims=True) + EPS)
        norm[g] = (y * gain[:, xc]).astype(BF)
    for k in range(6):
        picked[:, k * GW : (k + 1) * GW] = norm[place[k]]
    for k in range(2):
        rest[:, k * GW : (k + 1) * GW] = norm[place[6 + k]]
    for load in loads[11:]:
        load.wait()
    proj[...] = resid[...].astype(F32) + jnp.dot(
        picked[...], wide[...], preferred_element_type=F32
    )


def mix_kernel(
    proj_in, rest, fgain_in, disp_in, w6, w7, mixed_out, ein_out, send_out,
    wide, fgain, disp, mixed_buf, ein_buf, send, sems, out_sems
):
    pairs = [(w6, wide.at[part(0, GW), :]), (w7, wide.at[part(1, GW), :])]
    loads = begin(pairs + [(fgain_in, fgain), (disp_in, disp)], sems)
    for load in loads[:2]:
        load.wait()
    proj = proj_in[...] + jnp.dot(rest[...], wide[...], preferred_element_type=F32)
    loads[2].wait()
    mixed = proj.astype(BF)
    mixed_buf[...] = mixed
    stores = [pltpu.make_async_copy(mixed_buf, mixed_out, out_sems.at[0])]
    stores[0].start()
    m = mixed.astype(F32)
    ein = (m * lax.rsqrt(jnp.mean(m * m, axis=1, keepdims=True) + EPS) * fgain[...]).astype(BF)
    ein_buf[...] = ein
    stores.append(pltpu.make_async_copy(ein_buf, ein_out, out_sems.at[1]))
    stores[1].start()
    stack = jnp.concatenate([ein[:, :HALF], ein[:, HALF:]], axis=0)
    loads[3].wait()
    for q in range(4):
        rows = part(q, 256)
        send[rows, :] = jnp.dot(disp[rows, :], stack, preferred_element_type=F32).astype(BF)
        store = pltpu.make_async_copy(send.at[rows, :], send_out.at[rows, :], out_sems.at[2 + q])
        store.start()
        stores.append(store)
    for store in stores:
        store.wait()


def shared_kernel(ein, mixed, sg, su, sd, out):
    x = ein[...]
    gate = jnp.dot(x, sg[...], preferred_element_type=F32)
    up = jnp.dot(x, su[...], preferred_element_type=F32)
    hidden = (silu(gate) * up).astype(BF)
    out[...] = mixed[...].astype(F32) + jnp.dot(hidden, sd[...], preferred_element_type=F32)


def expert_kernel(got, wg_in, wu_in, wd_in, out, xbuf, wg, wu, wd, sems):
    pairs = ((wg_in, wg), (wu_in, wu), (wd_in, wd))
    loads = [pltpu.make_async_copy(v, w, sems.at[k]) for k, (v, w) in enumerate(pairs)]
    for load in loads:
        load.start()
    n = 256
    sub = lax.broadcasted_iota(jnp.int32, (ROWS // 16, 8, n), 1)
    for q in range(HALF // n):
        t = got[:, q * n : (q + 1) * n].astype(F32).reshape(ROWS // 16, 2, 8, n)
        r0, r1 = t[:, 0], t[:, 1]
        x0 = jnp.where(sub < 4, r0, pltpu.roll(r1, 4, 1))
        x1 = jnp.where(sub < 4, pltpu.roll(r0, 4, 1), r1)
        xbuf[:, q * n : (q + 1) * n] = x0.reshape(ROWS // 2, n).astype(BF)
        xbuf[:, HALF + q * n : HALF + (q + 1) * n] = x1.reshape(ROWS // 2, n).astype(BF)
    x = xbuf[...]
    loads[0].wait()
    gate = jnp.dot(x, wg[...], preferred_element_type=F32)
    loads[1].wait()
    up = jnp.dot(x, wu[...], preferred_element_type=F32)
    hidden = (silu(gate) * up).astype(BF)
    loads[2].wait()
    for q in range(HALF // n):
        y0 = jnp.dot(hidden, wd[:, q * n : (q + 1) * n], preferred_element_type=F32)
        y1 = jnp.dot(hidden, wd[:, HALF + q * n : HALF + (q + 1) * n], preferred_element_type=F32)
        y0 = y0.reshape(ROWS // 16, 8, n)
        y1 = y1.reshape(ROWS // 16, 8, n)
        o0 = jnp.where(sub < 4, y0, pltpu.roll(y1, 4, 1))
        o1 = jnp.where(sub < 4, pltpu.roll(y0, 4, 1), y1)
        out[:, q * n : (q + 1) * n] = jnp.stack([o0, o1], axis=1).reshape(ROWS, n).astype(BF)


def combine_kernel(got, w_in, base_in, out_ref, w, base, out, sems, out_sems):
    loads = begin([(w_in, w), (base_in, base)], sems)
    loads[0].wait()
    stores = []
    for h in range(2):
        cols = part(h, HALF)
        y = jnp.dot(w[part(h, TOK), :], got[...], preferred_element_type=F32)
        if h == 0:
            loads[1].wait()
        out[:, cols] = (base[:, cols] + y).astype(BF)
        stores.append(pltpu.make_async_copy(out.at[:, cols], out_ref.at[:, cols], out_sems.at[h]))
        stores[h].start()
    for copy in stores:
        copy.wait()


def plain(v):
    return with_memory_space_constraint(v, MemorySpace.Device)


def exchange(v, axis):
    return lax.all_to_all(plain(v), axis, split_axis=0, concat_axis=0, tiled=True)


def layer(
    residual, head_input, gate_input, b_input, c_input, step_input, conv_weight,
    conv_b_weight, conv_c_weight, step_bias, decay_log, skip, norm_gain, out_weight,
    ffn_gain, shared_gate, shared_up, shared_down, expert_gate, expert_up, expert_down,
    routes, route_weights,
):
    ways = lax.axis_size("sp")
    dps = lax.axis_size("dp")
    experts = ways * dps
    x, b, c = head_input[0], b_input[0], c_input[0]

    def ring(v):
        return lax.ppermute(v, "dp", [(i, (i + (-2 if i % 2 else 2)) % dps) for i in range(dps)])

    def swap(v):
        return lax.ppermute(v, "dp", [(i, i ^ 1) for i in range(dps)])

    partner = swap(out_weight)
    near = ring(out_weight)
    near2 = ring(partner)
    far = ring(near)
    pieces = [out_weight, partner, near, near2, swap(near), swap(near2)]
    pieces += [far, swap(far)]
    me = lax.axis_index("dp")
    odd = me & 1
    at = (me + dps - 2 + 4 * odd) % dps
    other = ((me ^ 1) + 2 + (dps - 4) * odd) % dps
    place = jnp.stack(
        [me, me ^ 1, at, at ^ 1, other, other ^ 1, me ^ 4, me ^ 5]
    ).astype(jnp.int32)

    st, ec, grow, ends = call(
        states_kernel,
        [((ways, ST_ROWS, 128), BF), ((TOK, HEADS), F32), ((TOK, HEADS), F32), ((8, 4096), BF)],
        (step_input[0].T, conv_weight, conv_b_weight, step_bias[None], decay_log[None], x, b, c),
        raw=(5, 6, 7),
        raw_out=range(4),
        scratch=[
            pltpu.VMEM((GROUPS, 2, TOK + 8, 128), F32),
            pltpu.VMEM((GROUPS, 1, TOK + 8, 128), F32),
            pltpu.VMEM((TOK, D), BF),
            pltpu.VMEM((TOK, 1024), BF),
            pltpu.VMEM((ways, ST_ROWS, 128), BF),
            pltpu.VMEM((TOK, HEADS), F32),
            pltpu.VMEM((TOK, HEADS), F32),
            pltpu.VMEM((8, 4096), BF),
            pltpu.SemaphoreType.DMA((17,)),
            pltpu.SemaphoreType.DMA((11,)),
        ],
    )
    got = exchange(st, "sp")
    halo = lax.ppermute(plain(ends), "sp", [(i, i + 1) for i in range(ways - 1)])
    ways_in = (routes[0].T, route_weights[0].T)
    a, cm, disp = call(
        inner_kernel,
        [((TOK, D), F32), ((TOK, 1024), BF), ((ROWS, 2 * TOK), BF)],
        (
            halo, conv_weight, conv_b_weight, conv_c_weight, ec, grow, skip[None], *ways_in,
            x, b, c,
        ),
        free=(0,),
        raw=(9, 10, 11),
        raw_out=range(3),
        scratch=[
            pltpu.VMEM((GROUPS, 2, TOK + 8, 128), F32),
            pltpu.VMEM((GROUPS, 1, TOK + 8, 128), F32),
            pltpu.VMEM((GROUPS, 1, TOK + 8, 128), F32),
            pltpu.VMEM((TOK, D), BF),
            pltpu.VMEM((TOK, 1024), BF),
            pltpu.VMEM((TOK, 1024), BF),
            pltpu.VMEM((TOK, D), F32),
            pltpu.VMEM((TOK, 1024), BF),
            pltpu.VMEM((ROWS, 2 * TOK), BF),
            pltpu.SemaphoreType.DMA((24,)),
            pltpu.SemaphoreType.DMA((10,)),
        ],
        flops=4 * 10**9,
    )
    (comb,) = call(weights_kernel, [((2 * TOK, ROWS), BF)], ways_in, flops=2 * 10**9)
    (carried,) = call(
        carry_kernel,
        [((ways, 128, 128), BF)],
        (got,),
        vmem=(0,),
        raw_out=(0,),
        scratch=[pltpu.VMEM((ways, 128, 128), BF), pltpu.SemaphoreType.DMA((4,))],
    )
    pref = exchange(carried, "sp")
    proj, rest = call(
        norm_kernel,
        [((TOK, D), F32), ((TOK, 2 * GW), BF)],
        (
            place, pref.reshape(GROUPS, GW, STATE), ec, a, cm, gate_input[0], norm_gain[None],
            residual[0], *pieces[:6],
        ),
        scratch=[
            pltpu.VMEM((GROUPS, TOK, GW), BF),
            pltpu.VMEM((6 * GW, D), BF),
            pltpu.VMEM((TOK, 6 * GW), BF),
            pltpu.VMEM((TOK, HEADS), F32),
            pltpu.VMEM((TOK, D), F32),
            pltpu.VMEM((TOK, 1024), BF),
            pltpu.VMEM((TOK, D), BF),
            pltpu.VMEM((1, D), F32),
            pltpu.VMEM((TOK, D), BF),
            pltpu.SemaphoreType.DMA((18,)),
        ],
        smem_in=(0,),
        vmem=(1,),
        raw=range(2, 14),
        free=range(9, 14),
        out_vmem=(0, 1),
        limit=32,
        flops=2 * 10**9,
    )
    mixed, ein, send = call(
        mix_kernel,
        [((TOK, D), BF), ((TOK, D), BF), ((ROWS, HALF), BF)],
        (proj, rest, ffn_gain[None], disp, *pieces[6:]),
        scratch=[
            pltpu.VMEM((2 * GW, D), BF),
            pltpu.VMEM((1, D), F32),
            pltpu.VMEM((ROWS, 2 * TOK), BF),
            pltpu.VMEM((TOK, D), BF),
            pltpu.VMEM((TOK, D), BF),
            pltpu.VMEM((ROWS, HALF), BF),
            pltpu.SemaphoreType.DMA((4,)),
            pltpu.SemaphoreType.DMA((6,)),
        ],
        vmem=(0, 1),
        raw=range(2, 6),
        free=range(4, 6),
        raw_out=(0, 1, 2),
        limit=28,
        flops=2 * 10**9,
    )
    arrived = exchange(plain(send).reshape(experts, 8, HALF), ("sp", "dp"))
    (base,) = call(
        shared_kernel,
        [((TOK, D), F32)],
        (ein, mixed, shared_gate, shared_up, shared_down),
        limit=20,
        flops=4 * 10**9,
    )
    (done,) = call(
        expert_kernel,
        [((ROWS, HALF), BF)],
        (arrived.reshape(ROWS, HALF), expert_gate[0], expert_up[0], expert_down[0]),
        scratch=[
            pltpu.VMEM((ROWS // 2, D), BF),
            pltpu.VMEM((D, 512), BF),
            pltpu.VMEM((D, 512), BF),
            pltpu.VMEM((512, D), BF),
            pltpu.SemaphoreType.DMA((3,)),
        ],
        vmem=(0,),
        raw=(1, 2, 3),
        out_vmem=(0,),
        limit=32,
        flops=3 * 10**9,
    )
    back = exchange(plain(done).reshape(experts, 8, HALF), ("sp", "dp"))
    (out,) = call(
        combine_kernel,
        [((TOK, D), BF)],
        (back.reshape(ROWS, HALF), comb, base),
        vmem=(0,),
        raw=(1, 2),
        raw_out=(0,),
        scratch=[
            pltpu.VMEM((2 * TOK, ROWS), BF),
            pltpu.VMEM((TOK, D), F32),
            pltpu.VMEM((TOK, D), BF),
            pltpu.SemaphoreType.DMA((2,)),
            pltpu.SemaphoreType.DMA((2,)),
        ],
    )
    return plain(out)[None]


def solution(mesh):
    rows = P("dp", "sp", None)
    one = P(("sp", "dp"), None, None)
    return jax.shard_map(
        layer,
        mesh=mesh,
        in_specs=(
            (rows,) * 6 + (P(),) * 7 + (P("dp", None),) + (P(),) * 4 + (one,) * 3 + (rows, rows)
        ),
        out_specs=rows,
        check_vma=False,
    )
```

```python
import jax
import jax.numpy as jnp
from jax import lax
from jax._src.core import MemorySpace
from jax._src.state.primitives import with_memory_space_constraint
from jax.experimental import pallas as pl
from jax.experimental.pallas import tpu as pltpu
from jax.sharding import PartitionSpec as P


D = 2048
HEADS = 32
HEAD_DIM = 64
GROUPS = 8
STATE = 128
TOK = 128
EPS = 1e-06
BF = jnp.bfloat16
F32 = jnp.float32
PER = HEADS // GROUPS
GW = PER * HEAD_DIM
HALF = D // 2
ROWS = 1024
ST_ROWS = 160


def full():
    return pl.BlockSpec(memory_space=pltpu.VMEM)


def smem():
    return pl.BlockSpec(memory_space=pltpu.SMEM)


def anywhere():
    return pl.BlockSpec(memory_space=pl.ANY)


def call(
    kernel, outs, args, scratch=(), vmem=(), smem_in=(), raw=(), free=(), out_vmem=(), raw_out=(), limit=12,
    flops=10**6,
):
    placed = [
        v
        if i in smem_in or i in free
        else pltpu.with_memory_space_constraint(v, pltpu.VMEM if i in vmem else pltpu.HBM)
        for i, v in enumerate(args)
    ]
    return pl.pallas_call(
        kernel,
        out_shape=tuple(
            pltpu.VMEM(s, d) if i in out_vmem else pltpu.HBM(s, d)
            for i, (s, d) in enumerate(outs)
        ),
        in_specs=[
            smem() if i in smem_in else anywhere() if i in raw else full() for i in range(len(args))
        ],
        out_specs=tuple(anywhere() if i in raw_out else full() for i in range(len(outs))),
        scratch_shapes=list(scratch),
        compiler_params=pltpu.CompilerParams(vmem_limit_bytes=limit << 20),
        cost_estimate=pl.CostEstimate(flops=flops, bytes_accessed=10**6, transcendentals=0),
    )(*placed)


def silu(v):
    return v / (1.0 + jnp.exp(-v))


def tap(pad, halo, rows, weight):
    out = []
    for i in range(rows.shape[1] // 128):
        cols = slice(i * 128, (i + 1) * 128)
        pad[i, 0:8, :] = jnp.zeros((8, 128), F32) if halo is None else halo[:, cols].astype(F32)
        pad[i, 8 : 8 + TOK, :] = rows[:, cols].astype(F32)
        w = weight[:, cols].astype(F32)
        total = pad[i, 5 : 5 + TOK, :] * w[0:1, :]
        for k in range(1, 4):
            total = total + pad[i, 5 + k : 5 + k + TOK, :] * w[k : k + 1, :]
        out.append(silu(total))
    return jnp.concatenate(out, axis=1) if len(out) > 1 else out[0]


def spread(cols, g):
    lane = lax.broadcasted_iota(jnp.int32, (cols.shape[0], 128), 1)
    out = []
    for i in range(0, PER, 2):
        h = g * PER + i
        out.append(jnp.where(lane < HEAD_DIM, cols[:, h : h + 1], cols[:, h + 1 : h + 2]))
    return jnp.concatenate(out, axis=1)


def begin(pairs, sems):
    copies = [pltpu.make_async_copy(v, w, sems.at[k]) for k, (v, w) in enumerate(pairs)]
    for copy in copies:
        copy.start()
    return copies


def group(g):
    return slice(g * GW, (g + 1) * GW), slice(g * STATE, (g + 1) * STATE)


def part(g, width):
    return pl.ds(g * width, width)


def states_kernel(
    step_in, cw, cbw, bias, dlog, x, b, c, st, ec, grow_out, ends_out, padx, padb, sem
):
    load = pltpu.make_async_copy(
        c.at[pl.ds(TOK - 8, 8), :], ends_out.at[:, pl.ds(D + 1024, 1024)], sem
    )
    load.start()
    s = step_in[...].astype(F32).T + bias[...]
    step = jnp.maximum(s, 0.0) + jnp.log(1.0 + jnp.exp(-jnp.abs(s)))
    logs = step * (-jnp.exp(dlog[...]))
    r = lax.broadcasted_iota(jnp.int32, (TOK, TOK), 0)
    c = lax.broadcasted_iota(jnp.int32, (TOK, TOK), 1)
    tri = (c <= r).astype(F32)
    cum = jnp.dot(tri, logs, precision=lax.Precision.HIGHEST, preferred_element_type=F32)
    ec[...] = jnp.exp(cum)
    grow = step * jnp.exp(-cum)
    grow_out[...] = grow
    later = jnp.where(lax.broadcasted_iota(jnp.int32, (TOK, HEADS), 0) < 3, 0.0, grow)
    tot = cum[TOK - 1 : TOK, :]
    etot = jnp.exp(tot)
    first = grow[0:8, :] * etot
    sub = lax.broadcasted_iota(jnp.int32, (8, 128), 0)
    low = lax.broadcasted_iota(jnp.int32, (8, 128), 1) < HEAD_DIM
    for g in range(GROUPS):
        xc, bc = group(g)
        xs = tap(padx.at[g], None, x[:, xc], cw[:, xc])
        bm = tap(padb.at[g], None, b[:, bc], cbw[:, bc]).astype(BF)
        v = (xs * spread(later, g)).astype(BF)
        fresh = lax.dot_general(v, bm, (((0,), (0,)), ((), ())), preferred_element_type=F32)

        def ends(rows, taps):
            out = jnp.where(sub < 3, pltpu.roll(rows[TOK - 8 :], 3, 0), pltpu.roll(rows[:8], 3, 0))
            return with_taps(out, taps)

        def with_taps(rows, taps):
            taps = taps.astype(F32)
            return jnp.where(sub == 6, taps[0:1], jnp.where(sub == 7, taps[1:2], rows))

        b_taps = cbw[:, bc]
        for i in range(2):
            h = g * PER + 2 * i
            o = g * 2 + i
            for j in range(2):
                k = (2 * i + j) * HEAD_DIM
                st[o, j * HEAD_DIM : (j + 1) * HEAD_DIM, :] = (
                    fresh[k : k + HEAD_DIM, :] * etot[0:1, h + j : h + j + 1]
                ).astype(BF)
            tail = jnp.zeros((8, 128), F32)
            for j in range(2):
                rest = jnp.broadcast_to(tot[0:1, h + j : h + j + 1], (8, 128))
                for q in range(3):
                    piece = rest.astype(BF).astype(F32)
                    tail = jnp.where(sub == 3 * j + q, piece, tail)
                    rest = rest - piece
            w = jnp.where(low, first[:, h : h + 1], first[:, h + 1 : h + 2])
            w_hi = w.astype(BF).astype(F32)
            w_both = jnp.where(sub < 3, w_hi, pltpu.roll(w - w_hi, 3, 0))
            oc = slice(o * 128, (o + 1) * 128)
            tail = with_taps(tail, cw[0:2, oc])
            w_both = with_taps(w_both, cw[2:4, oc])
            x_ends = ends(x[:, oc].astype(F32), b_taps[0:2])
            b_ends = ends(b[:, bc].astype(F32), b_taps[2:4])
            st[o, 128:144, :] = jnp.concatenate([tail, w_both], axis=0).astype(BF)
            st[o, 144:160, :] = jnp.concatenate([x_ends, b_ends], axis=0).astype(BF)
    ends_out[:, 0:D] = x[TOK - 8 :, :]
    ends_out[:, D : D + 1024] = b[TOK - 8 :, :]
    load.wait()


def inner_kernel(x, b, c, halo, cw, cbw, ccw, ec, grow, skip, a_out, c_out, padx, padb, padc):
    r = lax.broadcasted_iota(jnp.int32, (TOK, TOK), 0)
    s = lax.broadcasted_iota(jnp.int32, (TOK, TOK), 1)
    lower = s <= r
    cols = ec[...]
    rows = grow[...]
    sk = jnp.broadcast_to(skip[...], (TOK, HEADS))
    for g in range(GROUPS):
        xc = slice(g * GW, (g + 1) * GW)
        bc = slice(g * STATE, (g + 1) * STATE)
        bh = slice(D + g * STATE, D + (g + 1) * STATE)
        ch = slice(D + 1024 + g * STATE, D + 1024 + (g + 1) * STATE)
        xs = tap(padx.at[g], halo[:, xc], x[:, xc], cw[:, xc])
        bm = tap(padb.at[g], halo[:, bh], b[:, bc], cbw[:, bc]).astype(BF)
        cm = tap(padc.at[g], halo[:, ch], c[:, bc], ccw[:, bc]).astype(BF)
        c_out[:, bc] = cm
        v = (xs * spread(rows, g)).astype(BF)
        cb = lax.dot_general(cm, bm, (((1,), (1,)), ((), ())), preferred_element_type=F32)
        cb = jnp.where(lower, cb, 0.0).astype(BF)
        u = jnp.dot(cb, v, preferred_element_type=F32)
        a_out[:, xc] = u * spread(cols, g) + xs * spread(sk, g)


def carry_kernel(got, out, buf, sems):
    count = got.shape[0]
    sub = lax.broadcasted_iota(jnp.int32, (count, 8, 128), 1)

    def starts(rows, w):
        before = jnp.concatenate([jnp.zeros((1, 8, 128), F32), rows[:-1]], axis=0)
        seq = jnp.where(sub < 3, before, rows)
        total = seq * w[0]
        for k in range(1, 4):
            total = total + pltpu.roll(seq, 8 - k, 1) * w[k]
        return jnp.where(sub < 3, silu(total), 0.0)

    tails = got[:, 128:144, :].astype(F32)
    ends = got[:, 144:160, :].astype(F32)
    w = tails[:, 8:16]
    w = w + pltpu.roll(w, 5, 1)
    x_taps = [tails[0:1, k : k + 1] for k in (6, 7, 14, 15)]
    b_taps = [ends[0:1, k : k + 1] for k in (6, 7, 14, 15)]
    xs = starts(ends[:, 0:8], x_taps)
    bm = starts(ends[:, 8:16], b_taps)
    vt = jnp.where(sub < 3, xs * w, 0.0).reshape(count * 8, 128).T
    bm = bm.reshape(count * 8, 128).astype(BF)
    lane = lax.broadcasted_iota(jnp.int32, (128, 128), 1)
    row = lax.broadcasted_iota(jnp.int32, (2 * HEAD_DIM, 128), 0)
    carry = jnp.zeros((2 * HEAD_DIM, 128), F32)
    stores = []
    for i in range(count):
        buf[i] = carry.astype(BF)
        if i % 4 == 3:
            rows = pl.ds(i - 3, 4)
            stores.append(pltpu.make_async_copy(buf.at[rows], out.at[rows], sems.at[i // 4]))
            stores[-1].start()
        if i + 1 < count:
            mine = jnp.where(lane // 8 == i, vt, 0.0).astype(BF)
            extra = jnp.dot(mine, bm, preferred_element_type=F32)
            tail = tails[i, 0:8]
            fa = jnp.exp(tail[0:1] + tail[1:2] + tail[2:3])
            fb = jnp.exp(tail[3:4] + tail[4:5] + tail[5:6])
            factor = jnp.where(row < HEAD_DIM, fa, fb)
            carry = carry * factor + (got[i, 0 : 2 * HEAD_DIM, :].astype(F32) + extra)
    for copy in stores:
        copy.wait()


def slots(routes, rw):
    both = jnp.concatenate([routes[...].astype(F32), rw[...], jnp.zeros((4, TOK), F32)], axis=0).T
    ids = both[:, 0:2].astype(jnp.int32)
    e = lax.broadcasted_iota(jnp.int32, (TOK, 128), 1)
    r = lax.broadcasted_iota(jnp.int32, (TOK, TOK), 0)
    s = lax.broadcasted_iota(jnp.int32, (TOK, TOK), 1)
    tri = (s < r).astype(BF)
    hot = [(ids[:, k : k + 1] == e).astype(F32) for k in range(2)]
    before0 = jnp.dot(tri, hot[0].astype(BF), preferred_element_type=F32)
    before1 = jnp.dot(tri, hot[1].astype(BF), preferred_element_type=F32)
    before1 = before1 + jnp.sum(hot[0], axis=0, keepdims=True)
    pos = [
        jnp.sum(before0 * hot[0], axis=1, keepdims=True).astype(jnp.int32),
        jnp.sum(before1 * hot[1], axis=1, keepdims=True).astype(jnp.int32),
    ]
    return [ids[:, k : k + 1] * 8 + pos[k] for k in range(2)], both[:, 2:4]


def routes_kernel(routes, rw, d_out):
    at, _ = slots(routes, rw)
    lane = lax.broadcasted_iota(jnp.int32, (TOK, ROWS), 1)
    for h in range(2):
        hit = (lane == at[0] + 4 * h) | (lane == at[1] + 4 * h)
        d_out[:, h * TOK : (h + 1) * TOK] = jnp.where(hit, 1.0, 0.0).T.astype(BF)


def weights_kernel(routes, rw, w_out):
    at, w = slots(routes, rw)
    lane = lax.broadcasted_iota(jnp.int32, (TOK, ROWS), 1)
    for h in range(2):
        comb = jnp.where(lane == at[0] + 4 * h, w[:, 0:1], 0.0)
        comb = comb + jnp.where(lane == at[1] + 4 * h, w[:, 1:2], 0.0)
        w_out[h * TOK : (h + 1) * TOK, :] = comb.astype(BF)


def norm_kernel(
    pref, ec_in, a_in, cm_in, gate_in, gain_in, resid_in, w0, w1, w2, w3, w4, w5, proj, rest,
    norm, wide, picked, ec, a, cm, gate, gain, resid, sems
):
    pairs = [(ec_in, ec), (cm_in, cm), (gain_in, gain)]
    for q in range(4):
        pairs.append((a_in.at[:, part(q, 512)], a.at[:, part(q, 512)]))
        pairs.append((gate_in.at[:, part(q, 512)], gate.at[:, part(q, 512)]))
    for k, w in enumerate((w0, w1, w2, w3, w4, w5)):
        pairs.append((w, wide.at[part(k, GW), :]))
    pairs.append((resid_in, resid))
    loads = begin(pairs, sems)
    for load in loads[:3]:
        load.wait()
    cols = ec[...]
    for g in range(GROUPS):
        xc, bc = group(g)
        if g % 2 == 0:
            loads[3 + g].wait()
            loads[4 + g].wait()
        outer = lax.dot_general(
            cm[:, bc], pref[g], (((1,), (1,)), ((), ())), preferred_element_type=F32
        )
        y = (a[:, xc] + outer * spread(cols, g)).astype(BF).astype(F32)
        y = y * silu(gate[:, xc].astype(F32))
        y = y * lax.rsqrt(jnp.mean(y * y, axis=1, keepdims=True) + EPS)
        norm[g] = (y * gain[:, xc]).astype(BF)
    me = lax.axis_index("dp")
    odd = me & 1
    at = (me + 6 + 4 * odd) & 7
    other = ((me ^ 1) + 6 - 4 * odd + 4) & 7
    place = [me, me ^ 1, at, at ^ 1, other, other ^ 1, me ^ 4, me ^ 5]
    for k in range(6):
        picked[:, k * GW : (k + 1) * GW] = norm[place[k]]
    for k in range(2):
        rest[:, k * GW : (k + 1) * GW] = norm[place[6 + k]]
    for load in loads[11:]:
        load.wait()
    proj[...] = resid[...].astype(F32) + jnp.dot(
        picked[...], wide[...], preferred_element_type=F32
    )


def mix_kernel(
    proj_in, rest, fgain_in, disp_in, w6, w7, mixed_out, ein_out, send_out,
    wide, fgain, disp, mixed_buf, ein_buf, send, sems, out_sems
):
    pairs = [(w6, wide.at[part(0, GW), :]), (w7, wide.at[part(1, GW), :])]
    loads = begin(pairs + [(fgain_in, fgain), (disp_in, disp)], sems)
    for load in loads[:2]:
        load.wait()
    proj = proj_in[...] + jnp.dot(rest[...], wide[...], preferred_element_type=F32)
    loads[2].wait()
    mixed = proj.astype(BF)
    mixed_buf[...] = mixed
    stores = [pltpu.make_async_copy(mixed_buf, mixed_out, out_sems.at[0])]
    stores[0].start()
    m = mixed.astype(F32)
    ein = (m * lax.rsqrt(jnp.mean(m * m, axis=1, keepdims=True) + EPS) * fgain[...]).astype(BF)
    ein_buf[...] = ein
    stores.append(pltpu.make_async_copy(ein_buf, ein_out, out_sems.at[1]))
    stores[1].start()
    stack = jnp.concatenate([ein[:, :HALF], ein[:, HALF:]], axis=0)
    loads[3].wait()
    for q in range(4):
        rows = part(q, 256)
        send[rows, :] = jnp.dot(disp[rows, :], stack, preferred_element_type=F32).astype(BF)
        store = pltpu.make_async_copy(send.at[rows, :], send_out.at[rows, :], out_sems.at[2 + q])
        store.start()
        stores.append(store)
    for store in stores:
        store.wait()


def shared_kernel(ein, mixed, sg, su, sd, out):
    x = ein[...]
    gate = jnp.dot(x, sg[...], preferred_element_type=F32)
    up = jnp.dot(x, su[...], preferred_element_type=F32)
    hidden = (silu(gate) * up).astype(BF)
    out[...] = mixed[...].astype(F32) + jnp.dot(hidden, sd[...], preferred_element_type=F32)


def expert_kernel(got, wg_in, wu_in, wd_in, out, xbuf, wg, wu, wd, sems):
    pairs = ((wg_in, wg), (wu_in, wu), (wd_in, wd))
    loads = [pltpu.make_async_copy(v, w, sems.at[k]) for k, (v, w) in enumerate(pairs)]
    for load in loads:
        load.start()
    n = 256
    sub = lax.broadcasted_iota(jnp.int32, (ROWS // 16, 8, n), 1)
    for q in range(HALF // n):
        t = got[:, q * n : (q + 1) * n].astype(F32).reshape(ROWS // 16, 2, 8, n)
        r0, r1 = t[:, 0], t[:, 1]
        x0 = jnp.where(sub < 4, r0, pltpu.roll(r1, 4, 1))
        x1 = jnp.where(sub < 4, pltpu.roll(r0, 4, 1), r1)
        xbuf[:, q * n : (q + 1) * n] = x0.reshape(ROWS // 2, n).astype(BF)
        xbuf[:, HALF + q * n : HALF + (q + 1) * n] = x1.reshape(ROWS // 2, n).astype(BF)
    x = xbuf[...]
    loads[0].wait()
    gate = jnp.dot(x, wg[...], preferred_element_type=F32)
    loads[1].wait()
    up = jnp.dot(x, wu[...], preferred_element_type=F32)
    hidden = (silu(gate) * up).astype(BF)
    loads[2].wait()
    for q in range(HALF // n):
        y0 = jnp.dot(hidden, wd[:, q * n : (q + 1) * n], preferred_element_type=F32)
        y1 = jnp.dot(hidden, wd[:, HALF + q * n : HALF + (q + 1) * n], preferred_element_type=F32)
        y0 = y0.reshape(ROWS // 16, 8, n)
        y1 = y1.reshape(ROWS // 16, 8, n)
        o0 = jnp.where(sub < 4, y0, pltpu.roll(y1, 4, 1))
        o1 = jnp.where(sub < 4, pltpu.roll(y0, 4, 1), y1)
        out[:, q * n : (q + 1) * n] = jnp.stack([o0, o1], axis=1).reshape(ROWS, n).astype(BF)


def combine_kernel(got, w_in, base_in, out_ref, w, base, out, sems, out_sems):
    loads = begin([(w_in, w), (base_in, base)], sems)
    loads[0].wait()
    stores = []
    for h in range(2):
        cols = part(h, HALF)
        y = jnp.dot(w[part(h, TOK), :], got[...], preferred_element_type=F32)
        if h == 0:
            loads[1].wait()
        out[:, cols] = (base[:, cols] + y).astype(BF)
        stores.append(pltpu.make_async_copy(out.at[:, cols], out_ref.at[:, cols], out_sems.at[h]))
        stores[h].start()
    for copy in stores:
        copy.wait()


def plain(v):
    return with_memory_space_constraint(v, MemorySpace.Device)


def exchange(v, axis):
    return lax.all_to_all(plain(v), axis, split_axis=0, concat_axis=0, tiled=True)


def layer(
    residual, head_input, gate_input, b_input, c_input, step_input, conv_weight,
    conv_b_weight, conv_c_weight, step_bias, decay_log, skip, norm_gain, out_weight,
    ffn_gain, shared_gate, shared_up, shared_down, expert_gate, expert_up, expert_down,
    routes, route_weights,
):
    ways = lax.axis_size("sp")
    dps = lax.axis_size("dp")
    experts = ways * dps
    x, b, c = head_input[0], b_input[0], c_input[0]

    def ring(v):
        return lax.ppermute(v, "dp", [(i, (i + (-2 if i % 2 else 2)) % dps) for i in range(dps)])

    def swap(v):
        return lax.ppermute(v, "dp", [(i, i ^ 1) for i in range(dps)])

    partner = swap(out_weight)
    near = ring(out_weight)
    near2 = ring(partner)
    far = ring(near)
    pieces = [out_weight, partner, near, near2, swap(near), swap(near2)]
    pieces += [far, swap(far)]
    st, ec, grow, ends = call(
        states_kernel,
        [((ways, ST_ROWS, 128), BF), ((TOK, HEADS), F32), ((TOK, HEADS), F32), ((8, 4096), BF)],
        (step_input[0].T, conv_weight, conv_b_weight, step_bias[None], decay_log[None], x, b, c),
        raw=(7,),
        scratch=[
            pltpu.VMEM((GROUPS, 2, TOK + 8, 128), F32),
            pltpu.VMEM((GROUPS, 1, TOK + 8, 128), F32),
            pltpu.SemaphoreType.DMA,
        ],
    )
    got = exchange(st, "sp")
    halo = lax.ppermute(plain(ends), "sp", [(i, i + 1) for i in range(ways - 1)])
    a, cm = call(
        inner_kernel,
        [((TOK, D), F32), ((TOK, 1024), BF)],
        (x, b, c, halo, conv_weight, conv_b_weight, conv_c_weight, ec, grow, skip[None]),
        free=(3,),
        scratch=[
            pltpu.VMEM((GROUPS, 2, TOK + 8, 128), F32),
            pltpu.VMEM((GROUPS, 1, TOK + 8, 128), F32),
            pltpu.VMEM((GROUPS, 1, TOK + 8, 128), F32),
        ],
        flops=4 * 10**9,
    )
    ways_in = (routes[0].T, route_weights[0].T)
    (disp,) = call(routes_kernel, [((ROWS, 2 * TOK), BF)], ways_in, flops=2 * 10**9)
    (comb,) = call(weights_kernel, [((2 * TOK, ROWS), BF)], ways_in, flops=2 * 10**9)
    (carried,) = call(
        carry_kernel,
        [((ways, 128, 128), BF)],
        (got,),
        vmem=(0,),
        raw_out=(0,),
        scratch=[pltpu.VMEM((ways, 128, 128), BF), pltpu.SemaphoreType.DMA((4,))],
    )
    pref = exchange(carried, "sp")
    proj, rest = call(
        norm_kernel,
        [((TOK, D), F32), ((TOK, 2 * GW), BF)],
        (
            pref.reshape(GROUPS, GW, STATE), ec, a, cm, gate_input[0], norm_gain[None],
            residual[0], *pieces[:6],
        ),
        scratch=[
            pltpu.VMEM((GROUPS, TOK, GW), BF),
            pltpu.VMEM((6 * GW, D), BF),
            pltpu.VMEM((TOK, 6 * GW), BF),
            pltpu.VMEM((TOK, HEADS), F32),
            pltpu.VMEM((TOK, D), F32),
            pltpu.VMEM((TOK, 1024), BF),
            pltpu.VMEM((TOK, D), BF),
            pltpu.VMEM((1, D), F32),
            pltpu.VMEM((TOK, D), BF),
            pltpu.SemaphoreType.DMA((18,)),
        ],
        vmem=(0,),
        raw=range(1, 13),
        free=range(8, 13),
        out_vmem=(0, 1),
        limit=32,
        flops=2 * 10**9,
    )
    mixed, ein, send = call(
        mix_kernel,
        [((TOK, D), BF), ((TOK, D), BF), ((ROWS, HALF), BF)],
        (proj, rest, ffn_gain[None], disp, *pieces[6:]),
        scratch=[
            pltpu.VMEM((2 * GW, D), BF),
            pltpu.VMEM((1, D), F32),
            pltpu.VMEM((ROWS, 2 * TOK), BF),
            pltpu.VMEM((TOK, D), BF),
            pltpu.VMEM((TOK, D), BF),
            pltpu.VMEM((ROWS, HALF), BF),
            pltpu.SemaphoreType.DMA((4,)),
            pltpu.SemaphoreType.DMA((6,)),
        ],
        vmem=(0, 1),
        raw=range(2, 6),
        free=range(4, 6),
        raw_out=(0, 1, 2),
        limit=28,
        flops=2 * 10**9,
    )
    arrived = exchange(plain(send).reshape(experts, 8, HALF), ("sp", "dp"))
    (base,) = call(
        shared_kernel,
        [((TOK, D), F32)],
        (ein, mixed, shared_gate, shared_up, shared_down),
        limit=20,
        flops=4 * 10**9,
    )
    (done,) = call(
        expert_kernel,
        [((ROWS, HALF), BF)],
        (arrived.reshape(ROWS, HALF), expert_gate[0], expert_up[0], expert_down[0]),
        scratch=[
            pltpu.VMEM((ROWS // 2, D), BF),
            pltpu.VMEM((D, 512), BF),
            pltpu.VMEM((D, 512), BF),
            pltpu.VMEM((512, D), BF),
            pltpu.SemaphoreType.DMA((3,)),
        ],
        vmem=(0,),
        raw=(1, 2, 3),
        out_vmem=(0,),
        limit=32,
        flops=3 * 10**9,
    )
    back = exchange(plain(done).reshape(experts, 8, HALF), ("sp", "dp"))
    (out,) = call(
        combine_kernel,
        [((TOK, D), BF)],
        (back.reshape(ROWS, HALF), comb, base),
        vmem=(0,),
        raw=(1, 2),
        raw_out=(0,),
        scratch=[
            pltpu.VMEM((2 * TOK, ROWS), BF),
            pltpu.VMEM((TOK, D), F32),
            pltpu.VMEM((TOK, D), BF),
            pltpu.SemaphoreType.DMA((2,)),
            pltpu.SemaphoreType.DMA((2,)),
        ],
    )
    return plain(out)[None]


def solution(mesh):
    rows = P("dp", "sp", None)
    one = P(("sp", "dp"), None, None)
    return jax.shard_map(
        layer,
        mesh=mesh,
        in_specs=(
            (rows,) * 6 + (P(),) * 7 + (P("dp", None),) + (P(),) * 4 + (one,) * 3 + (rows, rows)
        ),
        out_specs=rows,
        check_vma=False,
    )
```

```python
import jax
import jax.numpy as jnp
from jax import lax
from jax._src.core import MemorySpace
from jax._src.state.primitives import with_memory_space_constraint
from jax.experimental import pallas as pl
from jax.experimental.pallas import tpu as pltpu
from jax.sharding import PartitionSpec as P


D = 2048
HEADS = 32
HEAD_DIM = 64
GROUPS = 8
STATE = 128
TOK = 128
EPS = 1e-06
BF = jnp.bfloat16
F32 = jnp.float32
PER = HEADS // GROUPS
GW = PER * HEAD_DIM
HALF = D // 2
ROWS = 1024
ST_ROWS = 160


def full():
    return pl.BlockSpec(memory_space=pltpu.VMEM)


def smem():
    return pl.BlockSpec(memory_space=pltpu.SMEM)


def anywhere():
    return pl.BlockSpec(memory_space=pl.ANY)


def call(
    kernel, outs, args, scratch=(), vmem=(), smem_in=(), raw=(), free=(), out_vmem=(), raw_out=(), limit=12,
    flops=10**6,
):
    placed = [
        v
        if i in smem_in or i in free
        else pltpu.with_memory_space_constraint(v, pltpu.VMEM if i in vmem else pltpu.HBM)
        for i, v in enumerate(args)
    ]
    return pl.pallas_call(
        kernel,
        out_shape=tuple(
            pltpu.VMEM(s, d) if i in out_vmem else pltpu.HBM(s, d)
            for i, (s, d) in enumerate(outs)
        ),
        in_specs=[
            smem() if i in smem_in else anywhere() if i in raw else full() for i in range(len(args))
        ],
        out_specs=tuple(anywhere() if i in raw_out else full() for i in range(len(outs))),
        scratch_shapes=list(scratch),
        compiler_params=pltpu.CompilerParams(vmem_limit_bytes=limit << 20),
        cost_estimate=pl.CostEstimate(flops=flops, bytes_accessed=10**6, transcendentals=0),
    )(*placed)


def silu(v):
    return v / (1.0 + jnp.exp(-v))


def tap(pad, halo, rows, weight):
    out = []
    for i in range(rows.shape[1] // 128):
        cols = slice(i * 128, (i + 1) * 128)
        pad[i, 0:8, :] = jnp.zeros((8, 128), F32) if halo is None else halo[:, cols].astype(F32)
        pad[i, 8 : 8 + TOK, :] = rows[:, cols].astype(F32)
        w = weight[:, cols].astype(F32)
        total = pad[i, 5 : 5 + TOK, :] * w[0:1, :]
        for k in range(1, 4):
            total = total + pad[i, 5 + k : 5 + k + TOK, :] * w[k : k + 1, :]
        out.append(silu(total))
    return jnp.concatenate(out, axis=1) if len(out) > 1 else out[0]


def spread(cols, g):
    lane = lax.broadcasted_iota(jnp.int32, (cols.shape[0], 128), 1)
    out = []
    for i in range(0, PER, 2):
        h = g * PER + i
        out.append(jnp.where(lane < HEAD_DIM, cols[:, h : h + 1], cols[:, h + 1 : h + 2]))
    return jnp.concatenate(out, axis=1)


def begin(pairs, sems):
    copies = [pltpu.make_async_copy(v, w, sems.at[k]) for k, (v, w) in enumerate(pairs)]
    for copy in copies:
        copy.start()
    return copies


def group(g):
    return slice(g * GW, (g + 1) * GW), slice(g * STATE, (g + 1) * STATE)


def part(g, width):
    return pl.ds(g * width, width)


def states_kernel(
    step_in, cw, cbw, bias, dlog, x, b, c, st, ec, grow_out, ends_out, padx, padb, sem
):
    load = pltpu.make_async_copy(
        c.at[pl.ds(TOK - 8, 8), :], ends_out.at[:, pl.ds(D + 1024, 1024)], sem
    )
    load.start()
    s = step_in[...].astype(F32).T + bias[...]
    step = jnp.maximum(s, 0.0) + jnp.log(1.0 + jnp.exp(-jnp.abs(s)))
    logs = step * (-jnp.exp(dlog[...]))
    r = lax.broadcasted_iota(jnp.int32, (TOK, TOK), 0)
    c = lax.broadcasted_iota(jnp.int32, (TOK, TOK), 1)
    tri = (c <= r).astype(F32)
    cum = jnp.dot(tri, logs, precision=lax.Precision.HIGHEST, preferred_element_type=F32)
    ec[...] = jnp.exp(cum)
    grow = step * jnp.exp(-cum)
    grow_out[...] = grow
    later = jnp.where(lax.broadcasted_iota(jnp.int32, (TOK, HEADS), 0) < 3, 0.0, grow)
    tot = cum[TOK - 1 : TOK, :]
    etot = jnp.exp(tot)
    first = grow[0:8, :] * etot
    sub = lax.broadcasted_iota(jnp.int32, (8, 128), 0)
    low = lax.broadcasted_iota(jnp.int32, (8, 128), 1) < HEAD_DIM
    for g in range(GROUPS):
        xc, bc = group(g)
        xs = tap(padx.at[g], None, x[:, xc], cw[:, xc])
        bm = tap(padb.at[g], None, b[:, bc], cbw[:, bc]).astype(BF)
        v = (xs * spread(later, g)).astype(BF)
        fresh = lax.dot_general(v, bm, (((0,), (0,)), ((), ())), preferred_element_type=F32)

        def ends(rows, taps):
            out = jnp.where(sub < 3, pltpu.roll(rows[TOK - 8 :], 3, 0), pltpu.roll(rows[:8], 3, 0))
            return with_taps(out, taps)

        def with_taps(rows, taps):
            taps = taps.astype(F32)
            return jnp.where(sub == 6, taps[0:1], jnp.where(sub == 7, taps[1:2], rows))

        b_taps = cbw[:, bc]
        for i in range(2):
            h = g * PER + 2 * i
            o = g * 2 + i
            for j in range(2):
                k = (2 * i + j) * HEAD_DIM
                st[o, j * HEAD_DIM : (j + 1) * HEAD_DIM, :] = (
                    fresh[k : k + HEAD_DIM, :] * etot[0:1, h + j : h + j + 1]
                ).astype(BF)
            tail = jnp.zeros((8, 128), F32)
            for j in range(2):
                rest = jnp.broadcast_to(tot[0:1, h + j : h + j + 1], (8, 128))
                for q in range(3):
                    piece = rest.astype(BF).astype(F32)
                    tail = jnp.where(sub == 3 * j + q, piece, tail)
                    rest = rest - piece
            w = jnp.where(low, first[:, h : h + 1], first[:, h + 1 : h + 2])
            w_hi = w.astype(BF).astype(F32)
            w_both = jnp.where(sub < 3, w_hi, pltpu.roll(w - w_hi, 3, 0))
            oc = slice(o * 128, (o + 1) * 128)
            tail = with_taps(tail, cw[0:2, oc])
            w_both = with_taps(w_both, cw[2:4, oc])
            x_ends = ends(x[:, oc].astype(F32), b_taps[0:2])
            b_ends = ends(b[:, bc].astype(F32), b_taps[2:4])
            st[o, 128:144, :] = jnp.concatenate([tail, w_both], axis=0).astype(BF)
            st[o, 144:160, :] = jnp.concatenate([x_ends, b_ends], axis=0).astype(BF)
    ends_out[:, 0:D] = x[TOK - 8 :, :]
    ends_out[:, D : D + 1024] = b[TOK - 8 :, :]
    load.wait()


def inner_kernel(x, b, c, halo, cw, cbw, ccw, ec, grow, skip, a_out, c_out, padx, padb, padc):
    r = lax.broadcasted_iota(jnp.int32, (TOK, TOK), 0)
    s = lax.broadcasted_iota(jnp.int32, (TOK, TOK), 1)
    lower = s <= r
    cols = ec[...]
    rows = grow[...]
    sk = jnp.broadcast_to(skip[...], (TOK, HEADS))
    for g in range(GROUPS):
        xc = slice(g * GW, (g + 1) * GW)
        bc = slice(g * STATE, (g + 1) * STATE)
        bh = slice(D + g * STATE, D + (g + 1) * STATE)
        ch = slice(D + 1024 + g * STATE, D + 1024 + (g + 1) * STATE)
        xs = tap(padx.at[g], halo[:, xc], x[:, xc], cw[:, xc])
        bm = tap(padb.at[g], halo[:, bh], b[:, bc], cbw[:, bc]).astype(BF)
        cm = tap(padc.at[g], halo[:, ch], c[:, bc], ccw[:, bc]).astype(BF)
        c_out[:, bc] = cm
        v = (xs * spread(rows, g)).astype(BF)
        cb = lax.dot_general(cm, bm, (((1,), (1,)), ((), ())), preferred_element_type=F32)
        cb = jnp.where(lower, cb, 0.0).astype(BF)
        u = jnp.dot(cb, v, preferred_element_type=F32)
        a_out[:, xc] = u * spread(cols, g) + xs * spread(sk, g)


def carry_kernel(got, out, buf, sems):
    count = got.shape[0]
    sub = lax.broadcasted_iota(jnp.int32, (count, 8, 128), 1)

    def starts(rows, w):
        before = jnp.concatenate([jnp.zeros((1, 8, 128), F32), rows[:-1]], axis=0)
        seq = jnp.where(sub < 3, before, rows)
        total = seq * w[0]
        for k in range(1, 4):
            total = total + pltpu.roll(seq, 8 - k, 1) * w[k]
        return jnp.where(sub < 3, silu(total), 0.0)

    tails = got[:, 128:144, :].astype(F32)
    ends = got[:, 144:160, :].astype(F32)
    w = tails[:, 8:16]
    w = w + pltpu.roll(w, 5, 1)
    x_taps = [tails[0:1, k : k + 1] for k in (6, 7, 14, 15)]
    b_taps = [ends[0:1, k : k + 1] for k in (6, 7, 14, 15)]
    xs = starts(ends[:, 0:8], x_taps)
    bm = starts(ends[:, 8:16], b_taps)
    vt = jnp.where(sub < 3, xs * w, 0.0).reshape(count * 8, 128).T
    bm = bm.reshape(count * 8, 128).astype(BF)
    lane = lax.broadcasted_iota(jnp.int32, (128, 128), 1)
    row = lax.broadcasted_iota(jnp.int32, (2 * HEAD_DIM, 128), 0)
    carry = jnp.zeros((2 * HEAD_DIM, 128), F32)
    stores = []
    for i in range(count):
        buf[i] = carry.astype(BF)
        if i % 4 == 3:
            rows = pl.ds(i - 3, 4)
            stores.append(pltpu.make_async_copy(buf.at[rows], out.at[rows], sems.at[i // 4]))
            stores[-1].start()
        if i + 1 < count:
            mine = jnp.where(lane // 8 == i, vt, 0.0).astype(BF)
            extra = jnp.dot(mine, bm, preferred_element_type=F32)
            tail = tails[i, 0:8]
            fa = jnp.exp(tail[0:1] + tail[1:2] + tail[2:3])
            fb = jnp.exp(tail[3:4] + tail[4:5] + tail[5:6])
            factor = jnp.where(row < HEAD_DIM, fa, fb)
            carry = carry * factor + (got[i, 0 : 2 * HEAD_DIM, :].astype(F32) + extra)
    for copy in stores:
        copy.wait()


def slots(routes, rw):
    both = jnp.concatenate([routes[...].astype(F32), rw[...], jnp.zeros((4, TOK), F32)], axis=0).T
    ids = both[:, 0:2].astype(jnp.int32)
    e = lax.broadcasted_iota(jnp.int32, (TOK, 128), 1)
    r = lax.broadcasted_iota(jnp.int32, (TOK, TOK), 0)
    s = lax.broadcasted_iota(jnp.int32, (TOK, TOK), 1)
    tri = (s < r).astype(BF)
    hot = [(ids[:, k : k + 1] == e).astype(F32) for k in range(2)]
    before0 = jnp.dot(tri, hot[0].astype(BF), preferred_element_type=F32)
    before1 = jnp.dot(tri, hot[1].astype(BF), preferred_element_type=F32)
    before1 = before1 + jnp.sum(hot[0], axis=0, keepdims=True)
    pos = [
        jnp.sum(before0 * hot[0], axis=1, keepdims=True).astype(jnp.int32),
        jnp.sum(before1 * hot[1], axis=1, keepdims=True).astype(jnp.int32),
    ]
    return [ids[:, k : k + 1] * 8 + pos[k] for k in range(2)], both[:, 2:4]


def routes_kernel(routes, rw, d_out):
    at, _ = slots(routes, rw)
    lane = lax.broadcasted_iota(jnp.int32, (TOK, ROWS), 1)
    for h in range(2):
        hit = (lane == at[0] + 4 * h) | (lane == at[1] + 4 * h)
        d_out[:, h * TOK : (h + 1) * TOK] = jnp.where(hit, 1.0, 0.0).T.astype(BF)


def weights_kernel(routes, rw, w_out):
    at, w = slots(routes, rw)
    lane = lax.broadcasted_iota(jnp.int32, (TOK, ROWS), 1)
    for h in range(2):
        comb = jnp.where(lane == at[0] + 4 * h, w[:, 0:1], 0.0)
        comb = comb + jnp.where(lane == at[1] + 4 * h, w[:, 1:2], 0.0)
        w_out[h * TOK : (h + 1) * TOK, :] = comb.astype(BF)


def norm_kernel(
    pref, ec_in, a_in, cm_in, gate_in, gain_in, resid_in, w0, w1, w2, w3, w4, w5, w6, proj, rest,
    norm, wide, picked, ec, a, cm, gate, gain, resid, sems
):
    pairs = [(ec_in, ec), (cm_in, cm), (gain_in, gain)]
    for q in range(4):
        pairs.append((a_in.at[:, part(q, 512)], a.at[:, part(q, 512)]))
        pairs.append((gate_in.at[:, part(q, 512)], gate.at[:, part(q, 512)]))
    for k, w in enumerate((w0, w1, w2, w3, w4, w5, w6)):
        pairs.append((w, wide.at[part(k, GW), :]))
    pairs.append((resid_in, resid))
    loads = begin(pairs, sems)
    for load in loads[:3]:
        load.wait()
    cols = ec[...]
    for g in range(GROUPS):
        xc, bc = group(g)
        if g % 2 == 0:
            loads[3 + g].wait()
            loads[4 + g].wait()
        outer = lax.dot_general(
            cm[:, bc], pref[g], (((1,), (1,)), ((), ())), preferred_element_type=F32
        )
        y = (a[:, xc] + outer * spread(cols, g)).astype(BF).astype(F32)
        y = y * silu(gate[:, xc].astype(F32))
        y = y * lax.rsqrt(jnp.mean(y * y, axis=1, keepdims=True) + EPS)
        norm[g] = (y * gain[:, xc]).astype(BF)
    me = lax.axis_index("dp")
    odd = me & 1
    at = (me + 6 + 4 * odd) & 7
    other = ((me ^ 1) + 6 - 4 * odd + 4) & 7
    place = [me, me ^ 1, at, at ^ 1, other, other ^ 1, me ^ 4, me ^ 5]
    for k in range(7):
        picked[:, k * GW : (k + 1) * GW] = norm[place[k]]
    rest[...] = norm[place[7]]
    for load in loads[11:]:
        load.wait()
    proj[...] = resid[...].astype(F32) + jnp.dot(
        picked[...], wide[...], preferred_element_type=F32
    )


def mix_kernel(
    proj_in, rest, fgain_in, disp_in, w7, mixed_out, ein_out, send_out,
    wide, fgain, disp, mixed_buf, ein_buf, send, sems, out_sems
):
    loads = begin([(w7, wide), (fgain_in, fgain), (disp_in, disp)], sems)
    loads[0].wait()
    proj = proj_in[...] + jnp.dot(rest[...], wide[...], preferred_element_type=F32)
    loads[1].wait()
    mixed = proj.astype(BF)
    mixed_buf[...] = mixed
    stores = [pltpu.make_async_copy(mixed_buf, mixed_out, out_sems.at[0])]
    stores[0].start()
    m = mixed.astype(F32)
    ein = (m * lax.rsqrt(jnp.mean(m * m, axis=1, keepdims=True) + EPS) * fgain[...]).astype(BF)
    ein_buf[...] = ein
    stores.append(pltpu.make_async_copy(ein_buf, ein_out, out_sems.at[1]))
    stores[1].start()
    stack = jnp.concatenate([ein[:, :HALF], ein[:, HALF:]], axis=0)
    loads[2].wait()
    for q in range(4):
        rows = part(q, 256)
        send[rows, :] = jnp.dot(disp[rows, :], stack, preferred_element_type=F32).astype(BF)
        store = pltpu.make_async_copy(send.at[rows, :], send_out.at[rows, :], out_sems.at[2 + q])
        store.start()
        stores.append(store)
    for store in stores:
        store.wait()


def shared_kernel(ein, mixed, sg, su, sd, out):
    x = ein[...]
    gate = jnp.dot(x, sg[...], preferred_element_type=F32)
    up = jnp.dot(x, su[...], preferred_element_type=F32)
    hidden = (silu(gate) * up).astype(BF)
    out[...] = mixed[...].astype(F32) + jnp.dot(hidden, sd[...], preferred_element_type=F32)


def expert_kernel(got, wg_in, wu_in, wd_in, out, xbuf, wg, wu, wd, sems):
    pairs = ((wg_in, wg), (wu_in, wu), (wd_in, wd))
    loads = [pltpu.make_async_copy(v, w, sems.at[k]) for k, (v, w) in enumerate(pairs)]
    for load in loads:
        load.start()
    n = 256
    sub = lax.broadcasted_iota(jnp.int32, (ROWS // 16, 8, n), 1)
    for q in range(HALF // n):
        t = got[:, q * n : (q + 1) * n].astype(F32).reshape(ROWS // 16, 2, 8, n)
        r0, r1 = t[:, 0], t[:, 1]
        x0 = jnp.where(sub < 4, r0, pltpu.roll(r1, 4, 1))
        x1 = jnp.where(sub < 4, pltpu.roll(r0, 4, 1), r1)
        xbuf[:, q * n : (q + 1) * n] = x0.reshape(ROWS // 2, n).astype(BF)
        xbuf[:, HALF + q * n : HALF + (q + 1) * n] = x1.reshape(ROWS // 2, n).astype(BF)
    x = xbuf[...]
    loads[0].wait()
    gate = jnp.dot(x, wg[...], preferred_element_type=F32)
    loads[1].wait()
    up = jnp.dot(x, wu[...], preferred_element_type=F32)
    hidden = (silu(gate) * up).astype(BF)
    loads[2].wait()
    for q in range(HALF // n):
        y0 = jnp.dot(hidden, wd[:, q * n : (q + 1) * n], preferred_element_type=F32)
        y1 = jnp.dot(hidden, wd[:, HALF + q * n : HALF + (q + 1) * n], preferred_element_type=F32)
        y0 = y0.reshape(ROWS // 16, 8, n)
        y1 = y1.reshape(ROWS // 16, 8, n)
        o0 = jnp.where(sub < 4, y0, pltpu.roll(y1, 4, 1))
        o1 = jnp.where(sub < 4, pltpu.roll(y0, 4, 1), y1)
        out[:, q * n : (q + 1) * n] = jnp.stack([o0, o1], axis=1).reshape(ROWS, n).astype(BF)


def combine_kernel(got, w_in, base_in, out_ref, w, base, out, sems, out_sems):
    loads = begin([(w_in, w), (base_in, base)], sems)
    loads[0].wait()
    stores = []
    for h in range(2):
        cols = part(h, HALF)
        y = jnp.dot(w[part(h, TOK), :], got[...], preferred_element_type=F32)
        if h == 0:
            loads[1].wait()
        out[:, cols] = (base[:, cols] + y).astype(BF)
        stores.append(pltpu.make_async_copy(out.at[:, cols], out_ref.at[:, cols], out_sems.at[h]))
        stores[h].start()
    for copy in stores:
        copy.wait()


def plain(v):
    return with_memory_space_constraint(v, MemorySpace.Device)


def exchange(v, axis):
    return lax.all_to_all(plain(v), axis, split_axis=0, concat_axis=0, tiled=True)


def layer(
    residual, head_input, gate_input, b_input, c_input, step_input, conv_weight,
    conv_b_weight, conv_c_weight, step_bias, decay_log, skip, norm_gain, out_weight,
    ffn_gain, shared_gate, shared_up, shared_down, expert_gate, expert_up, expert_down,
    routes, route_weights,
):
    ways = lax.axis_size("sp")
    dps = lax.axis_size("dp")
    experts = ways * dps
    x, b, c = head_input[0], b_input[0], c_input[0]

    def ring(v):
        return lax.ppermute(v, "dp", [(i, (i + (-2 if i % 2 else 2)) % dps) for i in range(dps)])

    def swap(v):
        return lax.ppermute(v, "dp", [(i, i ^ 1) for i in range(dps)])

    partner = swap(out_weight)
    near = ring(out_weight)
    near2 = ring(partner)
    far = ring(near)
    pieces = [out_weight, partner, near, near2, swap(near), swap(near2)]
    pieces += [far, swap(far)]
    st, ec, grow, ends = call(
        states_kernel,
        [((ways, ST_ROWS, 128), BF), ((TOK, HEADS), F32), ((TOK, HEADS), F32), ((8, 4096), BF)],
        (step_input[0].T, conv_weight, conv_b_weight, step_bias[None], decay_log[None], x, b, c),
        raw=(7,),
        scratch=[
            pltpu.VMEM((GROUPS, 2, TOK + 8, 128), F32),
            pltpu.VMEM((GROUPS, 1, TOK + 8, 128), F32),
            pltpu.SemaphoreType.DMA,
        ],
    )
    got = exchange(st, "sp")
    halo = lax.ppermute(plain(ends), "sp", [(i, i + 1) for i in range(ways - 1)])
    a, cm = call(
        inner_kernel,
        [((TOK, D), F32), ((TOK, 1024), BF)],
        (x, b, c, halo, conv_weight, conv_b_weight, conv_c_weight, ec, grow, skip[None]),
        free=(3,),
        scratch=[
            pltpu.VMEM((GROUPS, 2, TOK + 8, 128), F32),
            pltpu.VMEM((GROUPS, 1, TOK + 8, 128), F32),
            pltpu.VMEM((GROUPS, 1, TOK + 8, 128), F32),
        ],
        flops=4 * 10**9,
    )
    ways_in = (routes[0].T, route_weights[0].T)
    (disp,) = call(routes_kernel, [((ROWS, 2 * TOK), BF)], ways_in, flops=2 * 10**9)
    (comb,) = call(weights_kernel, [((2 * TOK, ROWS), BF)], ways_in, flops=2 * 10**9)
    (carried,) = call(
        carry_kernel,
        [((ways, 128, 128), BF)],
        (got,),
        vmem=(0,),
        raw_out=(0,),
        scratch=[pltpu.VMEM((ways, 128, 128), BF), pltpu.SemaphoreType.DMA((4,))],
    )
    pref = exchange(carried, "sp")
    proj, rest = call(
        norm_kernel,
        [((TOK, D), F32), ((TOK, GW), BF)],
        (
            pref.reshape(GROUPS, GW, STATE), ec, a, cm, gate_input[0], norm_gain[None],
            residual[0], *pieces[:7],
        ),
        scratch=[
            pltpu.VMEM((GROUPS, TOK, GW), BF),
            pltpu.VMEM((7 * GW, D), BF),
            pltpu.VMEM((TOK, 7 * GW), BF),
            pltpu.VMEM((TOK, HEADS), F32),
            pltpu.VMEM((TOK, D), F32),
            pltpu.VMEM((TOK, 1024), BF),
            pltpu.VMEM((TOK, D), BF),
            pltpu.VMEM((1, D), F32),
            pltpu.VMEM((TOK, D), BF),
            pltpu.SemaphoreType.DMA((19,)),
        ],
        vmem=(0,),
        raw=range(1, 14),
        free=range(8, 14),
        out_vmem=(0, 1),
        limit=32,
        flops=2 * 10**9,
    )
    mixed, ein, send = call(
        mix_kernel,
        [((TOK, D), BF), ((TOK, D), BF), ((ROWS, HALF), BF)],
        (proj, rest, ffn_gain[None], disp, *pieces[7:]),
        scratch=[
            pltpu.VMEM((GW, D), BF),
            pltpu.VMEM((1, D), F32),
            pltpu.VMEM((ROWS, 2 * TOK), BF),
            pltpu.VMEM((TOK, D), BF),
            pltpu.VMEM((TOK, D), BF),
            pltpu.VMEM((ROWS, HALF), BF),
            pltpu.SemaphoreType.DMA((3,)),
            pltpu.SemaphoreType.DMA((6,)),
        ],
        vmem=(0, 1),
        raw=range(2, 5),
        free=(4,),
        raw_out=(0, 1, 2),
        limit=28,
        flops=2 * 10**9,
    )
    arrived = exchange(plain(send).reshape(experts, 8, HALF), ("sp", "dp"))
    (base,) = call(
        shared_kernel,
        [((TOK, D), F32)],
        (ein, mixed, shared_gate, shared_up, shared_down),
        limit=20,
        flops=4 * 10**9,
    )
    (done,) = call(
        expert_kernel,
        [((ROWS, HALF), BF)],
        (arrived.reshape(ROWS, HALF), expert_gate[0], expert_up[0], expert_down[0]),
        scratch=[
            pltpu.VMEM((ROWS // 2, D), BF),
            pltpu.VMEM((D, 512), BF),
            pltpu.VMEM((D, 512), BF),
            pltpu.VMEM((512, D), BF),
            pltpu.SemaphoreType.DMA((3,)),
        ],
        vmem=(0,),
        raw=(1, 2, 3),
        out_vmem=(0,),
        limit=32,
        flops=3 * 10**9,
    )
    back = exchange(plain(done).reshape(experts, 8, HALF), ("sp", "dp"))
    (out,) = call(
        combine_kernel,
        [((TOK, D), BF)],
        (back.reshape(ROWS, HALF), comb, base),
        vmem=(0,),
        raw=(1, 2),
        raw_out=(0,),
        scratch=[
            pltpu.VMEM((2 * TOK, ROWS), BF),
            pltpu.VMEM((TOK, D), F32),
            pltpu.VMEM((TOK, D), BF),
            pltpu.SemaphoreType.DMA((2,)),
            pltpu.SemaphoreType.DMA((2,)),
        ],
    )
    return plain(out)[None]


def solution(mesh):
    rows = P("dp", "sp", None)
    one = P(("sp", "dp"), None, None)
    return jax.shard_map(
        layer,
        mesh=mesh,
        in_specs=(
            (rows,) * 6 + (P(),) * 7 + (P("dp", None),) + (P(),) * 4 + (one,) * 3 + (rows, rows)
        ),
        out_specs=rows,
        check_vma=False,
    )
```

```python
import jax
import jax.numpy as jnp
from jax import lax
from jax._src.core import MemorySpace
from jax._src.state.primitives import with_memory_space_constraint
from jax.experimental import pallas as pl
from jax.experimental.pallas import tpu as pltpu
from jax.sharding import PartitionSpec as P


D = 2048
HEADS = 32
HEAD_DIM = 64
GROUPS = 8
STATE = 128
TOK = 128
EPS = 1e-06
BF = jnp.bfloat16
F32 = jnp.float32
PER = HEADS // GROUPS
GW = PER * HEAD_DIM
HALF = D // 2
ROWS = 1024
ST_ROWS = 160


def full():
    return pl.BlockSpec(memory_space=pltpu.VMEM)


def smem():
    return pl.BlockSpec(memory_space=pltpu.SMEM)


def anywhere():
    return pl.BlockSpec(memory_space=pl.ANY)


def call(
    kernel, outs, args, scratch=(), vmem=(), smem_in=(), raw=(), free=(), out_vmem=(), raw_out=(), limit=12,
    flops=10**6,
):
    placed = [
        v
        if i in smem_in or i in free
        else pltpu.with_memory_space_constraint(v, pltpu.VMEM if i in vmem else pltpu.HBM)
        for i, v in enumerate(args)
    ]
    return pl.pallas_call(
        kernel,
        out_shape=tuple(
            pltpu.VMEM(s, d) if i in out_vmem else pltpu.HBM(s, d)
            for i, (s, d) in enumerate(outs)
        ),
        in_specs=[
            smem() if i in smem_in else anywhere() if i in raw else full() for i in range(len(args))
        ],
        out_specs=tuple(anywhere() if i in raw_out else full() for i in range(len(outs))),
        scratch_shapes=list(scratch),
        compiler_params=pltpu.CompilerParams(vmem_limit_bytes=limit << 20),
        cost_estimate=pl.CostEstimate(flops=flops, bytes_accessed=10**6, transcendentals=0),
    )(*placed)


def silu(v):
    return v / (1.0 + jnp.exp(-v))


def tap(pad, halo, rows, weight):
    out = []
    for i in range(rows.shape[1] // 128):
        cols = slice(i * 128, (i + 1) * 128)
        pad[i, 0:8, :] = jnp.zeros((8, 128), F32) if halo is None else halo[:, cols].astype(F32)
        pad[i, 8 : 8 + TOK, :] = rows[:, cols].astype(F32)
        w = weight[:, cols].astype(F32)
        total = pad[i, 5 : 5 + TOK, :] * w[0:1, :]
        for k in range(1, 4):
            total = total + pad[i, 5 + k : 5 + k + TOK, :] * w[k : k + 1, :]
        out.append(silu(total))
    return jnp.concatenate(out, axis=1) if len(out) > 1 else out[0]


def spread(cols, g):
    lane = lax.broadcasted_iota(jnp.int32, (cols.shape[0], 128), 1)
    out = []
    for i in range(0, PER, 2):
        h = g * PER + i
        out.append(jnp.where(lane < HEAD_DIM, cols[:, h : h + 1], cols[:, h + 1 : h + 2]))
    return jnp.concatenate(out, axis=1)


def begin(pairs, sems):
    copies = [pltpu.make_async_copy(v, w, sems.at[k]) for k, (v, w) in enumerate(pairs)]
    for copy in copies:
        copy.start()
    return copies


def group(g):
    return slice(g * GW, (g + 1) * GW), slice(g * STATE, (g + 1) * STATE)


def part(g, width):
    return pl.ds(g * width, width)


def states_kernel(
    step_from, bias_in, dlog_in, x_in, b_in, cw_in, cbw_in, c_in, st, ec, grow_out, ends_out,
    padx, padb, step_in, bias, dlog, x, b, cw, cbw, sems
):
    pairs = [(step_from, step_in), (bias_in, bias), (dlog_in, dlog)]
    pairs += [(x_in, x), (b_in, b), (cw_in, cw), (cbw_in, cbw)]
    pairs.append((c_in.at[pl.ds(TOK - 8, 8), :], ends_out.at[:, pl.ds(D + 1024, 1024)]))
    loads = begin(pairs, sems)
    for load in loads[:3]:
        load.wait()
    s = step_in[...].astype(F32).T + bias[...]
    step = jnp.maximum(s, 0.0) + jnp.log(1.0 + jnp.exp(-jnp.abs(s)))
    logs = step * (-jnp.exp(dlog[...]))
    r = lax.broadcasted_iota(jnp.int32, (TOK, TOK), 0)
    c = lax.broadcasted_iota(jnp.int32, (TOK, TOK), 1)
    tri = (c <= r).astype(F32)
    cum = jnp.dot(tri, logs, precision=lax.Precision.HIGHEST, preferred_element_type=F32)
    ec[...] = jnp.exp(cum)
    grow = step * jnp.exp(-cum)
    grow_out[...] = grow
    later = jnp.where(lax.broadcasted_iota(jnp.int32, (TOK, HEADS), 0) < 3, 0.0, grow)
    tot = cum[TOK - 1 : TOK, :]
    etot = jnp.exp(tot)
    first = grow[0:8, :] * etot
    sub = lax.broadcasted_iota(jnp.int32, (8, 128), 0)
    low = lax.broadcasted_iota(jnp.int32, (8, 128), 1) < HEAD_DIM
    for load in loads[3:]:
        load.wait()
    for g in range(GROUPS):
        xc, bc = group(g)
        xs = tap(padx.at[g], None, x[:, xc], cw[:, xc])
        bm = tap(padb.at[g], None, b[:, bc], cbw[:, bc]).astype(BF)
        v = (xs * spread(later, g)).astype(BF)
        fresh = lax.dot_general(v, bm, (((0,), (0,)), ((), ())), preferred_element_type=F32)

        def ends(rows, taps):
            out = jnp.where(sub < 3, pltpu.roll(rows[TOK - 8 :], 3, 0), pltpu.roll(rows[:8], 3, 0))
            return with_taps(out, taps)

        def with_taps(rows, taps):
            taps = taps.astype(F32)
            return jnp.where(sub == 6, taps[0:1], jnp.where(sub == 7, taps[1:2], rows))

        b_taps = cbw[:, bc]
        for i in range(2):
            h = g * PER + 2 * i
            o = g * 2 + i
            for j in range(2):
                k = (2 * i + j) * HEAD_DIM
                st[o, j * HEAD_DIM : (j + 1) * HEAD_DIM, :] = (
                    fresh[k : k + HEAD_DIM, :] * etot[0:1, h + j : h + j + 1]
                ).astype(BF)
            tail = jnp.zeros((8, 128), F32)
            for j in range(2):
                rest = jnp.broadcast_to(tot[0:1, h + j : h + j + 1], (8, 128))
                for q in range(3):
                    piece = rest.astype(BF).astype(F32)
                    tail = jnp.where(sub == 3 * j + q, piece, tail)
                    rest = rest - piece
            w = jnp.where(low, first[:, h : h + 1], first[:, h + 1 : h + 2])
            w_hi = w.astype(BF).astype(F32)
            w_both = jnp.where(sub < 3, w_hi, pltpu.roll(w - w_hi, 3, 0))
            oc = slice(o * 128, (o + 1) * 128)
            tail = with_taps(tail, cw[0:2, oc])
            w_both = with_taps(w_both, cw[2:4, oc])
            x_ends = ends(x[:, oc].astype(F32), b_taps[0:2])
            b_ends = ends(b[:, bc].astype(F32), b_taps[2:4])
            st[o, 128:144, :] = jnp.concatenate([tail, w_both], axis=0).astype(BF)
            st[o, 144:160, :] = jnp.concatenate([x_ends, b_ends], axis=0).astype(BF)
    ends_out[:, 0:D] = x[TOK - 8 :, :]
    ends_out[:, D : D + 1024] = b[TOK - 8 :, :]


def inner_kernel(x, b, c, halo, cw, cbw, ccw, ec, grow, skip, a_out, c_out, padx, padb, padc):
    r = lax.broadcasted_iota(jnp.int32, (TOK, TOK), 0)
    s = lax.broadcasted_iota(jnp.int32, (TOK, TOK), 1)
    lower = s <= r
    cols = ec[...]
    rows = grow[...]
    sk = jnp.broadcast_to(skip[...], (TOK, HEADS))
    for g in range(GROUPS):
        xc = slice(g * GW, (g + 1) * GW)
        bc = slice(g * STATE, (g + 1) * STATE)
        bh = slice(D + g * STATE, D + (g + 1) * STATE)
        ch = slice(D + 1024 + g * STATE, D + 1024 + (g + 1) * STATE)
        xs = tap(padx.at[g], halo[:, xc], x[:, xc], cw[:, xc])
        bm = tap(padb.at[g], halo[:, bh], b[:, bc], cbw[:, bc]).astype(BF)
        cm = tap(padc.at[g], halo[:, ch], c[:, bc], ccw[:, bc]).astype(BF)
        c_out[:, bc] = cm
        v = (xs * spread(rows, g)).astype(BF)
        cb = lax.dot_general(cm, bm, (((1,), (1,)), ((), ())), preferred_element_type=F32)
        cb = jnp.where(lower, cb, 0.0).astype(BF)
        u = jnp.dot(cb, v, preferred_element_type=F32)
        a_out[:, xc] = u * spread(cols, g) + xs * spread(sk, g)


def carry_kernel(got, out, buf, sems):
    count = got.shape[0]
    sub = lax.broadcasted_iota(jnp.int32, (count, 8, 128), 1)

    def starts(rows, w):
        before = jnp.concatenate([jnp.zeros((1, 8, 128), F32), rows[:-1]], axis=0)
        seq = jnp.where(sub < 3, before, rows)
        total = seq * w[0]
        for k in range(1, 4):
            total = total + pltpu.roll(seq, 8 - k, 1) * w[k]
        return jnp.where(sub < 3, silu(total), 0.0)

    tails = got[:, 128:144, :].astype(F32)
    ends = got[:, 144:160, :].astype(F32)
    w = tails[:, 8:16]
    w = w + pltpu.roll(w, 5, 1)
    x_taps = [tails[0:1, k : k + 1] for k in (6, 7, 14, 15)]
    b_taps = [ends[0:1, k : k + 1] for k in (6, 7, 14, 15)]
    xs = starts(ends[:, 0:8], x_taps)
    bm = starts(ends[:, 8:16], b_taps)
    vt = jnp.where(sub < 3, xs * w, 0.0).reshape(count * 8, 128).T
    bm = bm.reshape(count * 8, 128).astype(BF)
    lane = lax.broadcasted_iota(jnp.int32, (128, 128), 1)
    row = lax.broadcasted_iota(jnp.int32, (2 * HEAD_DIM, 128), 0)
    carry = jnp.zeros((2 * HEAD_DIM, 128), F32)
    stores = []
    for i in range(count):
        buf[i] = carry.astype(BF)
        if i % 4 == 3:
            rows = pl.ds(i - 3, 4)
            stores.append(pltpu.make_async_copy(buf.at[rows], out.at[rows], sems.at[i // 4]))
            stores[-1].start()
        if i + 1 < count:
            mine = jnp.where(lane // 8 == i, vt, 0.0).astype(BF)
            extra = jnp.dot(mine, bm, preferred_element_type=F32)
            tail = tails[i, 0:8]
            fa = jnp.exp(tail[0:1] + tail[1:2] + tail[2:3])
            fb = jnp.exp(tail[3:4] + tail[4:5] + tail[5:6])
            factor = jnp.where(row < HEAD_DIM, fa, fb)
            carry = carry * factor + (got[i, 0 : 2 * HEAD_DIM, :].astype(F32) + extra)
    for copy in stores:
        copy.wait()


def slots(routes, rw):
    both = jnp.concatenate([routes[...].astype(F32), rw[...], jnp.zeros((4, TOK), F32)], axis=0).T
    ids = both[:, 0:2].astype(jnp.int32)
    e = lax.broadcasted_iota(jnp.int32, (TOK, 128), 1)
    r = lax.broadcasted_iota(jnp.int32, (TOK, TOK), 0)
    s = lax.broadcasted_iota(jnp.int32, (TOK, TOK), 1)
    tri = (s < r).astype(BF)
    hot = [(ids[:, k : k + 1] == e).astype(F32) for k in range(2)]
    before0 = jnp.dot(tri, hot[0].astype(BF), preferred_element_type=F32)
    before1 = jnp.dot(tri, hot[1].astype(BF), preferred_element_type=F32)
    before1 = before1 + jnp.sum(hot[0], axis=0, keepdims=True)
    pos = [
        jnp.sum(before0 * hot[0], axis=1, keepdims=True).astype(jnp.int32),
        jnp.sum(before1 * hot[1], axis=1, keepdims=True).astype(jnp.int32),
    ]
    return [ids[:, k : k + 1] * 8 + pos[k] for k in range(2)], both[:, 2:4]


def routes_kernel(routes, rw, d_out):
    at, _ = slots(routes, rw)
    lane = lax.broadcasted_iota(jnp.int32, (TOK, ROWS), 1)
    for h in range(2):
        hit = (lane == at[0] + 4 * h) | (lane == at[1] + 4 * h)
        d_out[:, h * TOK : (h + 1) * TOK] = jnp.where(hit, 1.0, 0.0).T.astype(BF)


def weights_kernel(routes, rw, w_out):
    at, w = slots(routes, rw)
    lane = lax.broadcasted_iota(jnp.int32, (TOK, ROWS), 1)
    for h in range(2):
        comb = jnp.where(lane == at[0] + 4 * h, w[:, 0:1], 0.0)
        comb = comb + jnp.where(lane == at[1] + 4 * h, w[:, 1:2], 0.0)
        w_out[h * TOK : (h + 1) * TOK, :] = comb.astype(BF)


def norm_kernel(
    pref, ec_in, a_in, cm_in, gate_in, gain_in, resid_in, w0, w1, w2, w3, w4, w5, w6, proj, rest,
    norm, wide, picked, ec, a, cm, gate, gain, resid, sems
):
    pairs = [(ec_in, ec), (cm_in, cm), (gain_in, gain)]
    for q in range(4):
        pairs.append((a_in.at[:, part(q, 512)], a.at[:, part(q, 512)]))
        pairs.append((gate_in.at[:, part(q, 512)], gate.at[:, part(q, 512)]))
    pairs.append((resid_in, resid))
    for k, w in enumerate((w0, w1, w2, w3, w4, w5, w6)):
        pairs.append((w, wide.at[part(k, GW), :]))
    loads = begin(pairs, sems)
    for load in loads[:3]:
        load.wait()
    cols = ec[...]
    for g in range(GROUPS):
        xc, bc = group(g)
        if g % 2 == 0:
            loads[3 + g].wait()
            loads[4 + g].wait()
        outer = lax.dot_general(
            cm[:, bc], pref[g], (((1,), (1,)), ((), ())), preferred_element_type=F32
        )
        y = (a[:, xc] + outer * spread(cols, g)).astype(BF).astype(F32)
        y = y * silu(gate[:, xc].astype(F32))
        y = y * lax.rsqrt(jnp.mean(y * y, axis=1, keepdims=True) + EPS)
        norm[g] = (y * gain[:, xc]).astype(BF)
    me = lax.axis_index("dp")
    odd = me & 1
    at = (me + 6 + 4 * odd) & 7
    other = ((me ^ 1) + 6 - 4 * odd + 4) & 7
    place = [me, me ^ 1, at, at ^ 1, other, other ^ 1, me ^ 4, me ^ 5]
    for k in range(7):
        picked[:, k * GW : (k + 1) * GW] = norm[place[k]]
    rest[...] = norm[place[7]]
    for load in loads[11:16]:
        load.wait()
    cut = 4 * GW
    proj[...] = resid[...].astype(F32) + jnp.dot(
        picked[:, :cut], wide[:cut, :], preferred_element_type=F32
    )
    for load in loads[16:]:
        load.wait()
    proj[...] += jnp.dot(picked[:, cut:], wide[cut:, :], preferred_element_type=F32)


def mix_kernel(
    proj_in, rest, fgain_in, disp_in, w7, mixed_out, ein_out, send_out,
    wide, fgain, disp, mixed_buf, ein_buf, send, sems, out_sems
):
    loads = begin([(w7, wide), (fgain_in, fgain), (disp_in, disp)], sems)
    loads[0].wait()
    proj = proj_in[...] + jnp.dot(rest[...], wide[...], preferred_element_type=F32)
    loads[1].wait()
    mixed = proj.astype(BF)
    mixed_buf[...] = mixed
    stores = [pltpu.make_async_copy(mixed_buf, mixed_out, out_sems.at[0])]
    stores[0].start()
    m = mixed.astype(F32)
    ein = (m * lax.rsqrt(jnp.mean(m * m, axis=1, keepdims=True) + EPS) * fgain[...]).astype(BF)
    ein_buf[...] = ein
    stores.append(pltpu.make_async_copy(ein_buf, ein_out, out_sems.at[1]))
    stores[1].start()
    stack = jnp.concatenate([ein[:, :HALF], ein[:, HALF:]], axis=0)
    loads[2].wait()
    for q in range(4):
        rows = part(q, 256)
        send[rows, :] = jnp.dot(disp[rows, :], stack, preferred_element_type=F32).astype(BF)
        store = pltpu.make_async_copy(send.at[rows, :], send_out.at[rows, :], out_sems.at[2 + q])
        store.start()
        stores.append(store)
    for store in stores:
        store.wait()


def shared_kernel(ein, mixed, sg, su, sd, out):
    x = ein[...]
    gate = jnp.dot(x, sg[...], preferred_element_type=F32)
    up = jnp.dot(x, su[...], preferred_element_type=F32)
    hidden = (silu(gate) * up).astype(BF)
    out[...] = mixed[...].astype(F32) + jnp.dot(hidden, sd[...], preferred_element_type=F32)


def expert_kernel(got, wg_in, wu_in, wd_in, out, xbuf, wg, wu, wd, gate, up, sems):
    n = 256
    sub = lax.broadcasted_iota(jnp.int32, (ROWS // 16, 8, n), 1)
    pairs = []
    for q in range(4):
        for v, w in ((wg_in, wg), (wu_in, wu)):
            for h in range(2):
                pairs.append((v.at[part(4 * h + q, n), :], w.at[q, part(h, n), :]))
    pairs.append((wd_in, wd))
    loads = begin(pairs, sems)

    def pack(q):
        t = got[:, q * n : (q + 1) * n].astype(F32).reshape(ROWS // 16, 2, 8, n)
        r0, r1 = t[:, 0], t[:, 1]
        x0 = jnp.where(sub < 4, r0, pltpu.roll(r1, 4, 1))
        x1 = jnp.where(sub < 4, pltpu.roll(r0, 4, 1), r1)
        xbuf[q, :, :n] = x0.reshape(ROWS // 2, n).astype(BF)
        xbuf[q, :, n:] = x1.reshape(ROWS // 2, n).astype(BF)

    pack(0)
    for q in range(4):
        for load in loads[4 * q : 4 * q + 4]:
            load.wait()
        if q < 3:
            pack(q + 1)
        for acc, w in ((gate, wg), (up, wu)):
            y = jnp.dot(xbuf[q], w[q], preferred_element_type=F32)
            acc[...] = y if q == 0 else acc[...] + y
    loads[16].wait()
    hidden = (silu(gate[...]) * up[...]).astype(BF)
    for q in range(HALF // n):
        y0 = jnp.dot(hidden, wd[:, q * n : (q + 1) * n], preferred_element_type=F32)
        y1 = jnp.dot(hidden, wd[:, HALF + q * n : HALF + (q + 1) * n], preferred_element_type=F32)
        y0 = y0.reshape(ROWS // 16, 8, n)
        y1 = y1.reshape(ROWS // 16, 8, n)
        o0 = jnp.where(sub < 4, y0, pltpu.roll(y1, 4, 1))
        o1 = jnp.where(sub < 4, pltpu.roll(y0, 4, 1), y1)
        out[:, q * n : (q + 1) * n] = jnp.stack([o0, o1], axis=1).reshape(ROWS, n).astype(BF)


def combine_kernel(got, w_in, base_in, out_ref, w, base, out, sems, out_sems):
    loads = begin([(w_in, w), (base_in, base)], sems)
    loads[0].wait()
    stores = []
    for h in range(2):
        cols = part(h, HALF)
        y = jnp.dot(w[part(h, TOK), :], got[...], preferred_element_type=F32)
        if h == 0:
            loads[1].wait()
        out[:, cols] = (base[:, cols] + y).astype(BF)
        stores.append(pltpu.make_async_copy(out.at[:, cols], out_ref.at[:, cols], out_sems.at[h]))
        stores[h].start()
    for copy in stores:
        copy.wait()


def plain(v):
    return with_memory_space_constraint(v, MemorySpace.Device)


def exchange(v, axis):
    return lax.all_to_all(plain(v), axis, split_axis=0, concat_axis=0, tiled=True)


def layer(
    residual, head_input, gate_input, b_input, c_input, step_input, conv_weight,
    conv_b_weight, conv_c_weight, step_bias, decay_log, skip, norm_gain, out_weight,
    ffn_gain, shared_gate, shared_up, shared_down, expert_gate, expert_up, expert_down,
    routes, route_weights,
):
    ways = lax.axis_size("sp")
    dps = lax.axis_size("dp")
    experts = ways * dps
    x, b, c = head_input[0], b_input[0], c_input[0]

    def ring(v):
        return lax.ppermute(v, "dp", [(i, (i + (-2 if i % 2 else 2)) % dps) for i in range(dps)])

    def swap(v):
        return lax.ppermute(v, "dp", [(i, i ^ 1) for i in range(dps)])

    partner = swap(out_weight)
    near = ring(out_weight)
    near2 = ring(partner)
    far = ring(near)
    pieces = [out_weight, partner, near, near2, swap(near), swap(near2)]
    pieces += [far, swap(far)]
    st, ec, grow, ends = call(
        states_kernel,
        [((ways, ST_ROWS, 128), BF), ((TOK, HEADS), F32), ((TOK, HEADS), F32), ((8, 4096), BF)],
        (step_input[0].T, step_bias[None], decay_log[None], x, b, conv_weight, conv_b_weight, c),
        raw=range(8),
        scratch=[
            pltpu.VMEM((GROUPS, 2, TOK + 8, 128), F32),
            pltpu.VMEM((GROUPS, 1, TOK + 8, 128), F32),
            pltpu.VMEM((HEADS, TOK), BF),
            pltpu.VMEM((1, HEADS), F32),
            pltpu.VMEM((1, HEADS), F32),
            pltpu.VMEM((TOK, D), BF),
            pltpu.VMEM((TOK, 1024), BF),
            pltpu.VMEM((4, D), BF),
            pltpu.VMEM((4, 1024), BF),
            pltpu.SemaphoreType.DMA((8,)),
        ],
    )
    got = exchange(st, "sp")
    halo = lax.ppermute(plain(ends), "sp", [(i, i + 1) for i in range(ways - 1)])
    a, cm = call(
        inner_kernel,
        [((TOK, D), F32), ((TOK, 1024), BF)],
        (x, b, c, halo, conv_weight, conv_b_weight, conv_c_weight, ec, grow, skip[None]),
        free=(3,),
        scratch=[
            pltpu.VMEM((GROUPS, 2, TOK + 8, 128), F32),
            pltpu.VMEM((GROUPS, 1, TOK + 8, 128), F32),
            pltpu.VMEM((GROUPS, 1, TOK + 8, 128), F32),
        ],
        flops=4 * 10**9,
    )
    ways_in = (routes[0].T, route_weights[0].T)
    (disp,) = call(routes_kernel, [((ROWS, 2 * TOK), BF)], ways_in, flops=2 * 10**9)
    (comb,) = call(weights_kernel, [((2 * TOK, ROWS), BF)], ways_in, flops=2 * 10**9)
    (carried,) = call(
        carry_kernel,
        [((ways, 128, 128), BF)],
        (got,),
        vmem=(0,),
        raw_out=(0,),
        scratch=[pltpu.VMEM((ways, 128, 128), BF), pltpu.SemaphoreType.DMA((4,))],
    )
    pref = exchange(carried, "sp")
    proj, rest = call(
        norm_kernel,
        [((TOK, D), F32), ((TOK, GW), BF)],
        (
            pref.reshape(GROUPS, GW, STATE), ec, a, cm, gate_input[0], norm_gain[None],
            residual[0], *pieces[:7],
        ),
        scratch=[
            pltpu.VMEM((GROUPS, TOK, GW), BF),
            pltpu.VMEM((7 * GW, D), BF),
            pltpu.VMEM((TOK, 7 * GW), BF),
            pltpu.VMEM((TOK, HEADS), F32),
            pltpu.VMEM((TOK, D), F32),
            pltpu.VMEM((TOK, 1024), BF),
            pltpu.VMEM((TOK, D), BF),
            pltpu.VMEM((1, D), F32),
            pltpu.VMEM((TOK, D), BF),
            pltpu.SemaphoreType.DMA((19,)),
        ],
        vmem=(0,),
        raw=range(1, 14),
        free=range(8, 14),
        out_vmem=(0, 1),
        limit=32,
        flops=2 * 10**9,
    )
    mixed, ein, send = call(
        mix_kernel,
        [((TOK, D), BF), ((TOK, D), BF), ((ROWS, HALF), BF)],
        (proj, rest, ffn_gain[None], disp, *pieces[7:]),
        scratch=[
            pltpu.VMEM((GW, D), BF),
            pltpu.VMEM((1, D), F32),
            pltpu.VMEM((ROWS, 2 * TOK), BF),
            pltpu.VMEM((TOK, D), BF),
            pltpu.VMEM((TOK, D), BF),
            pltpu.VMEM((ROWS, HALF), BF),
            pltpu.SemaphoreType.DMA((3,)),
            pltpu.SemaphoreType.DMA((6,)),
        ],
        vmem=(0, 1),
        raw=range(2, 5),
        free=(4,),
        raw_out=(0, 1, 2),
        limit=28,
        flops=2 * 10**9,
    )
    arrived = exchange(plain(send).reshape(experts, 8, HALF), ("sp", "dp"))
    (base,) = call(
        shared_kernel,
        [((TOK, D), F32)],
        (ein, mixed, shared_gate, shared_up, shared_down),
        limit=20,
        flops=4 * 10**9,
    )
    (done,) = call(
        expert_kernel,
        [((ROWS, HALF), BF)],
        (arrived.reshape(ROWS, HALF), expert_gate[0], expert_up[0], expert_down[0]),
        scratch=[
            pltpu.VMEM((4, ROWS // 2, 512), BF),
            pltpu.VMEM((4, 512, 512), BF),
            pltpu.VMEM((4, 512, 512), BF),
            pltpu.VMEM((512, D), BF),
            pltpu.VMEM((ROWS // 2, 512), F32),
            pltpu.VMEM((ROWS // 2, 512), F32),
            pltpu.SemaphoreType.DMA((17,)),
        ],
        vmem=(0,),
        raw=(1, 2, 3),
        out_vmem=(0,),
        limit=32,
        flops=3 * 10**9,
    )
    back = exchange(plain(done).reshape(experts, 8, HALF), ("sp", "dp"))
    (out,) = call(
        combine_kernel,
        [((TOK, D), BF)],
        (back.reshape(ROWS, HALF), comb, base),
        vmem=(0,),
        raw=(1, 2),
        raw_out=(0,),
        scratch=[
            pltpu.VMEM((2 * TOK, ROWS), BF),
            pltpu.VMEM((TOK, D), F32),
            pltpu.VMEM((TOK, D), BF),
            pltpu.SemaphoreType.DMA((2,)),
            pltpu.SemaphoreType.DMA((2,)),
        ],
    )
    return plain(out)[None]


def solution(mesh):
    rows = P("dp", "sp", None)
    one = P(("sp", "dp"), None, None)
    return jax.shard_map(
        layer,
        mesh=mesh,
        in_specs=(
            (rows,) * 6 + (P(),) * 7 + (P("dp", None),) + (P(),) * 4 + (one,) * 3 + (rows, rows)
        ),
        out_specs=rows,
        check_vma=False,
    )
```

```python
import jax
import jax.numpy as jnp
from jax import lax
from jax._src.core import MemorySpace
from jax._src.state.primitives import with_memory_space_constraint
from jax.experimental import pallas as pl
from jax.experimental.pallas import tpu as pltpu
from jax.sharding import PartitionSpec as P


D = 2048
HEADS = 32
HEAD_DIM = 64
GROUPS = 8
STATE = 128
TOK = 128
EPS = 1e-06
BF = jnp.bfloat16
F32 = jnp.float32
PER = HEADS // GROUPS
GW = PER * HEAD_DIM
HALF = D // 2
ROWS = 1024
ST_ROWS = 160


def full():
    return pl.BlockSpec(memory_space=pltpu.VMEM)


def smem():
    return pl.BlockSpec(memory_space=pltpu.SMEM)


def anywhere():
    return pl.BlockSpec(memory_space=pl.ANY)


def call(
    kernel, outs, args, scratch=(), vmem=(), smem_in=(), raw=(), free=(), out_vmem=(), raw_out=(), limit=12,
    flops=10**6,
):
    placed = [
        v
        if i in smem_in or i in free
        else pltpu.with_memory_space_constraint(v, pltpu.VMEM if i in vmem else pltpu.HBM)
        for i, v in enumerate(args)
    ]
    return pl.pallas_call(
        kernel,
        out_shape=tuple(
            pltpu.VMEM(s, d) if i in out_vmem else pltpu.HBM(s, d)
            for i, (s, d) in enumerate(outs)
        ),
        in_specs=[
            smem() if i in smem_in else anywhere() if i in raw else full() for i in range(len(args))
        ],
        out_specs=tuple(anywhere() if i in raw_out else full() for i in range(len(outs))),
        scratch_shapes=list(scratch),
        compiler_params=pltpu.CompilerParams(vmem_limit_bytes=limit << 20),
        cost_estimate=pl.CostEstimate(flops=flops, bytes_accessed=10**6, transcendentals=0),
    )(*placed)


def silu(v):
    return v / (1.0 + jnp.exp(-v))


def tap(pad, halo, rows, weight):
    out = []
    for i in range(rows.shape[1] // 128):
        cols = slice(i * 128, (i + 1) * 128)
        pad[i, 0:8, :] = jnp.zeros((8, 128), F32) if halo is None else halo[:, cols].astype(F32)
        pad[i, 8 : 8 + TOK, :] = rows[:, cols].astype(F32)
        w = weight[:, cols].astype(F32)
        total = pad[i, 5 : 5 + TOK, :] * w[0:1, :]
        for k in range(1, 4):
            total = total + pad[i, 5 + k : 5 + k + TOK, :] * w[k : k + 1, :]
        out.append(silu(total))
    return jnp.concatenate(out, axis=1) if len(out) > 1 else out[0]


def spread(cols, g):
    lane = lax.broadcasted_iota(jnp.int32, (cols.shape[0], 128), 1)
    out = []
    for i in range(0, PER, 2):
        h = g * PER + i
        out.append(jnp.where(lane < HEAD_DIM, cols[:, h : h + 1], cols[:, h + 1 : h + 2]))
    return jnp.concatenate(out, axis=1)


def begin(pairs, sems):
    copies = [pltpu.make_async_copy(v, w, sems.at[k]) for k, (v, w) in enumerate(pairs)]
    for copy in copies:
        copy.start()
    return copies


def group(g):
    return slice(g * GW, (g + 1) * GW), slice(g * STATE, (g + 1) * STATE)


def part(g, width):
    return pl.ds(g * width, width)


def states_kernel(
    step_from, bias_in, dlog_in, x_in, b_in, cw_in, cbw_in, c_in, st, ec, grow_out, ends_out,
    padx, padb, step_in, bias, dlog, x, b, cw, cbw, sems
):
    pairs = [(step_from, step_in), (bias_in, bias), (dlog_in, dlog)]
    pairs += [(x_in, x), (b_in, b), (cw_in, cw), (cbw_in, cbw)]
    pairs.append((c_in.at[pl.ds(TOK - 8, 8), :], ends_out.at[:, pl.ds(D + 1024, 1024)]))
    loads = begin(pairs, sems)
    for load in loads[:3]:
        load.wait()
    s = step_in[...].astype(F32).T + bias[...]
    step = jnp.maximum(s, 0.0) + jnp.log(1.0 + jnp.exp(-jnp.abs(s)))
    logs = step * (-jnp.exp(dlog[...]))
    r = lax.broadcasted_iota(jnp.int32, (TOK, TOK), 0)
    c = lax.broadcasted_iota(jnp.int32, (TOK, TOK), 1)
    tri = (c <= r).astype(F32)
    cum = jnp.dot(tri, logs, precision=lax.Precision.HIGHEST, preferred_element_type=F32)
    ec[...] = jnp.exp(cum)
    grow = step * jnp.exp(-cum)
    grow_out[...] = grow
    later = jnp.where(lax.broadcasted_iota(jnp.int32, (TOK, HEADS), 0) < 3, 0.0, grow)
    tot = cum[TOK - 1 : TOK, :]
    etot = jnp.exp(tot)
    first = grow[0:8, :] * etot
    sub = lax.broadcasted_iota(jnp.int32, (8, 128), 0)
    low = lax.broadcasted_iota(jnp.int32, (8, 128), 1) < HEAD_DIM
    for load in loads[3:]:
        load.wait()
    for g in range(GROUPS):
        xc, bc = group(g)
        xs = tap(padx.at[g], None, x[:, xc], cw[:, xc])
        bm = tap(padb.at[g], None, b[:, bc], cbw[:, bc]).astype(BF)
        v = (xs * spread(later, g)).astype(BF)
        fresh = lax.dot_general(v, bm, (((0,), (0,)), ((), ())), preferred_element_type=F32)

        def ends(rows, taps):
            out = jnp.where(sub < 3, pltpu.roll(rows[TOK - 8 :], 3, 0), pltpu.roll(rows[:8], 3, 0))
            return with_taps(out, taps)

        def with_taps(rows, taps):
            taps = taps.astype(F32)
            return jnp.where(sub == 6, taps[0:1], jnp.where(sub == 7, taps[1:2], rows))

        b_taps = cbw[:, bc]
        for i in range(2):
            h = g * PER + 2 * i
            o = g * 2 + i
            for j in range(2):
                k = (2 * i + j) * HEAD_DIM
                st[o, j * HEAD_DIM : (j + 1) * HEAD_DIM, :] = (
                    fresh[k : k + HEAD_DIM, :] * etot[0:1, h + j : h + j + 1]
                ).astype(BF)
            tail = jnp.zeros((8, 128), F32)
            for j in range(2):
                rest = jnp.broadcast_to(tot[0:1, h + j : h + j + 1], (8, 128))
                for q in range(3):
                    piece = rest.astype(BF).astype(F32)
                    tail = jnp.where(sub == 3 * j + q, piece, tail)
                    rest = rest - piece
            w = jnp.where(low, first[:, h : h + 1], first[:, h + 1 : h + 2])
            w_hi = w.astype(BF).astype(F32)
            w_both = jnp.where(sub < 3, w_hi, pltpu.roll(w - w_hi, 3, 0))
            oc = slice(o * 128, (o + 1) * 128)
            tail = with_taps(tail, cw[0:2, oc])
            w_both = with_taps(w_both, cw[2:4, oc])
            x_ends = ends(x[:, oc].astype(F32), b_taps[0:2])
            b_ends = ends(b[:, bc].astype(F32), b_taps[2:4])
            st[o, 128:144, :] = jnp.concatenate([tail, w_both], axis=0).astype(BF)
            st[o, 144:160, :] = jnp.concatenate([x_ends, b_ends], axis=0).astype(BF)
    ends_out[:, 0:D] = x[TOK - 8 :, :]
    ends_out[:, D : D + 1024] = b[TOK - 8 :, :]


def inner_kernel(
    x_in, b_in, c_in, halo_in, cw_in, cbw_in, ccw_in, ec_in, grow_in, skip_in, a_out, c_out,
    padx, padb, padc, x, b, c, halo, cw, cbw, ccw, ec, grow, skip, a_buf, cm_buf, sems, out_sems
):
    pairs = [(x_in, x), (b_in, b), (c_in, c), (halo_in, halo), (cw_in, cw), (cbw_in, cbw)]
    pairs += [(ccw_in, ccw), (ec_in, ec), (grow_in, grow), (skip_in, skip)]
    for load in begin(pairs, sems):
        load.wait()
    stores = []
    r = lax.broadcasted_iota(jnp.int32, (TOK, TOK), 0)
    s = lax.broadcasted_iota(jnp.int32, (TOK, TOK), 1)
    lower = s <= r
    cols = ec[...]
    rows = grow[...]
    sk = jnp.broadcast_to(skip[...], (TOK, HEADS))
    for g in range(GROUPS):
        xc = slice(g * GW, (g + 1) * GW)
        bc = slice(g * STATE, (g + 1) * STATE)
        bh = slice(D + g * STATE, D + (g + 1) * STATE)
        ch = slice(D + 1024 + g * STATE, D + 1024 + (g + 1) * STATE)
        xs = tap(padx.at[g], halo[:, xc], x[:, xc], cw[:, xc])
        bm = tap(padb.at[g], halo[:, bh], b[:, bc], cbw[:, bc]).astype(BF)
        cm = tap(padc.at[g], halo[:, ch], c[:, bc], ccw[:, bc]).astype(BF)
        cm_buf[:, bc] = cm
        v = (xs * spread(rows, g)).astype(BF)
        cb = lax.dot_general(cm, bm, (((1,), (1,)), ((), ())), preferred_element_type=F32)
        cb = jnp.where(lower, cb, 0.0).astype(BF)
        u = jnp.dot(cb, v, preferred_element_type=F32)
        a_buf[:, xc] = u * spread(cols, g) + xs * spread(sk, g)
        if g % 4 == 3:
            cols4 = part(g // 4, D // 2)
            stores.append(
                pltpu.make_async_copy(a_buf.at[:, cols4], a_out.at[:, cols4], out_sems.at[g // 4])
            )
            stores[-1].start()
    stores.append(pltpu.make_async_copy(cm_buf, c_out, out_sems.at[2]))
    stores[-1].start()
    for store in stores:
        store.wait()


def carry_kernel(got, out, buf, sems):
    count = got.shape[0]
    sub = lax.broadcasted_iota(jnp.int32, (count, 8, 128), 1)

    def starts(rows, w):
        before = jnp.concatenate([jnp.zeros((1, 8, 128), F32), rows[:-1]], axis=0)
        seq = jnp.where(sub < 3, before, rows)
        total = seq * w[0]
        for k in range(1, 4):
            total = total + pltpu.roll(seq, 8 - k, 1) * w[k]
        return jnp.where(sub < 3, silu(total), 0.0)

    tails = got[:, 128:144, :].astype(F32)
    ends = got[:, 144:160, :].astype(F32)
    w = tails[:, 8:16]
    w = w + pltpu.roll(w, 5, 1)
    x_taps = [tails[0:1, k : k + 1] for k in (6, 7, 14, 15)]
    b_taps = [ends[0:1, k : k + 1] for k in (6, 7, 14, 15)]
    xs = starts(ends[:, 0:8], x_taps)
    bm = starts(ends[:, 8:16], b_taps)
    vt = jnp.where(sub < 3, xs * w, 0.0).reshape(count * 8, 128).T
    bm = bm.reshape(count * 8, 128).astype(BF)
    lane = lax.broadcasted_iota(jnp.int32, (128, 128), 1)
    row = lax.broadcasted_iota(jnp.int32, (2 * HEAD_DIM, 128), 0)
    carry = jnp.zeros((2 * HEAD_DIM, 128), F32)
    stores = []
    for i in range(count):
        buf[i] = carry.astype(BF)
        if i % 4 == 3:
            rows = pl.ds(i - 3, 4)
            stores.append(pltpu.make_async_copy(buf.at[rows], out.at[rows], sems.at[i // 4]))
            stores[-1].start()
        if i + 1 < count:
            mine = jnp.where(lane // 8 == i, vt, 0.0).astype(BF)
            extra = jnp.dot(mine, bm, preferred_element_type=F32)
            tail = tails[i, 0:8]
            fa = jnp.exp(tail[0:1] + tail[1:2] + tail[2:3])
            fb = jnp.exp(tail[3:4] + tail[4:5] + tail[5:6])
            factor = jnp.where(row < HEAD_DIM, fa, fb)
            carry = carry * factor + (got[i, 0 : 2 * HEAD_DIM, :].astype(F32) + extra)
    for copy in stores:
        copy.wait()


def slots(routes, rw):
    both = jnp.concatenate([routes[...].astype(F32), rw[...], jnp.zeros((4, TOK), F32)], axis=0).T
    ids = both[:, 0:2].astype(jnp.int32)
    e = lax.broadcasted_iota(jnp.int32, (TOK, 128), 1)
    r = lax.broadcasted_iota(jnp.int32, (TOK, TOK), 0)
    s = lax.broadcasted_iota(jnp.int32, (TOK, TOK), 1)
    tri = (s < r).astype(BF)
    hot = [(ids[:, k : k + 1] == e).astype(F32) for k in range(2)]
    before0 = jnp.dot(tri, hot[0].astype(BF), preferred_element_type=F32)
    before1 = jnp.dot(tri, hot[1].astype(BF), preferred_element_type=F32)
    before1 = before1 + jnp.sum(hot[0], axis=0, keepdims=True)
    pos = [
        jnp.sum(before0 * hot[0], axis=1, keepdims=True).astype(jnp.int32),
        jnp.sum(before1 * hot[1], axis=1, keepdims=True).astype(jnp.int32),
    ]
    return [ids[:, k : k + 1] * 8 + pos[k] for k in range(2)], both[:, 2:4]


def routes_kernel(routes, rw, d_out):
    at, _ = slots(routes, rw)
    lane = lax.broadcasted_iota(jnp.int32, (TOK, ROWS), 1)
    for h in range(2):
        hit = (lane == at[0] + 4 * h) | (lane == at[1] + 4 * h)
        d_out[:, h * TOK : (h + 1) * TOK] = jnp.where(hit, 1.0, 0.0).T.astype(BF)


def weights_kernel(routes, rw, w_out):
    at, w = slots(routes, rw)
    lane = lax.broadcasted_iota(jnp.int32, (TOK, ROWS), 1)
    for h in range(2):
        comb = jnp.where(lane == at[0] + 4 * h, w[:, 0:1], 0.0)
        comb = comb + jnp.where(lane == at[1] + 4 * h, w[:, 1:2], 0.0)
        w_out[h * TOK : (h + 1) * TOK, :] = comb.astype(BF)


def norm_kernel(
    pref, ec_in, a_in, cm_in, gate_in, gain_in, resid_in, w0, w1, w2, w3, w4, w5, w6, proj, rest,
    norm, wide, picked, ec, a, cm, gate, gain, resid, sems
):
    pairs = [(ec_in, ec), (cm_in, cm), (gain_in, gain)]
    for q in range(4):
        pairs.append((a_in.at[:, part(q, 512)], a.at[:, part(q, 512)]))
        pairs.append((gate_in.at[:, part(q, 512)], gate.at[:, part(q, 512)]))
    pairs.append((resid_in, resid))
    for k, w in enumerate((w0, w1, w2, w3, w4, w5, w6)):
        pairs.append((w, wide.at[part(k, GW), :]))
    loads = begin(pairs, sems)
    for load in loads[:3]:
        load.wait()
    cols = ec[...]
    for g in range(GROUPS):
        xc, bc = group(g)
        if g % 2 == 0:
            loads[3 + g].wait()
            loads[4 + g].wait()
        outer = lax.dot_general(
            cm[:, bc], pref[g], (((1,), (1,)), ((), ())), preferred_element_type=F32
        )
        y = (a[:, xc] + outer * spread(cols, g)).astype(BF).astype(F32)
        y = y * silu(gate[:, xc].astype(F32))
        y = y * lax.rsqrt(jnp.mean(y * y, axis=1, keepdims=True) + EPS)
        norm[g] = (y * gain[:, xc]).astype(BF)
    me = lax.axis_index("dp")
    odd = me & 1
    at = (me + 6 + 4 * odd) & 7
    other = ((me ^ 1) + 6 - 4 * odd + 4) & 7
    place = [me, me ^ 1, at, at ^ 1, other, other ^ 1, me ^ 4, me ^ 5]
    for k in range(7):
        picked[:, k * GW : (k + 1) * GW] = norm[place[k]]
    rest[...] = norm[place[7]]
    for load in loads[11:16]:
        load.wait()
    cut = 4 * GW
    proj[...] = resid[...].astype(F32) + jnp.dot(
        picked[:, :cut], wide[:cut, :], preferred_element_type=F32
    )
    for load in loads[16:]:
        load.wait()
    proj[...] += jnp.dot(picked[:, cut:], wide[cut:, :], preferred_element_type=F32)


def mix_kernel(
    proj_in, rest, fgain_in, disp_in, w7, mixed_out, ein_out, send_out,
    wide, fgain, disp, mixed_buf, ein_buf, send, sems, out_sems
):
    loads = begin([(w7, wide), (fgain_in, fgain), (disp_in, disp)], sems)
    loads[0].wait()
    proj = proj_in[...] + jnp.dot(rest[...], wide[...], preferred_element_type=F32)
    loads[1].wait()
    mixed = proj.astype(BF)
    mixed_buf[...] = mixed
    stores = [pltpu.make_async_copy(mixed_buf, mixed_out, out_sems.at[0])]
    stores[0].start()
    m = mixed.astype(F32)
    ein = (m * lax.rsqrt(jnp.mean(m * m, axis=1, keepdims=True) + EPS) * fgain[...]).astype(BF)
    ein_buf[...] = ein
    stores.append(pltpu.make_async_copy(ein_buf, ein_out, out_sems.at[1]))
    stores[1].start()
    stack = jnp.concatenate([ein[:, :HALF], ein[:, HALF:]], axis=0)
    loads[2].wait()
    for q in range(4):
        rows = part(q, 256)
        send[rows, :] = jnp.dot(disp[rows, :], stack, preferred_element_type=F32).astype(BF)
        store = pltpu.make_async_copy(send.at[rows, :], send_out.at[rows, :], out_sems.at[2 + q])
        store.start()
        stores.append(store)
    for store in stores:
        store.wait()


def shared_kernel(ein, mixed, sg, su, sd, out):
    x = ein[...]
    gate = jnp.dot(x, sg[...], preferred_element_type=F32)
    up = jnp.dot(x, su[...], preferred_element_type=F32)
    hidden = (silu(gate) * up).astype(BF)
    out[...] = mixed[...].astype(F32) + jnp.dot(hidden, sd[...], preferred_element_type=F32)


def expert_kernel(got, wg_in, wu_in, wd_in, out, xbuf, wg, wu, wd, sems):
    pairs = ((wg_in, wg), (wu_in, wu), (wd_in, wd))
    loads = [pltpu.make_async_copy(v, w, sems.at[k]) for k, (v, w) in enumerate(pairs)]
    for load in loads:
        load.start()
    n = 256
    sub = lax.broadcasted_iota(jnp.int32, (ROWS // 16, 8, n), 1)
    for q in range(HALF // n):
        t = got[:, q * n : (q + 1) * n].astype(F32).reshape(ROWS // 16, 2, 8, n)
        r0, r1 = t[:, 0], t[:, 1]
        x0 = jnp.where(sub < 4, r0, pltpu.roll(r1, 4, 1))
        x1 = jnp.where(sub < 4, pltpu.roll(r0, 4, 1), r1)
        xbuf[:, q * n : (q + 1) * n] = x0.reshape(ROWS // 2, n).astype(BF)
        xbuf[:, HALF + q * n : HALF + (q + 1) * n] = x1.reshape(ROWS // 2, n).astype(BF)
    x = xbuf[...]
    loads[0].wait()
    gate = jnp.dot(x, wg[...], preferred_element_type=F32)
    loads[1].wait()
    up = jnp.dot(x, wu[...], preferred_element_type=F32)
    hidden = (silu(gate) * up).astype(BF)
    loads[2].wait()
    for q in range(HALF // n):
        y0 = jnp.dot(hidden, wd[:, q * n : (q + 1) * n], preferred_element_type=F32)
        y1 = jnp.dot(hidden, wd[:, HALF + q * n : HALF + (q + 1) * n], preferred_element_type=F32)
        y0 = y0.reshape(ROWS // 16, 8, n)
        y1 = y1.reshape(ROWS // 16, 8, n)
        o0 = jnp.where(sub < 4, y0, pltpu.roll(y1, 4, 1))
        o1 = jnp.where(sub < 4, pltpu.roll(y0, 4, 1), y1)
        out[:, q * n : (q + 1) * n] = jnp.stack([o0, o1], axis=1).reshape(ROWS, n).astype(BF)


def combine_kernel(got, w_in, base_in, out_ref, w, base, out, sems, out_sems):
    loads = begin([(w_in, w), (base_in, base)], sems)
    loads[0].wait()
    stores = []
    for h in range(2):
        cols = part(h, HALF)
        y = jnp.dot(w[part(h, TOK), :], got[...], preferred_element_type=F32)
        if h == 0:
            loads[1].wait()
        out[:, cols] = (base[:, cols] + y).astype(BF)
        stores.append(pltpu.make_async_copy(out.at[:, cols], out_ref.at[:, cols], out_sems.at[h]))
        stores[h].start()
    for copy in stores:
        copy.wait()


def plain(v):
    return with_memory_space_constraint(v, MemorySpace.Device)


def exchange(v, axis):
    return lax.all_to_all(plain(v), axis, split_axis=0, concat_axis=0, tiled=True)


def layer(
    residual, head_input, gate_input, b_input, c_input, step_input, conv_weight,
    conv_b_weight, conv_c_weight, step_bias, decay_log, skip, norm_gain, out_weight,
    ffn_gain, shared_gate, shared_up, shared_down, expert_gate, expert_up, expert_down,
    routes, route_weights,
):
    ways = lax.axis_size("sp")
    dps = lax.axis_size("dp")
    experts = ways * dps
    x, b, c = head_input[0], b_input[0], c_input[0]

    def ring(v):
        return lax.ppermute(v, "dp", [(i, (i + (-2 if i % 2 else 2)) % dps) for i in range(dps)])

    def swap(v):
        return lax.ppermute(v, "dp", [(i, i ^ 1) for i in range(dps)])

    partner = swap(out_weight)
    near = ring(out_weight)
    near2 = ring(partner)
    far = ring(near)
    pieces = [out_weight, partner, near, near2, swap(near), swap(near2)]
    pieces += [far, swap(far)]
    st, ec, grow, ends = call(
        states_kernel,
        [((ways, ST_ROWS, 128), BF), ((TOK, HEADS), F32), ((TOK, HEADS), F32), ((8, 4096), BF)],
        (step_input[0].T, step_bias[None], decay_log[None], x, b, conv_weight, conv_b_weight, c),
        raw=range(8),
        scratch=[
            pltpu.VMEM((GROUPS, 2, TOK + 8, 128), F32),
            pltpu.VMEM((GROUPS, 1, TOK + 8, 128), F32),
            pltpu.VMEM((HEADS, TOK), BF),
            pltpu.VMEM((1, HEADS), F32),
            pltpu.VMEM((1, HEADS), F32),
            pltpu.VMEM((TOK, D), BF),
            pltpu.VMEM((TOK, 1024), BF),
            pltpu.VMEM((4, D), BF),
            pltpu.VMEM((4, 1024), BF),
            pltpu.SemaphoreType.DMA((8,)),
        ],
    )
    got = exchange(st, "sp")
    halo = lax.ppermute(plain(ends), "sp", [(i, i + 1) for i in range(ways - 1)])
    a, cm = call(
        inner_kernel,
        [((TOK, D), F32), ((TOK, 1024), BF)],
        (x, b, c, halo, conv_weight, conv_b_weight, conv_c_weight, ec, grow, skip[None]),
        raw=range(10),
        free=(3,),
        raw_out=(0, 1),
        scratch=[
            pltpu.VMEM((GROUPS, 2, TOK + 8, 128), F32),
            pltpu.VMEM((GROUPS, 1, TOK + 8, 128), F32),
            pltpu.VMEM((GROUPS, 1, TOK + 8, 128), F32),
            pltpu.VMEM((TOK, D), BF),
            pltpu.VMEM((TOK, 1024), BF),
            pltpu.VMEM((TOK, 1024), BF),
            pltpu.VMEM((8, 4096), BF),
            pltpu.VMEM((4, D), BF),
            pltpu.VMEM((4, 1024), BF),
            pltpu.VMEM((4, 1024), BF),
            pltpu.VMEM((TOK, HEADS), F32),
            pltpu.VMEM((TOK, HEADS), F32),
            pltpu.VMEM((1, HEADS), F32),
            pltpu.VMEM((TOK, D), F32),
            pltpu.VMEM((TOK, 1024), BF),
            pltpu.SemaphoreType.DMA((10,)),
            pltpu.SemaphoreType.DMA((3,)),
        ],
        flops=4 * 10**9,
    )
    ways_in = (routes[0].T, route_weights[0].T)
    (disp,) = call(routes_kernel, [((ROWS, 2 * TOK), BF)], ways_in, flops=2 * 10**9)
    (comb,) = call(weights_kernel, [((2 * TOK, ROWS), BF)], ways_in, flops=2 * 10**9)
    (carried,) = call(
        carry_kernel,
        [((ways, 128, 128), BF)],
        (got,),
        vmem=(0,),
        raw_out=(0,),
        scratch=[pltpu.VMEM((ways, 128, 128), BF), pltpu.SemaphoreType.DMA((4,))],
    )
    pref = exchange(carried, "sp")
    proj, rest = call(
        norm_kernel,
        [((TOK, D), F32), ((TOK, GW), BF)],
        (
            pref.reshape(GROUPS, GW, STATE), ec, a, cm, gate_input[0], norm_gain[None],
            residual[0], *pieces[:7],
        ),
        scratch=[
            pltpu.VMEM((GROUPS, TOK, GW), BF),
            pltpu.VMEM((7 * GW, D), BF),
            pltpu.VMEM((TOK, 7 * GW), BF),
            pltpu.VMEM((TOK, HEADS), F32),
            pltpu.VMEM((TOK, D), F32),
            pltpu.VMEM((TOK, 1024), BF),
            pltpu.VMEM((TOK, D), BF),
            pltpu.VMEM((1, D), F32),
            pltpu.VMEM((TOK, D), BF),
            pltpu.SemaphoreType.DMA((19,)),
        ],
        vmem=(0,),
        raw=range(1, 14),
        free=range(8, 14),
        out_vmem=(0, 1),
        limit=32,
        flops=2 * 10**9,
    )
    mixed, ein, send = call(
        mix_kernel,
        [((TOK, D), BF), ((TOK, D), BF), ((ROWS, HALF), BF)],
        (proj, rest, ffn_gain[None], disp, *pieces[7:]),
        scratch=[
            pltpu.VMEM((GW, D), BF),
            pltpu.VMEM((1, D), F32),
            pltpu.VMEM((ROWS, 2 * TOK), BF),
            pltpu.VMEM((TOK, D), BF),
            pltpu.VMEM((TOK, D), BF),
            pltpu.VMEM((ROWS, HALF), BF),
            pltpu.SemaphoreType.DMA((3,)),
            pltpu.SemaphoreType.DMA((6,)),
        ],
        vmem=(0, 1),
        raw=range(2, 5),
        free=(4,),
        raw_out=(0, 1, 2),
        limit=28,
        flops=2 * 10**9,
    )
    arrived = exchange(plain(send).reshape(experts, 8, HALF), ("sp", "dp"))
    (base,) = call(
        shared_kernel,
        [((TOK, D), F32)],
        (ein, mixed, shared_gate, shared_up, shared_down),
        limit=20,
        flops=4 * 10**9,
    )
    (done,) = call(
        expert_kernel,
        [((ROWS, HALF), BF)],
        (arrived.reshape(ROWS, HALF), expert_gate[0], expert_up[0], expert_down[0]),
        scratch=[
            pltpu.VMEM((ROWS // 2, D), BF),
            pltpu.VMEM((D, 512), BF),
            pltpu.VMEM((D, 512), BF),
            pltpu.VMEM((512, D), BF),
            pltpu.SemaphoreType.DMA((3,)),
        ],
        vmem=(0,),
        raw=(1, 2, 3),
        out_vmem=(0,),
        limit=32,
        flops=3 * 10**9,
    )
    back = exchange(plain(done).reshape(experts, 8, HALF), ("sp", "dp"))
    (out,) = call(
        combine_kernel,
        [((TOK, D), BF)],
        (back.reshape(ROWS, HALF), comb, base),
        vmem=(0,),
        raw=(1, 2),
        raw_out=(0,),
        scratch=[
            pltpu.VMEM((2 * TOK, ROWS), BF),
            pltpu.VMEM((TOK, D), F32),
            pltpu.VMEM((TOK, D), BF),
            pltpu.SemaphoreType.DMA((2,)),
            pltpu.SemaphoreType.DMA((2,)),
        ],
    )
    return plain(out)[None]


def solution(mesh):
    rows = P("dp", "sp", None)
    one = P(("sp", "dp"), None, None)
    return jax.shard_map(
        layer,
        mesh=mesh,
        in_specs=(
            (rows,) * 6 + (P(),) * 7 + (P("dp", None),) + (P(),) * 4 + (one,) * 3 + (rows, rows)
        ),
        out_specs=rows,
        check_vma=False,
    )
```

```python
import jax
import jax.numpy as jnp
from jax import lax
from jax._src.core import MemorySpace
from jax._src.state.primitives import with_memory_space_constraint
from jax.experimental import pallas as pl
from jax.experimental.pallas import tpu as pltpu
from jax.sharding import PartitionSpec as P


D = 2048
HEADS = 32
HEAD_DIM = 64
GROUPS = 8
STATE = 128
TOK = 128
EPS = 1e-06
BF = jnp.bfloat16
F32 = jnp.float32
PER = HEADS // GROUPS
GW = PER * HEAD_DIM
HALF = D // 2
ROWS = 1024
ST_ROWS = 160


def full():
    return pl.BlockSpec(memory_space=pltpu.VMEM)


def smem():
    return pl.BlockSpec(memory_space=pltpu.SMEM)


def anywhere():
    return pl.BlockSpec(memory_space=pl.ANY)


def call(
    kernel, outs, args, scratch=(), vmem=(), smem_in=(), raw=(), free=(), out_vmem=(), raw_out=(), limit=12,
    flops=10**6,
):
    placed = [
        v
        if i in smem_in or i in free
        else pltpu.with_memory_space_constraint(v, pltpu.VMEM if i in vmem else pltpu.HBM)
        for i, v in enumerate(args)
    ]
    return pl.pallas_call(
        kernel,
        out_shape=tuple(
            pltpu.VMEM(s, d) if i in out_vmem else pltpu.HBM(s, d)
            for i, (s, d) in enumerate(outs)
        ),
        in_specs=[
            smem() if i in smem_in else anywhere() if i in raw else full() for i in range(len(args))
        ],
        out_specs=tuple(anywhere() if i in raw_out else full() for i in range(len(outs))),
        scratch_shapes=list(scratch),
        compiler_params=pltpu.CompilerParams(vmem_limit_bytes=limit << 20),
        cost_estimate=pl.CostEstimate(flops=flops, bytes_accessed=10**6, transcendentals=0),
    )(*placed)


def silu(v):
    return v / (1.0 + jnp.exp(-v))


def tap(pad, halo, rows, weight):
    out = []
    for i in range(rows.shape[1] // 128):
        cols = slice(i * 128, (i + 1) * 128)
        pad[i, 0:8, :] = jnp.zeros((8, 128), F32) if halo is None else halo[:, cols].astype(F32)
        pad[i, 8 : 8 + TOK, :] = rows[:, cols].astype(F32)
        w = weight[:, cols].astype(F32)
        total = pad[i, 5 : 5 + TOK, :] * w[0:1, :]
        for k in range(1, 4):
            total = total + pad[i, 5 + k : 5 + k + TOK, :] * w[k : k + 1, :]
        out.append(silu(total))
    return jnp.concatenate(out, axis=1) if len(out) > 1 else out[0]


def spread(cols, g):
    lane = lax.broadcasted_iota(jnp.int32, (cols.shape[0], 128), 1)
    out = []
    for i in range(0, PER, 2):
        h = g * PER + i
        out.append(jnp.where(lane < HEAD_DIM, cols[:, h : h + 1], cols[:, h + 1 : h + 2]))
    return jnp.concatenate(out, axis=1)


def begin(pairs, sems):
    copies = [pltpu.make_async_copy(v, w, sems.at[k]) for k, (v, w) in enumerate(pairs)]
    for copy in copies:
        copy.start()
    return copies


def group(g):
    return slice(g * GW, (g + 1) * GW), slice(g * STATE, (g + 1) * STATE)


def part(g, width):
    return pl.ds(g * width, width)


def states_kernel(
    step_from, bias_in, dlog_in, x_in, b_in, cw_in, cbw_in, c_in, st, ec, grow_out, ends_out,
    padx, padb, step_in, bias, dlog, x, b, cw, cbw, sems
):
    pairs = [(step_from, step_in), (bias_in, bias), (dlog_in, dlog)]
    pairs += [(x_in, x), (b_in, b), (cw_in, cw), (cbw_in, cbw)]
    pairs.append((c_in.at[pl.ds(TOK - 8, 8), :], ends_out.at[:, pl.ds(D + 1024, 1024)]))
    loads = begin(pairs, sems)
    for load in loads[:3]:
        load.wait()
    s = step_in[...].astype(F32).T + bias[...]
    step = jnp.maximum(s, 0.0) + jnp.log(1.0 + jnp.exp(-jnp.abs(s)))
    logs = step * (-jnp.exp(dlog[...]))
    r = lax.broadcasted_iota(jnp.int32, (TOK, TOK), 0)
    c = lax.broadcasted_iota(jnp.int32, (TOK, TOK), 1)
    tri = (c <= r).astype(F32)
    cum = jnp.dot(tri, logs, precision=lax.Precision.HIGHEST, preferred_element_type=F32)
    ec[...] = jnp.exp(cum)
    grow = step * jnp.exp(-cum)
    grow_out[...] = grow
    later = jnp.where(lax.broadcasted_iota(jnp.int32, (TOK, HEADS), 0) < 3, 0.0, grow)
    tot = cum[TOK - 1 : TOK, :]
    etot = jnp.exp(tot)
    first = grow[0:8, :] * etot
    sub = lax.broadcasted_iota(jnp.int32, (8, 128), 0)
    low = lax.broadcasted_iota(jnp.int32, (8, 128), 1) < HEAD_DIM
    for load in loads[3:]:
        load.wait()
    for g in range(GROUPS):
        xc, bc = group(g)
        xs = tap(padx.at[g], None, x[:, xc], cw[:, xc])
        bm = tap(padb.at[g], None, b[:, bc], cbw[:, bc]).astype(BF)
        v = (xs * spread(later, g)).astype(BF)
        fresh = lax.dot_general(v, bm, (((0,), (0,)), ((), ())), preferred_element_type=F32)

        def ends(rows, taps):
            out = jnp.where(sub < 3, pltpu.roll(rows[TOK - 8 :], 3, 0), pltpu.roll(rows[:8], 3, 0))
            return with_taps(out, taps)

        def with_taps(rows, taps):
            taps = taps.astype(F32)
            return jnp.where(sub == 6, taps[0:1], jnp.where(sub == 7, taps[1:2], rows))

        b_taps = cbw[:, bc]
        for i in range(2):
            h = g * PER + 2 * i
            o = g * 2 + i
            for j in range(2):
                k = (2 * i + j) * HEAD_DIM
                st[o, j * HEAD_DIM : (j + 1) * HEAD_DIM, :] = (
                    fresh[k : k + HEAD_DIM, :] * etot[0:1, h + j : h + j + 1]
                ).astype(BF)
            tail = jnp.zeros((8, 128), F32)
            for j in range(2):
                rest = jnp.broadcast_to(tot[0:1, h + j : h + j + 1], (8, 128))
                for q in range(3):
                    piece = rest.astype(BF).astype(F32)
                    tail = jnp.where(sub == 3 * j + q, piece, tail)
                    rest = rest - piece
            w = jnp.where(low, first[:, h : h + 1], first[:, h + 1 : h + 2])
            w_hi = w.astype(BF).astype(F32)
            w_both = jnp.where(sub < 3, w_hi, pltpu.roll(w - w_hi, 3, 0))
            oc = slice(o * 128, (o + 1) * 128)
            tail = with_taps(tail, cw[0:2, oc])
            w_both = with_taps(w_both, cw[2:4, oc])
            x_ends = ends(x[:, oc].astype(F32), b_taps[0:2])
            b_ends = ends(b[:, bc].astype(F32), b_taps[2:4])
            st[o, 128:144, :] = jnp.concatenate([tail, w_both], axis=0).astype(BF)
            st[o, 144:160, :] = jnp.concatenate([x_ends, b_ends], axis=0).astype(BF)
    ends_out[:, 0:D] = x[TOK - 8 :, :]
    ends_out[:, D : D + 1024] = b[TOK - 8 :, :]


def inner_kernel(
    x_in, b_in, c_in, halo_in, cw_in, cbw_in, ccw_in, ec_in, grow_in, skip_in, a_out, c_out,
    padx, padb, padc, x, b, c, halo, cw, cbw, ccw, ec, grow, skip, a_buf, cm_buf, sems, out_sems
):
    pairs = [(x_in, x), (b_in, b), (c_in, c), (halo_in, halo), (cw_in, cw), (cbw_in, cbw)]
    pairs += [(ccw_in, ccw), (ec_in, ec), (grow_in, grow), (skip_in, skip)]
    for load in begin(pairs, sems):
        load.wait()
    stores = []
    r = lax.broadcasted_iota(jnp.int32, (TOK, TOK), 0)
    s = lax.broadcasted_iota(jnp.int32, (TOK, TOK), 1)
    lower = s <= r
    cols = ec[...]
    rows = grow[...]
    sk = jnp.broadcast_to(skip[...], (TOK, HEADS))
    for g in range(GROUPS):
        xc = slice(g * GW, (g + 1) * GW)
        bc = slice(g * STATE, (g + 1) * STATE)
        bh = slice(D + g * STATE, D + (g + 1) * STATE)
        ch = slice(D + 1024 + g * STATE, D + 1024 + (g + 1) * STATE)
        xs = tap(padx.at[g], halo[:, xc], x[:, xc], cw[:, xc])
        bm = tap(padb.at[g], halo[:, bh], b[:, bc], cbw[:, bc]).astype(BF)
        cm = tap(padc.at[g], halo[:, ch], c[:, bc], ccw[:, bc]).astype(BF)
        cm_buf[:, bc] = cm
        v = (xs * spread(rows, g)).astype(BF)
        cb = lax.dot_general(cm, bm, (((1,), (1,)), ((), ())), preferred_element_type=F32)
        cb = jnp.where(lower, cb, 0.0).astype(BF)
        u = jnp.dot(cb, v, preferred_element_type=F32)
        a_buf[:, xc] = u * spread(cols, g) + xs * spread(sk, g)
        if g % 4 == 3:
            cols4 = part(g // 4, D // 2)
            stores.append(
                pltpu.make_async_copy(a_buf.at[:, cols4], a_out.at[:, cols4], out_sems.at[g // 4])
            )
            stores[-1].start()
    stores.append(pltpu.make_async_copy(cm_buf, c_out, out_sems.at[2]))
    stores[-1].start()
    for store in stores:
        store.wait()


def carry_kernel(got, out, buf, sems):
    count = got.shape[0]
    sub = lax.broadcasted_iota(jnp.int32, (count, 8, 128), 1)

    def starts(rows, w):
        before = jnp.concatenate([jnp.zeros((1, 8, 128), F32), rows[:-1]], axis=0)
        seq = jnp.where(sub < 3, before, rows)
        total = seq * w[0]
        for k in range(1, 4):
            total = total + pltpu.roll(seq, 8 - k, 1) * w[k]
        return jnp.where(sub < 3, silu(total), 0.0)

    tails = got[:, 128:144, :].astype(F32)
    ends = got[:, 144:160, :].astype(F32)
    w = tails[:, 8:16]
    w = w + pltpu.roll(w, 5, 1)
    x_taps = [tails[0:1, k : k + 1] for k in (6, 7, 14, 15)]
    b_taps = [ends[0:1, k : k + 1] for k in (6, 7, 14, 15)]
    xs = starts(ends[:, 0:8], x_taps)
    bm = starts(ends[:, 8:16], b_taps)
    vt = jnp.where(sub < 3, xs * w, 0.0).reshape(count * 8, 128).T
    bm = bm.reshape(count * 8, 128).astype(BF)
    lane = lax.broadcasted_iota(jnp.int32, (128, 128), 1)
    row = lax.broadcasted_iota(jnp.int32, (2 * HEAD_DIM, 128), 0)
    carry = jnp.zeros((2 * HEAD_DIM, 128), F32)
    stores = []
    for i in range(count):
        buf[i] = carry.astype(BF)
        if i % 4 == 3:
            rows = pl.ds(i - 3, 4)
            stores.append(pltpu.make_async_copy(buf.at[rows], out.at[rows], sems.at[i // 4]))
            stores[-1].start()
        if i + 1 < count:
            mine = jnp.where(lane // 8 == i, vt, 0.0).astype(BF)
            extra = jnp.dot(mine, bm, preferred_element_type=F32)
            tail = tails[i, 0:8]
            fa = jnp.exp(tail[0:1] + tail[1:2] + tail[2:3])
            fb = jnp.exp(tail[3:4] + tail[4:5] + tail[5:6])
            factor = jnp.where(row < HEAD_DIM, fa, fb)
            carry = carry * factor + (got[i, 0 : 2 * HEAD_DIM, :].astype(F32) + extra)
    for copy in stores:
        copy.wait()


def slots(routes, rw):
    both = jnp.concatenate([routes[...].astype(F32), rw[...], jnp.zeros((4, TOK), F32)], axis=0).T
    ids = both[:, 0:2].astype(jnp.int32)
    e = lax.broadcasted_iota(jnp.int32, (TOK, 128), 1)
    r = lax.broadcasted_iota(jnp.int32, (TOK, TOK), 0)
    s = lax.broadcasted_iota(jnp.int32, (TOK, TOK), 1)
    tri = (s < r).astype(BF)
    hot = [(ids[:, k : k + 1] == e).astype(F32) for k in range(2)]
    before0 = jnp.dot(tri, hot[0].astype(BF), preferred_element_type=F32)
    before1 = jnp.dot(tri, hot[1].astype(BF), preferred_element_type=F32)
    before1 = before1 + jnp.sum(hot[0], axis=0, keepdims=True)
    pos = [
        jnp.sum(before0 * hot[0], axis=1, keepdims=True).astype(jnp.int32),
        jnp.sum(before1 * hot[1], axis=1, keepdims=True).astype(jnp.int32),
    ]
    return [ids[:, k : k + 1] * 8 + pos[k] for k in range(2)], both[:, 2:4]


def routes_kernel(routes, rw, d_out):
    at, _ = slots(routes, rw)
    lane = lax.broadcasted_iota(jnp.int32, (TOK, ROWS), 1)
    for h in range(2):
        hit = (lane == at[0] + 4 * h) | (lane == at[1] + 4 * h)
        d_out[:, h * TOK : (h + 1) * TOK] = jnp.where(hit, 1.0, 0.0).T.astype(BF)


def weights_kernel(routes, rw, w_out):
    at, w = slots(routes, rw)
    lane = lax.broadcasted_iota(jnp.int32, (TOK, ROWS), 1)
    for h in range(2):
        comb = jnp.where(lane == at[0] + 4 * h, w[:, 0:1], 0.0)
        comb = comb + jnp.where(lane == at[1] + 4 * h, w[:, 1:2], 0.0)
        w_out[h * TOK : (h + 1) * TOK, :] = comb.astype(BF)


def norm_kernel(
    pref, ec_in, a_in, cm_in, gate_in, gain_in, w0, w1, w2, w3, w4, w5, w6, proj, rest,
    norm, wide, picked, ec, a, cm, gate, gain, sems
):
    pairs = [(ec_in, ec), (cm_in, cm), (gain_in, gain)]
    for q in range(4):
        pairs.append((a_in.at[:, part(q, 512)], a.at[:, part(q, 512)]))
        pairs.append((gate_in.at[:, part(q, 512)], gate.at[:, part(q, 512)]))
    for k, w in enumerate((w0, w1, w2, w3, w4, w5, w6)):
        pairs.append((w, wide.at[part(k, GW), :]))
    loads = begin(pairs, sems)
    for load in loads[:3]:
        load.wait()
    cols = ec[...]
    for g in range(GROUPS):
        xc, bc = group(g)
        if g % 2 == 0:
            loads[3 + g].wait()
            loads[4 + g].wait()
        outer = lax.dot_general(
            cm[:, bc], pref[g], (((1,), (1,)), ((), ())), preferred_element_type=F32
        )
        y = (a[:, xc] + outer * spread(cols, g)).astype(BF).astype(F32)
        y = y * silu(gate[:, xc].astype(F32))
        y = y * lax.rsqrt(jnp.mean(y * y, axis=1, keepdims=True) + EPS)
        norm[g] = (y * gain[:, xc]).astype(BF)
    me = lax.axis_index("dp")
    odd = me & 1
    at = (me + 6 + 4 * odd) & 7
    other = ((me ^ 1) + 6 - 4 * odd + 4) & 7
    place = [me, me ^ 1, at, at ^ 1, other, other ^ 1, me ^ 4, me ^ 5]
    for k in range(7):
        picked[:, k * GW : (k + 1) * GW] = norm[place[k]]
    rest[...] = norm[place[7]]
    for first, last in ((0, 4), (4, 6), (6, 7)):
        for load in loads[11 + first : 11 + last]:
            load.wait()
        rows = slice(first * GW, last * GW)
        y = jnp.dot(picked[:, rows], wide[rows, :], preferred_element_type=F32)
        proj[...] = y if first == 0 else proj[...] + y


def mix_kernel(
    proj_in, rest, fgain_in, resid_in, disp_in, w7, mixed_out, ein_out, send_out,
    wide, fgain, resid, disp, mixed_buf, ein_buf, send, sems, out_sems
):
    loads = begin([(w7, wide), (resid_in, resid), (fgain_in, fgain), (disp_in, disp)], sems)
    loads[0].wait()
    loads[1].wait()
    proj = resid[...].astype(F32) + proj_in[...] + jnp.dot(rest[...], wide[...], preferred_element_type=F32)
    loads[2].wait()
    mixed = proj.astype(BF)
    mixed_buf[...] = mixed
    stores = [pltpu.make_async_copy(mixed_buf, mixed_out, out_sems.at[0])]
    stores[0].start()
    m = mixed.astype(F32)
    ein = (m * lax.rsqrt(jnp.mean(m * m, axis=1, keepdims=True) + EPS) * fgain[...]).astype(BF)
    ein_buf[...] = ein
    stores.append(pltpu.make_async_copy(ein_buf, ein_out, out_sems.at[1]))
    stores[1].start()
    stack = jnp.concatenate([ein[:, :HALF], ein[:, HALF:]], axis=0)
    loads[3].wait()
    for q in range(4):
        rows = part(q, 256)
        send[rows, :] = jnp.dot(disp[rows, :], stack, preferred_element_type=F32).astype(BF)
        store = pltpu.make_async_copy(send.at[rows, :], send_out.at[rows, :], out_sems.at[2 + q])
        store.start()
        stores.append(store)
    for store in stores:
        store.wait()


def shared_kernel(ein, mixed, sg, su, sd, out):
    x = ein[...]
    gate = jnp.dot(x, sg[...], preferred_element_type=F32)
    up = jnp.dot(x, su[...], preferred_element_type=F32)
    hidden = (silu(gate) * up).astype(BF)
    out[...] = mixed[...].astype(F32) + jnp.dot(hidden, sd[...], preferred_element_type=F32)


def expert_kernel(got, wg_in, wu_in, wd_in, out, xbuf, wg, wu, wd, sems):
    pairs = ((wg_in, wg), (wu_in, wu), (wd_in, wd))
    loads = [pltpu.make_async_copy(v, w, sems.at[k]) for k, (v, w) in enumerate(pairs)]
    for load in loads:
        load.start()
    n = 256
    sub = lax.broadcasted_iota(jnp.int32, (ROWS // 16, 8, n), 1)
    for q in range(HALF // n):
        t = got[:, q * n : (q + 1) * n].astype(F32).reshape(ROWS // 16, 2, 8, n)
        r0, r1 = t[:, 0], t[:, 1]
        x0 = jnp.where(sub < 4, r0, pltpu.roll(r1, 4, 1))
        x1 = jnp.where(sub < 4, pltpu.roll(r0, 4, 1), r1)
        xbuf[:, q * n : (q + 1) * n] = x0.reshape(ROWS // 2, n).astype(BF)
        xbuf[:, HALF + q * n : HALF + (q + 1) * n] = x1.reshape(ROWS // 2, n).astype(BF)
    x = xbuf[...]
    loads[0].wait()
    gate = jnp.dot(x, wg[...], preferred_element_type=F32)
    loads[1].wait()
    up = jnp.dot(x, wu[...], preferred_element_type=F32)
    hidden = (silu(gate) * up).astype(BF)
    loads[2].wait()
    for q in range(HALF // n):
        y0 = jnp.dot(hidden, wd[:, q * n : (q + 1) * n], preferred_element_type=F32)
        y1 = jnp.dot(hidden, wd[:, HALF + q * n : HALF + (q + 1) * n], preferred_element_type=F32)
        y0 = y0.reshape(ROWS // 16, 8, n)
        y1 = y1.reshape(ROWS // 16, 8, n)
        o0 = jnp.where(sub < 4, y0, pltpu.roll(y1, 4, 1))
        o1 = jnp.where(sub < 4, pltpu.roll(y0, 4, 1), y1)
        out[:, q * n : (q + 1) * n] = jnp.stack([o0, o1], axis=1).reshape(ROWS, n).astype(BF)


def combine_kernel(got, w_in, base_in, out_ref, w, base, out, sems, out_sems):
    loads = begin([(w_in, w), (base_in, base)], sems)
    loads[0].wait()
    stores = []
    for h in range(2):
        cols = part(h, HALF)
        y = jnp.dot(w[part(h, TOK), :], got[...], preferred_element_type=F32)
        if h == 0:
            loads[1].wait()
        out[:, cols] = (base[:, cols] + y).astype(BF)
        stores.append(pltpu.make_async_copy(out.at[:, cols], out_ref.at[:, cols], out_sems.at[h]))
        stores[h].start()
    for copy in stores:
        copy.wait()


def plain(v):
    return with_memory_space_constraint(v, MemorySpace.Device)


def exchange(v, axis):
    return lax.all_to_all(plain(v), axis, split_axis=0, concat_axis=0, tiled=True)


def layer(
    residual, head_input, gate_input, b_input, c_input, step_input, conv_weight,
    conv_b_weight, conv_c_weight, step_bias, decay_log, skip, norm_gain, out_weight,
    ffn_gain, shared_gate, shared_up, shared_down, expert_gate, expert_up, expert_down,
    routes, route_weights,
):
    ways = lax.axis_size("sp")
    dps = lax.axis_size("dp")
    experts = ways * dps
    x, b, c = head_input[0], b_input[0], c_input[0]

    def ring(v):
        return lax.ppermute(v, "dp", [(i, (i + (-2 if i % 2 else 2)) % dps) for i in range(dps)])

    def swap(v):
        return lax.ppermute(v, "dp", [(i, i ^ 1) for i in range(dps)])

    partner = swap(out_weight)
    near = ring(out_weight)
    near2 = ring(partner)
    far = ring(near)
    pieces = [out_weight, partner, near, near2, swap(near), swap(near2)]
    pieces += [far, swap(far)]
    st, ec, grow, ends = call(
        states_kernel,
        [((ways, ST_ROWS, 128), BF), ((TOK, HEADS), F32), ((TOK, HEADS), F32), ((8, 4096), BF)],
        (step_input[0].T, step_bias[None], decay_log[None], x, b, conv_weight, conv_b_weight, c),
        raw=range(8),
        scratch=[
            pltpu.VMEM((GROUPS, 2, TOK + 8, 128), F32),
            pltpu.VMEM((GROUPS, 1, TOK + 8, 128), F32),
            pltpu.VMEM((HEADS, TOK), BF),
            pltpu.VMEM((1, HEADS), F32),
            pltpu.VMEM((1, HEADS), F32),
            pltpu.VMEM((TOK, D), BF),
            pltpu.VMEM((TOK, 1024), BF),
            pltpu.VMEM((4, D), BF),
            pltpu.VMEM((4, 1024), BF),
            pltpu.SemaphoreType.DMA((8,)),
        ],
    )
    got = exchange(st, "sp")
    halo = lax.ppermute(plain(ends), "sp", [(i, i + 1) for i in range(ways - 1)])
    a, cm = call(
        inner_kernel,
        [((TOK, D), F32), ((TOK, 1024), BF)],
        (x, b, c, halo, conv_weight, conv_b_weight, conv_c_weight, ec, grow, skip[None]),
        raw=range(10),
        free=(3,),
        raw_out=(0, 1),
        scratch=[
            pltpu.VMEM((GROUPS, 2, TOK + 8, 128), F32),
            pltpu.VMEM((GROUPS, 1, TOK + 8, 128), F32),
            pltpu.VMEM((GROUPS, 1, TOK + 8, 128), F32),
            pltpu.VMEM((TOK, D), BF),
            pltpu.VMEM((TOK, 1024), BF),
            pltpu.VMEM((TOK, 1024), BF),
            pltpu.VMEM((8, 4096), BF),
            pltpu.VMEM((4, D), BF),
            pltpu.VMEM((4, 1024), BF),
            pltpu.VMEM((4, 1024), BF),
            pltpu.VMEM((TOK, HEADS), F32),
            pltpu.VMEM((TOK, HEADS), F32),
            pltpu.VMEM((1, HEADS), F32),
            pltpu.VMEM((TOK, D), F32),
            pltpu.VMEM((TOK, 1024), BF),
            pltpu.SemaphoreType.DMA((10,)),
            pltpu.SemaphoreType.DMA((3,)),
        ],
        flops=4 * 10**9,
    )
    ways_in = (routes[0].T, route_weights[0].T)
    (disp,) = call(routes_kernel, [((ROWS, 2 * TOK), BF)], ways_in, flops=2 * 10**9)
    (comb,) = call(weights_kernel, [((2 * TOK, ROWS), BF)], ways_in, flops=2 * 10**9)
    (carried,) = call(
        carry_kernel,
        [((ways, 128, 128), BF)],
        (got,),
        vmem=(0,),
        raw_out=(0,),
        scratch=[pltpu.VMEM((ways, 128, 128), BF), pltpu.SemaphoreType.DMA((4,))],
    )
    pref = exchange(carried, "sp")
    proj, rest = call(
        norm_kernel,
        [((TOK, D), F32), ((TOK, GW), BF)],
        (
            pref.reshape(GROUPS, GW, STATE), ec, a, cm, gate_input[0], norm_gain[None],
            *pieces[:7],
        ),
        scratch=[
            pltpu.VMEM((GROUPS, TOK, GW), BF),
            pltpu.VMEM((7 * GW, D), BF),
            pltpu.VMEM((TOK, 7 * GW), BF),
            pltpu.VMEM((TOK, HEADS), F32),
            pltpu.VMEM((TOK, D), F32),
            pltpu.VMEM((TOK, 1024), BF),
            pltpu.VMEM((TOK, D), BF),
            pltpu.VMEM((1, D), F32),
            pltpu.SemaphoreType.DMA((18,)),
        ],
        vmem=(0,),
        raw=range(1, 13),
        free=range(7, 13),
        out_vmem=(0, 1),
        limit=32,
        flops=2 * 10**9,
    )
    mixed, ein, send = call(
        mix_kernel,
        [((TOK, D), BF), ((TOK, D), BF), ((ROWS, HALF), BF)],
        (proj, rest, ffn_gain[None], residual[0], disp, *pieces[7:]),
        scratch=[
            pltpu.VMEM((GW, D), BF),
            pltpu.VMEM((1, D), F32),
            pltpu.VMEM((TOK, D), BF),
            pltpu.VMEM((ROWS, 2 * TOK), BF),
            pltpu.VMEM((TOK, D), BF),
            pltpu.VMEM((TOK, D), BF),
            pltpu.VMEM((ROWS, HALF), BF),
            pltpu.SemaphoreType.DMA((4,)),
            pltpu.SemaphoreType.DMA((6,)),
        ],
        vmem=(0, 1),
        raw=range(2, 6),
        free=(5,),
        raw_out=(0, 1, 2),
        limit=28,
        flops=2 * 10**9,
    )
    arrived = exchange(plain(send).reshape(experts, 8, HALF), ("sp", "dp"))
    (base,) = call(
        shared_kernel,
        [((TOK, D), F32)],
        (ein, mixed, shared_gate, shared_up, shared_down),
        limit=20,
        flops=4 * 10**9,
    )
    (done,) = call(
        expert_kernel,
        [((ROWS, HALF), BF)],
        (arrived.reshape(ROWS, HALF), expert_gate[0], expert_up[0], expert_down[0]),
        scratch=[
            pltpu.VMEM((ROWS // 2, D), BF),
            pltpu.VMEM((D, 512), BF),
            pltpu.VMEM((D, 512), BF),
            pltpu.VMEM((512, D), BF),
            pltpu.SemaphoreType.DMA((3,)),
        ],
        vmem=(0,),
        raw=(1, 2, 3),
        out_vmem=(0,),
        limit=32,
        flops=3 * 10**9,
    )
    back = exchange(plain(done).reshape(experts, 8, HALF), ("sp", "dp"))
    (out,) = call(
        combine_kernel,
        [((TOK, D), BF)],
        (back.reshape(ROWS, HALF), comb, base),
        vmem=(0,),
        raw=(1, 2),
        raw_out=(0,),
        scratch=[
            pltpu.VMEM((2 * TOK, ROWS), BF),
            pltpu.VMEM((TOK, D), F32),
            pltpu.VMEM((TOK, D), BF),
            pltpu.SemaphoreType.DMA((2,)),
            pltpu.SemaphoreType.DMA((2,)),
        ],
    )
    return plain(out)[None]


def solution(mesh):
    rows = P("dp", "sp", None)
    one = P(("sp", "dp"), None, None)
    return jax.shard_map(
        layer,
        mesh=mesh,
        in_specs=(
            (rows,) * 6 + (P(),) * 7 + (P("dp", None),) + (P(),) * 4 + (one,) * 3 + (rows, rows)
        ),
        out_specs=rows,
        check_vma=False,
    )
```
